32 devices in a mesh: grp: 2 (over y), kv: 4 (over z), tp: 4 (over x, core).
Axes of the slice: x: 2, y: 2, z: 4, core: 2. Of those that a mesh axis runs over, the one named last changes fastest.
Arguments:
- candidate_embeddings: bfloat16 [1536, 4096], P(('grp', 'kv'), 'tp'), parts along dimension 0, may hold values from -100 to 100
- incoming_rms_scaling: float32 [4096], replicated, may hold values from 0.1 to 1.9
- probe_projector: bfloat16 [4096, 2048], P('kv', 'tp'), may hold values from -0.09375 to 0.09375
- address_projector: bfloat16 [4096, 2048], P('kv', 'tp'), may hold values from -0.09375 to 0.09375
- content_projector: bfloat16 [4096, 2048], P('kv', 'tp'), may hold values from -0.09375 to 0.09375
- sigmoid_mask_matrix: bfloat16 [4096, 2048], P('kv', 'tp'), may hold values from -0.09375 to 0.09375
- forgetting_projector: bfloat16 [4096, 16], replicated, may hold values from -0.09375 to 0.09375
- strength_projector_matrix: bfloat16 [4096, 16], replicated, may hold values from -0.09375 to 0.09375
- channel_forgetting_rates: float32 [16], P('tp'), may hold values from -3 to 0.5
- forgetting_offset: float32 [16], P('tp'), may hold values from -1 to 1
- extra_forgetting: float32 [384, 4, 16], P(('grp', 'kv'), None, 'tp'), parts along dimension 0, may hold values from -0.7 to 0, as said below
- outgoing_rms_scaling: float32 [128], replicated, may hold values from 0.1 to 1.9
- final_projector: bfloat16 [2048, 4096], P('tp', 'kv'), may hold values from -0.125 to 0.125
- memory_matrix: float32 [384, 16, 128, 128], P(('grp', 'kv'), 'tp'), parts along dimension 0, may hold values from -4 to 4
- earlier_addresses: bfloat16 [384, 4, 16, 128], P(('grp', 'kv'), None, 'tp'), parts along dimension 0, may hold values from -6 to 6
- earlier_contents: bfloat16 [384, 4, 16, 128], P(('grp', 'kv'), None, 'tp'), parts along dimension 0, may hold values from -6 to 6
- earlier_strengths: float32 [384, 4, 16], P(('grp', 'kv'), None, 'tp'), parts along dimension 0, may hold values from 0.1 to 0.9
- earlier_forgetting: float32 [384, 4, 16], P(('grp', 'kv'), None, 'tp'), parts along dimension 0, may hold values from -1.5 to -0.02
- admitted_counts: int32 [384], P(('grp', 'kv')), parts along dimension 0, may hold values from 0 to 4
Outputs:
- mixed: bfloat16 [1536, 4096], P(('grp', 'kv'), 'tp'), parts along dimension 0
- taken_state: float32 [384, 16, 128, 128], P(('grp', 'kv'), 'tp'), parts along dimension 0
The draws below stay inside these ranges and needn't reach their ends.
There are 2 independent parts, one for each index of `grp`. The reference program is written for one: setup_inputs(seed, part) draws one part's arguments, and reference() takes and returns one part's arrays. A program takes and returns all parts, laid end to end along the dimension named above; an argument that names none is the same for every part. Nothing has to cross between parts.
Inputs may be any that keep to these rules, and one draw needn't show every extreme that they name: `extra_forgetting`: mostly zero; elsewhere the logarithm of a factor between 0.5 and 0.8.
All inputs are finite; a program needn't handle non-finite values.
Results may differ from the reference program's by a relative error of at most 0.015.
Values may be sent and summed in bfloat16 or wider, within the bound.
A program may use at most 128 MiB of HBM per device.

```python
import math
import jax
import jax.numpy as jnp
from jax import lax

D = 4096
H = 16
DK = 128
P_SIZE = 4
SEQS = 192
ROWS = 768
N_TP = 4


def draw_candidate_embeddings(key, part):
    key = jax.random.fold_in(key, 11)
    key_base, key_rows = jax.random.split(key)
    values_raw = jax.random.truncated_normal(key_base, -4.0, 4.0, (ROWS, D), jnp.float32)
    column = jnp.exp(math.log(10.0) * jnp.arange(D, dtype=jnp.float32) / D)
    row_scale = jnp.exp(jax.random.uniform(key_rows, (ROWS, 1), jnp.float32, 0.0, math.log(10.0)))
    return (values_raw * column[None, :] * row_scale / 4.0).astype(jnp.bfloat16)


def draw_extra_forgetting(key, part):
    key = jax.random.fold_in(key, 23)
    key_where, key_size = jax.random.split(key)
    struck = jax.random.randint(key_where, (SEQS, P_SIZE, H), 0, 8) == 0
    strength = jnp.log(jax.random.uniform(key_size, (SEQS, P_SIZE, H), jnp.float32, 0.5, 0.8))
    return jnp.where(struck, strength, jnp.zeros((SEQS, P_SIZE, H), jnp.float32))


def draw_admitted_counts(key, part):
    key = jax.random.fold_in(key, 37)
    return jax.random.randint(key, (SEQS,), 0, P_SIZE + 1).astype(jnp.int32)


def level_of(own_key, shape, pieces, low, largest):
    level, own = 1.0, jax.random.fold_in(own_key, 6)
    for position, shards_of in pieces:
        draws = jnp.exp(jax.random.uniform(jax.random.fold_in(own, position), (shards_of,), jnp.float32, low / len(pieces), largest / len(pieces)))
        level = level * jnp.repeat(draws, shape[position] // shards_of).reshape([-1 if axis == position else 1 for axis in range(len(shape))])
    return level


def noise(own_key, extent, scale, bound, pieces=(), kind=jnp.bfloat16):
    result = scale * jax.random.normal(own_key, extent, jnp.float32)
    if pieces:
        result = result * level_of(own_key, extent, pieces, -0.22, 0.18)
    return jnp.clip(result, -bound, bound).astype(kind)


def setup_inputs(seed: int = 0, part: int = 0) -> dict:
    seeds = jax.random.split(jax.random.key(seed), 20)
    own_keys = jax.random.split(jax.random.fold_in(seeds[19], part), 20)
    candidate_embeddings = draw_candidate_embeddings(jax.random.fold_in(jax.random.fold_in(seeds[19], part), 71), part)
    incoming_rms_scaling = jnp.clip(1.0 + 0.18 * jax.random.normal(seeds[1], (D,), jnp.float32), 0.1, 1.9)
    probe_projector = noise(seeds[2], (D, H * DK), D ** -0.5, 0.09375, ((0, 4), (1, 4)))
    address_projector = noise(seeds[3], (D, H * DK), D ** -0.5, 0.09375, ((0, 4), (1, 4)))
    content_projector = noise(seeds[4], (D, H * DK), D ** -0.5, 0.09375, ((0, 4), (1, 4)))
    sigmoid_mask_matrix = noise(seeds[5], (D, H * DK), D ** -0.5, 0.09375, ((0, 4), (1, 4)))
    forgetting_projector = noise(seeds[6], (D, H), D ** -0.5, 0.09375)
    strength_projector_matrix = noise(seeds[7], (D, H), D ** -0.5, 0.09375)
    channel_forgetting_rates = jnp.clip(-3.0 + 3.5 * jax.random.uniform(seeds[8], (H,), jnp.float32) ** level_of(seeds[8], (H,), ((0, 4),), -0.2, 0.2), -3.0, 0.5)
    forgetting_offset = jnp.clip(jax.random.uniform(seeds[9], (H,), jnp.float32, -1.0, 1.0) * level_of(seeds[9], (H,), ((0, 4),), -0.4, 0.0), -1.0, 1.0)
    extra_forgetting = draw_extra_forgetting(jax.random.fold_in(jax.random.fold_in(seeds[19], part), 71), part)
    outgoing_rms_scaling = jnp.clip(1.0 + 0.18 * jax.random.normal(seeds[11], (DK,), jnp.float32), 0.1, 1.9)
    final_projector = noise(seeds[12], (H * DK, D), (H * DK) ** -0.5, 0.125, ((0, 4), (1, 4)))
    memory_matrix = noise(own_keys[13], (SEQS, H, DK, DK), 0.25, 4.0, ((0, 4), (1, 4)), jnp.float32)
    earlier_addresses = noise(own_keys[14], (SEQS, P_SIZE, H, DK), 1.0, 6.0, ((0, 4), (2, 4)))
    earlier_contents = noise(own_keys[15], (SEQS, P_SIZE, H, DK), 1.0, 6.0, ((0, 4), (2, 4)))
    earlier_strengths = jnp.clip(0.1 + 0.79999997 * jax.random.uniform(own_keys[16], (SEQS, P_SIZE, H), jnp.float32) ** level_of(own_keys[16], (SEQS, P_SIZE, H), ((0, 4), (2, 4)), -0.2, 0.2), 0.1, 0.9)
    earlier_forgetting = jnp.clip(-1.5 + 1.48 * jax.random.uniform(own_keys[17], (SEQS, P_SIZE, H), jnp.float32) ** level_of(own_keys[17], (SEQS, P_SIZE, H), ((0, 4), (2, 4)), -0.2, 0.2), -1.5, -0.02)
    admitted_counts = draw_admitted_counts(jax.random.fold_in(jax.random.fold_in(seeds[19], part), 71), part)
    return {"candidate_embeddings": candidate_embeddings, "incoming_rms_scaling": incoming_rms_scaling, "probe_projector": probe_projector, "address_projector": address_projector, "content_projector": content_projector, "sigmoid_mask_matrix": sigmoid_mask_matrix, "forgetting_projector": forgetting_projector, "strength_projector_matrix": strength_projector_matrix, "channel_forgetting_rates": channel_forgetting_rates, "forgetting_offset": forgetting_offset, "extra_forgetting": extra_forgetting, "outgoing_rms_scaling": outgoing_rms_scaling, "final_projector": final_projector, "memory_matrix": memory_matrix, "earlier_addresses": earlier_addresses, "earlier_contents": earlier_contents, "earlier_strengths": earlier_strengths, "earlier_forgetting": earlier_forgetting, "admitted_counts": admitted_counts}


epsilon = 1e-06
highest = lax.Precision.HIGHEST

def unit_norm(vector):
    return vector * lax.rsqrt(lax.optimization_barrier(jnp.sum(vector * vector, axis=-1, keepdims=True)) + epsilon)

def update(carry, key_vec, value_vec, beta, log_decay):
    decayed = jnp.exp(log_decay)[..., None, None] * carry
    recalled = jnp.einsum('shde,shd->she', decayed, key_vec, precision=highest)
    return decayed + jnp.einsum('shd,she->shde', key_vec, beta[..., None] * (value_vec - recalled), precision=highest)

def stored(values):
    return lax.optimization_barrier(values.astype(jnp.bfloat16)).astype(jnp.float32)

def reference(candidate_embeddings, incoming_rms_scaling, probe_projector, address_projector, content_projector, sigmoid_mask_matrix, forgetting_projector, strength_projector_matrix, channel_forgetting_rates, forgetting_offset, extra_forgetting, outgoing_rms_scaling, final_projector, memory_matrix, earlier_addresses, earlier_contents, earlier_strengths, earlier_forgetting, admitted_counts):
    floated = candidate_embeddings.astype(jnp.float32)
    normed = (floated * lax.rsqrt(lax.optimization_barrier(jnp.mean(floated * floated, axis=1, keepdims=True)) + epsilon) * incoming_rms_scaling).astype(jnp.bfloat16)

    def project(weight):
        return stored(jnp.dot(normed, weight, preferred_element_type=jnp.float32)).reshape(SEQS, P_SIZE, H, DK)
    query = unit_norm(project(probe_projector)) * DK ** (-0.5)
    keyed = unit_norm(project(address_projector))
    valued = project(content_projector)
    gated = project(sigmoid_mask_matrix)
    forgetting_argument = jnp.dot(normed, forgetting_projector, preferred_element_type=jnp.float32).reshape(SEQS, P_SIZE, H)
    beta_in = jnp.dot(normed, strength_projector_matrix, preferred_element_type=jnp.float32).reshape(SEQS, P_SIZE, H)
    forgetting_multiplier = -jnp.exp(channel_forgetting_rates) * jax.nn.softplus(forgetting_argument + forgetting_offset) + extra_forgetting
    beta = jax.nn.sigmoid(beta_in)
    carried = memory_matrix
    for proposal in range(P_SIZE):
        fresh = update(carried, unit_norm(earlier_addresses[:, proposal].astype(jnp.float32)), earlier_contents[:, proposal].astype(jnp.float32), earlier_strengths[:, proposal], earlier_forgetting[:, proposal])
        live = (admitted_counts > proposal)[:, None, None, None]
        carried = jnp.where(live, fresh, carried)
    running = carried
    outputs = []
    for proposal in range(P_SIZE):
        running = update(running, keyed[:, proposal], valued[:, proposal], beta[:, proposal], forgetting_multiplier[:, proposal])
        outputs.append(jnp.einsum('shde,shd->she', running, query[:, proposal], precision=highest))
    attended = jnp.stack(outputs, axis=1)
    scaled = attended * lax.rsqrt(lax.optimization_barrier(jnp.mean(attended * attended, axis=-1, keepdims=True)) + epsilon) * outgoing_rms_scaling * jax.nn.silu(gated)
    flat = scaled.astype(jnp.bfloat16).reshape(ROWS, N_TP, H * DK // N_TP)
    weights = final_projector.reshape(N_TP, H * DK // N_TP, D)
    partial_value = jnp.einsum('rtc,tcd->rtd', flat.astype(jnp.float32), weights.astype(jnp.float32))
    mixed = lax.optimization_barrier(jnp.sum(stored(partial_value), axis=1)).astype(jnp.bfloat16)
    return (mixed, carried)
```

```python
import functools

import jax
import jax.numpy as jnp
from jax import lax
from jax.experimental import pallas as pl
from jax.experimental.pallas import tpu as pltpu
from jax.sharding import PartitionSpec as P

DK = 128
P_SIZE = 4
SB = 8
TALL = SB * P_SIZE
epsilon = 1e-06
f32 = jnp.float32
bf16 = jnp.bfloat16


def lane_dot(a, b):
    return jnp.sum(a * b, axis=-1, keepdims=True)


def first_half():
    return lax.broadcasted_iota(jnp.int32, (8, DK), 0) < P_SIZE


def load_heads(heads, src, dst, factor=None):
    for h in range(heads):
        part = src[:, h * DK : (h + 1) * DK].astype(f32)
        dst[pl.ds(h * TALL, TALL), :] = part if factor is None else (part * factor).astype(bf16).astype(f32)


def tile(h, pair):
    return pl.ds(h * TALL + pair * 8, 8)


def proposal(h, p):
    return pl.ds(h * TALL + p, SB, stride=P_SIZE)


def accepted_kernel(heads, s_ref, k_ref, v_ref, n_ref, o_ref, r_scr, u_scr, c_scr, kf, vf):
    load_heads(heads, k_ref, kf)
    load_heads(heads, v_ref, vf)
    low = first_half()
    for pair in range(SB // 2):
        for h in range(heads):
            at = tile(h, pair)
            lhs = kf[at, :].astype(bf16)
            r0 = jnp.dot(lhs, s_ref[2 * pair, h].astype(bf16), preferred_element_type=f32)
            r1 = jnp.dot(lhs, s_ref[2 * pair + 1, h].astype(bf16), preferred_element_type=f32)
            r_scr[at, :] = jnp.where(low, r0, r1)
    few = n_ref[...]
    span = P_SIZE * heads
    count = few[:, 2 * span : 2 * span + 1]
    for h in range(heads):
        scale = jnp.ones((SB, 1), f32)
        ks, us, norms = [], [], []
        for p in range(P_SIZE):
            at = proposal(h, p)
            col = slice(p * heads + h, p * heads + h + 1)
            key = kf[at, :]
            norm = lax.rsqrt(lane_dot(key, key) + epsilon)
            live = count > float(p)
            g = jnp.where(live, jnp.exp(few[:, p * heads + h : p * heads + h + 1]), 1.0)
            b = jnp.where(live, few[:, span + p * heads + h : span + p * heads + h + 1], 0.0)
            rec = (scale * norm) * r_scr[at, :]
            for ki, ui, ni in zip(ks, us, norms):
                rec = rec + (lane_dot(ki, key) * (ni * norm)) * ui
            us = [ui * g for ui in us]
            scale = scale * g
            us.append(b * (vf[at, :] - g * rec))
            ks.append(key)
            norms.append(norm)
        for p in range(P_SIZE):
            u_scr[proposal(h, p), :] = us[p] * norms[p]
        c_scr[pl.ds(h * SB, SB), :] = jnp.broadcast_to(scale, (SB, DK))
    for pair in range(SB // 2):
        for h in range(heads):
            at = tile(h, pair)
            key = kf[at, :]
            lhs = jnp.concatenate([key, key], axis=0).astype(bf16)
            u = u_scr[at, :]
            hi = u.astype(bf16).astype(f32)
            lo = u - hi
            for half in range(2):
                keep = low if half == 0 else jnp.logical_not(low)
                rhs = jnp.concatenate([jnp.where(keep, hi, 0.0), jnp.where(keep, lo, 0.0)], axis=0).astype(bf16)
                seq = 2 * pair + half
                add = lax.dot_general(lhs, rhs, (((0,), (0,)), ((), ())), preferred_element_type=f32)
                o_ref[seq, h] = c_scr[pl.ds(h * SB + seq, 1), :] * s_ref[seq, h] + add


def attend_kernel(heads, s_ref, a_ref, q_ref, k_ref, v_ref, z_ref, d_ref, b_ref, w_ref, o_ref, kept, rk, rq, qf, kf, vf, zf, of, done):
    keep = pltpu.make_async_copy(s_ref, kept.at[pl.ds(pl.program_id(0) * SB, SB)], done)
    keep.start()
    for src, dst in ((q_ref, qf), (k_ref, kf), (v_ref, vf), (z_ref, zf)):
        load_heads(heads, src, dst, a_ref[...])
    low = first_half()
    for pair in range(SB // 2):
        for h in range(heads):
            at = tile(h, pair)
            lhs = jnp.concatenate([kf[at, :], qf[at, :]], axis=0).astype(bf16)
            r0 = jnp.dot(lhs, s_ref[2 * pair, h].astype(bf16), preferred_element_type=f32)
            r1 = jnp.dot(lhs, s_ref[2 * pair + 1, h].astype(bf16), preferred_element_type=f32)
            rk[at, :] = jnp.where(low, r0[:8], r1[:8])
            rq[at, :] = jnp.where(low, r0[8:], r1[8:])
    gain = w_ref[...]
    for h in range(heads):
        scale = jnp.ones((SB, 1), f32)
        ks, us, norms = [], [], []
        for p in range(P_SIZE):
            at = proposal(h, p)
            col = slice(p * heads + h, p * heads + h + 1)
            key = kf[at, :]
            query = qf[at, :]
            norm = lax.rsqrt(lane_dot(key, key) + epsilon)
            qnorm = lax.rsqrt(lane_dot(query, query) + epsilon) * DK ** (-0.5)
            g = jnp.exp(d_ref[:, col])
            rec = (scale * norm) * rk[at, :]
            for ki, ui, ni in zip(ks, us, norms):
                rec = rec + (lane_dot(ki, key) * (ni * norm)) * ui
            us = [ui * g for ui in us]
            scale = scale * g
            us.append(b_ref[:, col] * (vf[at, :] - g * rec))
            ks.append(key)
            norms.append(norm)
            att = (scale * qnorm) * rq[at, :]
            for ki, ui, ni in zip(ks, us, norms):
                att = att + (lane_dot(ki, query) * (ni * qnorm)) * ui
            gate = zf[at, :]
            mean = jnp.sum(att * att, axis=-1, keepdims=True) / DK
            of[at, :] = att * lax.rsqrt(mean + epsilon) * gain * (gate * jax.nn.sigmoid(gate))
    for h in range(heads):
        o_ref[:, h * DK : (h + 1) * DK] = of[pl.ds(h * TALL, TALL), :].astype(bf16)
    keep.wait()


def accepted(state, keys, values, few):
    seqs, heads = state.shape[:2]
    width = heads * DK
    rows = TALL
    tall = pl.BlockSpec((rows, width), lambda i: (i, 0))
    thin = pl.BlockSpec((SB, few.shape[1]), lambda i: (i, 0))
    block = pl.BlockSpec((SB, heads, DK, DK), lambda i: (i, 0, 0, 0))
    return pl.pallas_call(
        functools.partial(accepted_kernel, heads),
        grid=(seqs // SB,),
        in_specs=[block, tall, tall, thin],
        out_specs=block,
        out_shape=jax.ShapeDtypeStruct(state.shape, f32),
        scratch_shapes=[pltpu.VMEM((heads * n, DK), f32) for n in (TALL, TALL, SB, TALL, TALL)],
        cost_estimate=pl.CostEstimate(flops=10_000_000_000, bytes_accessed=2 * state.size * 4, transcendentals=0),
        name="accepted",
    )(state, keys, values, few)


def attend(state, packed, factor, decay, beta, gain):
    seqs, heads = state.shape[:2]
    width = heads * DK
    rows = TALL
    thin = pl.BlockSpec((SB, P_SIZE * heads), lambda i: (i, 0))
    block = pl.BlockSpec((SB, heads, DK, DK), lambda i: (i, 0, 0, 0))

    def part(n):
        return pl.BlockSpec((None, rows, width), lambda i: (n, i, 0))

    return pl.pallas_call(
        functools.partial(attend_kernel, heads),
        grid=(seqs // SB,),
        in_specs=[block, pl.BlockSpec((rows, 1), lambda i: (i, 0)), part(0), part(1), part(2), part(3), thin, thin, pl.BlockSpec((1, DK), lambda i: (0, 0))],
        out_specs=[pl.BlockSpec((rows, width), lambda i: (i, 0)), pl.BlockSpec(memory_space=pl.ANY)],
        out_shape=[jax.ShapeDtypeStruct((seqs * P_SIZE, width), bf16), jax.ShapeDtypeStruct(state.shape, f32)],
        scratch_shapes=[pltpu.VMEM((heads * TALL, DK), f32)] * 7 + [pltpu.SemaphoreType.DMA],
        cost_estimate=pl.CostEstimate(flops=5_000_000_000, bytes_accessed=state.size * 4, transcendentals=0),
        name="attend",
    )(state, factor, packed, packed, packed, packed, decay, beta, gain.reshape(1, DK))


def pick(index, values):
    chosen = values[-1]
    for at, value in enumerate(values[:-1]):
        chosen = jnp.where(index == at, value, chosen)
    return chosen


def turned_slot(t):
    return pick(t, (0, 2, 1, 3))


def project_kernel(x_ref, gain_ref, keys, values, thin, fs, wq, wk, wv, wz, wo, state, acc, few_ref, taken, f_out,
                   xbuf, gbuf, w, fbuf, sbuf, abuf, bbuf, cbuf, esend, erecv, s_in, s_out, r_scr, u_scr, c_scr, kf, vf,
                   xs, xr, wsem, ss, ar, br, cr, es, er, ins, outs, fsem, fss, fzr, fys, fyr, fos):
    k, t, g = lax.axis_index("kv"), lax.axis_index("tp"), lax.axis_index("grp")
    depth, width = w.shape[1], w.shape[2]
    rows = x_ref.shape[0]

    def remote(src, dst, send, recv, kv, tp, grp=g):
        return pltpu.make_async_remote_copy(
            src, dst, send, recv, device_id={"grp": grp, "kv": kv, "tp": tp}, device_id_type=pl.DeviceIdType.MESH
        )

    loads = [pltpu.make_async_copy(src, w.at[i], wsem.at[i]) for i, src in enumerate((wq, wk, wv, wz))]
    slot = turned_slot(t)
    far_t, far_k = turned_slot(k), t
    home = jnp.logical_and(far_k == k, far_t == t)
    first = remote(x_ref, xbuf.at[k], xs.at[0], xr.at[k], far_k, far_t)
    local = pltpu.make_async_copy(x_ref, xbuf.at[k], xr.at[k])

    @pl.when(jnp.logical_not(home))
    def _():
        first.start()

    @pl.when(home)
    def _():
        local.start()

    f_load = pltpu.make_async_copy(wo, fbuf.at[k], fsem)
    f_load.start()
    for load in loads:
        load.start()

    blocks = state.shape[0] // SB
    heads = state.shape[1]

    def fetch(i):
        return pltpu.make_async_copy(state.at[pl.ds(i * SB, SB)], s_in.at[i % 2], ins.at[i % 2])

    def put(i):
        return pltpu.make_async_copy(s_out.at[i % 2], taken.at[pl.ds(i * SB, SB)], outs.at[i % 2])

    fetch(0).start()

    beside = t + 1 - 2 * (t % 2)
    across = (t + 2) % 4

    def arrived(s):
        remote(xbuf.at[s], xbuf.at[s], xs.at[0], xr.at[s], k, beside).wait_recv()

    @pl.when(home)
    def _():
        local.wait()

    @pl.when(jnp.logical_not(home))
    def _():
        arrived(slot)

    over = remote(xbuf.at[slot], xbuf.at[slot], xs.at[1], xr.at[slot], k, across)
    over.start()
    near_x = remote(xbuf.at[slot], xbuf.at[slot], xs.at[2], xr.at[slot], k, beside)
    near_x.start()

    half_rows = fbuf.shape[1] // 2
    half = pl.ds(g * half_rows, half_rows)

    def f_pass(c, to, sem):
        return remote(fbuf.at[c, half], fbuf.at[c, half], fss.at[sem], fzr.at[c], to, t)

    def f_swap(c):
        return remote(fbuf.at[c, half], fbuf.at[c, half], fys.at[c], fyr.at[c], k, t, 1 - g)

    f_load.wait()

    @pl.when(k < 3)
    def _():
        f_pass(k, k + 1, 4).start()

    @pl.when(k > 0)
    def _():
        f_pass(k, k - 1, 5).start()

    def f_forwards(c):
        return jnp.logical_or(jnp.logical_and(c < k, k < 3), jnp.logical_and(c > k, k > 0))

    def f_take(c):
        to = jnp.where(c < k, k + 1, k - 1)
        f_pass(c, k, c).wait_recv()

        @pl.when(f_forwards(c))
        def _():
            f_pass(c, to, c).start()

        f_swap(c).start()

    end = jnp.where(k <= 1, 0, 3)
    near = jnp.where(k <= 1, 1, 2)
    is_end = k == end
    inside = jnp.logical_not(is_end)
    f_order = (jnp.where(is_end, near, end), 3 - near, 3 - end)

    other = turned_slot(across)
    arrived(other)
    onward = remote(xbuf.at[other], xbuf.at[other], xs.at[3], xr.at[other], k, beside)
    onward.start()
    arrived(turned_slot(beside))
    arrived(turned_slot((beside + 2) % 4))
    for load in loads:
        load.wait()

    nt = (((1,), (1,)), ((), ()))
    thin_rows = fs.shape[0]

    def prepare(r):
        floated = xbuf[r].astype(f32)
        gained = (floated * gain_ref[k]).astype(bf16)
        gbuf[r] = gained
        squares = floated * floated
        high = squares.astype(bf16)
        rest = (squares - high.astype(f32)).astype(bf16)
        ones = jnp.ones((8, depth), bf16)
        esend[r, 0:thin_rows, :] = lax.dot_general(fs[...], gained, nt, preferred_element_type=f32)
        esend[r, thin_rows:, :] = lax.dot_general(ones, high, nt, preferred_element_type=f32) + lax.dot_general(
            ones, rest, nt, preferred_element_type=f32
        )

        @pl.when(r != k)
        def _():
            remote(esend.at[r], erecv.at[k], es.at[r], er.at[k], r, t).start()

    def product(r, c):
        return jnp.dot(gbuf[r], w[c], preferred_element_type=f32)

    def from_end(i):
        remote(abuf.at[i], abuf.at[i], ss.at[i], ar.at[i], k, beside).wait_recv()
        return abuf[i].astype(f32)

    def from_inner(i):
        remote(bbuf.at[i], bbuf.at[i], ss.at[i], br.at[i], k, beside).wait_recv()
        return bbuf[i].astype(f32)

    def accept(i):
        @pl.when(i + 1 < blocks)
        def _():
            fetch(i + 1).start()

        fetch(i).wait()

        @pl.when(i >= 2)
        def _():
            put(i - 2).wait()

        tall, few_rows = pl.ds(i * TALL, TALL), pl.ds(i * SB, SB)
        accepted_kernel(
            heads, s_in.at[i % 2], keys.at[tall], values.at[tall], thin.at[few_rows], s_out.at[i % 2],
            r_scr, u_scr, c_scr, kf, vf,
        )
        put(i).start()

    def step(i, carry):
        stage, c = i // 4, i % 4
        r = pick(stage, (3 - end, 3 - near, near))

        @pl.when(c == 0)
        def _():
            prepare(r)

        @pl.when(i == 2)
        def _():
            prepare(end)

        @pl.when(is_end)
        def _():
            sbuf[i] = product(r, c).astype(bf16)
            remote(sbuf.at[i], abuf.at[i], ss.at[i], ar.at[i], near, t).start()

        @pl.when(jnp.logical_and(inside, i == 1))
        def _():
            f_take(f_order[0])
            f_take(f_order[1])

        @pl.when(jnp.logical_and(inside, i == 5))
        def _():
            f_take(f_order[2])

        @pl.when(jnp.logical_and(is_end, i == 4))
        def _():
            f_take(f_order[0])

        @pl.when(jnp.logical_and(inside, i < 8))
        def _():
            part = product(r, c)
            sbuf[i] = (part + from_end(i)).astype(bf16)
            remote(sbuf.at[i], bbuf.at[i], ss.at[i], br.at[i], 3 - near, t).start()

        @pl.when(jnp.logical_and(inside, stage == 1))
        def _():
            part = product(end, c)
            sbuf[8 + c] = (part + from_inner(c)).astype(bf16)
            remote(sbuf.at[8 + c], cbuf.at[c], ss.at[8 + c], cr.at[c], end, t).start()

        @pl.when(jnp.logical_and(inside, stage == 2))
        def _():
            acc[c] = product(r, c) + from_inner(4 + c) + from_end(i)

        @pl.when(i % 2 == 0)
        def _():
            accept(i // 2)

        return carry

    lax.fori_loop(0, 12, step, 0)
    for i in range(max(blocks - 2, 0), blocks):
        put(i).wait()

    @pl.when(is_end)
    def _():
        f_take(f_order[1])

        def finish(c, carry):
            part = product(end, c)
            remote(cbuf.at[c], cbuf.at[c], ss.at[c], cr.at[c], k, beside).wait_recv()
            acc[c] = part + cbuf[c].astype(f32)
            return carry

        lax.fori_loop(0, 4, finish, 0)
        f_take(f_order[2])

    few_ref[...] = esend[k]
    for src in range(4):

        @pl.when(k != src)
        def _():
            remote(esend.at[src], erecv.at[src], es.at[src], er.at[src], k, beside).wait()
            few_ref[...] += erecv[src]
            remote(fbuf.at[src, half], fbuf.at[src, half], fys.at[src], fyr.at[src], k, beside).wait()

        pltpu.make_async_copy(fbuf.at[src], f_out.at[src], fos.at[src]).start()

    @pl.when(jnp.logical_not(home))
    def _():
        first.wait_send()

    over.wait_send()
    near_x.wait_send()
    onward.wait_send()

    @pl.when(k < 3)
    def _():
        f_pass(k, k, 4).wait_send()

    @pl.when(k > 0)
    def _():
        f_pass(k, k, 5).wait_send()

    for src in range(4):

        @pl.when(jnp.logical_and(k != src, f_forwards(src)))
        def _():
            f_pass(src, k, src).wait_send()

        pltpu.make_async_copy(fbuf.at[src], f_out.at[src], fos.at[src]).wait()

    for i in range(12):
        remote(sbuf.at[i], abuf.at[i], ss.at[i], ar.at[i], k, beside).wait_send()


def project(x, gain, weights, few_weights, final, state, keys, values, thin):
    rows, depth = x.shape
    width = weights[0].shape[1]
    thin_rows = few_weights.shape[0]
    vmem, hbm = pl.BlockSpec(memory_space=pltpu.VMEM), pl.BlockSpec(memory_space=pl.ANY)
    dma = pltpu.SemaphoreType.DMA
    heads = state.shape[1]

    def chunks(n):
        return pltpu.VMEM((n, rows, width), bf16)

    return pl.pallas_call(
        project_kernel,
        in_specs=[vmem] * 6 + [hbm] * 6,
        out_specs=[vmem, vmem, hbm, hbm],
        out_shape=[
            jax.ShapeDtypeStruct((4, rows, width), f32),
            jax.ShapeDtypeStruct((thin_rows + 8, rows), f32),
            jax.ShapeDtypeStruct(state.shape, f32),
            jax.ShapeDtypeStruct((4,) + final.shape, bf16),
        ],
        scratch_shapes=[
            pltpu.VMEM((4, rows, depth), bf16),
            pltpu.VMEM((4, rows, depth), bf16),
            pltpu.VMEM((4, depth, width), bf16),
            pltpu.VMEM((4,) + final.shape, bf16),
            chunks(12), chunks(12), chunks(8), chunks(4),
            pltpu.VMEM((4, thin_rows + 8, rows), f32),
            pltpu.VMEM((4, thin_rows + 8, rows), f32),
            pltpu.VMEM((2, SB) + state.shape[1:], f32),
            pltpu.VMEM((2, SB) + state.shape[1:], f32),
            *[pltpu.VMEM((heads * n, DK), f32) for n in (TALL, TALL, SB, TALL, TALL)],
            dma((4,)), dma((4,)), dma((4,)), dma((12,)), dma((12,)), dma((8,)), dma((4,)), dma((4,)), dma((4,)),
            dma((2,)), dma((2,)), dma, dma((6,)), dma((4,)), dma((4,)), dma((4,)), dma((4,)),
        ],
        compiler_params=pltpu.CompilerParams(has_side_effects=True, vmem_limit_bytes=56 * 2**20),
        name="project",
    )(x, gain.reshape(-1, 1, depth), keys, values, thin, few_weights, *weights, final, state)


PIECES = 3


def mix_kernel(flat_ref, f_hbm, o_ref, w, part, mate, cross, wsem, ms, mr, xs, xr):
    k, t, g = lax.axis_index("kv"), lax.axis_index("tp"), lax.axis_index("grp")
    rows = flat_ref.shape[0]
    piece = rows // PIECES
    beside = t + 1 - 2 * (t % 2)
    across = (t + 2) % 4
    order = ((beside + 2) % 4, across, beside, t)

    def remote(src, dst, send, recv, tp):
        return pltpu.make_async_remote_copy(
            src, dst, send, recv, device_id={"grp": g, "kv": k, "tp": tp}, device_id_type=pl.DeviceIdType.MESH
        )

    loads = [pltpu.make_async_copy(f_hbm.at[c], w.at[n], wsem.at[n]) for n, c in enumerate(order)]
    for load in loads:
        load.start()

    def to_mate(n, s):
        at = pl.ds(s * piece, piece)
        return remote(part.at[2 * n, at], mate.at[n, at], ms.at[n, s], mr.at[n, s], beside)

    def to_cross(s):
        at = pl.ds(s * piece, piece)
        return remote(part.at[1, at], cross.at[at], xs.at[s], xr.at[s], across)

    def fill(n, s):
        at = pl.ds(s * piece, piece)
        return jnp.dot(flat_ref[at, :], w[n], preferred_element_type=f32).astype(bf16)

    loads[0].wait()
    for s in range(PIECES):
        part[0, s * piece : (s + 1) * piece, :] = fill(0, s)
        to_mate(0, s).start()
    loads[1].wait()
    for s in range(PIECES):
        at = slice(s * piece, (s + 1) * piece)
        mine = fill(1, s).astype(f32)
        to_mate(0, s).wait_recv()
        part[1, at, :] = (mine + mate[0, at, :].astype(f32)).astype(bf16)
        to_cross(s).start()
    loads[2].wait()
    for s in range(PIECES):
        part[2, s * piece : (s + 1) * piece, :] = fill(2, s)
        to_mate(1, s).start()
    loads[3].wait()
    for s in range(PIECES):
        part[3, s * piece : (s + 1) * piece, :] = fill(3, s)
    for s in range(PIECES):
        at = slice(s * piece, (s + 1) * piece)
        to_mate(1, s).wait_recv()
        to_cross(s).wait_recv()
        o_ref[at, :] = (
            part[3, at, :].astype(f32) + mate[1, at, :].astype(f32) + cross[at, :].astype(f32)
        ).astype(bf16)
    for s in range(PIECES):
        to_mate(0, s).wait_send()
        to_mate(1, s).wait_send()
        to_cross(s).wait_send()


def mix(flat, final):
    rows, width = flat.shape
    cols = final.shape[2]
    vmem, hbm = pl.BlockSpec(memory_space=pltpu.VMEM), pl.BlockSpec(memory_space=pl.ANY)
    dma = pltpu.SemaphoreType.DMA
    return pl.pallas_call(
        mix_kernel,
        in_specs=[vmem, hbm],
        out_specs=vmem,
        out_shape=jax.ShapeDtypeStruct((rows, cols), bf16),
        scratch_shapes=[
            pltpu.VMEM((4, width, cols), bf16),
            pltpu.VMEM((4, rows, cols), bf16),
            pltpu.VMEM((2, rows, cols), bf16),
            pltpu.VMEM((rows, cols), bf16),
            dma((4,)), dma((2, PIECES)), dma((2, PIECES)), dma((PIECES,)), dma((PIECES,)),
        ],
        compiler_params=pltpu.CompilerParams(has_side_effects=True, vmem_limit_bytes=56 * 2**20),
        name="mix",
    )(flat, final)


def on_device(
    n_kv,
    n_tp,
    candidate_embeddings,
    incoming_rms_scaling,
    probe_projector,
    address_projector,
    content_projector,
    sigmoid_mask_matrix,
    forgetting_projector,
    strength_projector_matrix,
    channel_forgetting_rates,
    forgetting_offset,
    extra_forgetting,
    outgoing_rms_scaling,
    final_projector,
    memory_matrix,
    earlier_addresses,
    earlier_contents,
    earlier_strengths,
    earlier_forgetting,
    admitted_counts,
):
    rows, local_cols = candidate_embeddings.shape
    features = incoming_rms_scaling.shape[0]
    depth, width = probe_projector.shape
    heads = width // DK
    seqs = rows // P_SIZE
    k_index, t_index = lax.axis_index("kv"), lax.axis_index("tp")

    def thin(values):
        return values.reshape(seqs, P_SIZE * heads)

    weights = (probe_projector, address_projector, content_projector, sigmoid_mask_matrix)
    earlier = (
        memory_matrix,
        earlier_addresses.reshape(rows, width),
        earlier_contents.reshape(rows, width),
        jnp.concatenate(
            [thin(earlier_forgetting), thin(earlier_strengths), admitted_counts.astype(f32).reshape(seqs, 1)], axis=1
        ),
    )
    if n_kv == 4 and n_tp == 4:
        few_weights = jnp.concatenate(
            [
                lax.dynamic_slice(m, (k_index * depth, t_index * heads), (depth, heads))
                for m in (forgetting_projector, strength_projector_matrix)
            ],
            axis=1,
        ).T
        summed, few, taken, columns = project(
            candidate_embeddings, incoming_rms_scaling, weights, few_weights, final_projector, *earlier
        )
        few = few[: 2 * heads + 1].T
    else:
        every = lax.all_gather(candidate_embeddings, "tp", axis=1, tiled=True)
        every = lax.all_to_all(every, "kv", split_axis=1, concat_axis=0, tiled=True)
        gain_part = lax.dynamic_slice_in_dim(incoming_rms_scaling, k_index * depth, depth)
        floated = every.astype(f32)
        gained = (floated * gain_part).astype(bf16)
        decay_cols = lax.dynamic_slice(forgetting_projector, (k_index * depth, t_index * heads), (depth, heads))
        beta_cols = lax.dynamic_slice(strength_projector_matrix, (k_index * depth, t_index * heads), (depth, heads))
        few = jnp.concatenate(
            [
                jnp.dot(gained, jnp.concatenate([decay_cols, beta_cols], axis=1), preferred_element_type=f32),
                jnp.sum(floated * floated, axis=1, keepdims=True),
            ],
            axis=1,
        )
        few = lax.psum_scatter(few, "kv", scatter_dimension=0, tiled=True)
        partial = jnp.stack([jnp.dot(gained, w, preferred_element_type=f32).astype(bf16) for w in weights])
        summed = lax.psum_scatter(partial, "kv", scatter_dimension=1, tiled=True).astype(f32)
        taken = accepted(*earlier)
    factor = lax.rsqrt(few[:, 2 * heads :] / features + epsilon)
    few = few[:, : 2 * heads] * factor
    decay_in = few[:, :heads].reshape(seqs, P_SIZE, heads)
    beta = jax.nn.sigmoid(few[:, heads:].reshape(seqs, P_SIZE, heads))
    decay = -jnp.exp(channel_forgetting_rates) * jax.nn.softplus(decay_in + forgetting_offset) + extra_forgetting
    flat, taken = attend(taken, summed, factor, thin(decay), thin(beta), outgoing_rms_scaling)
    if n_kv == 4 and n_tp == 4:
        mixed = mix(flat, columns)
    else:
        gathered = lax.all_gather(flat, "kv", axis=0, tiled=True)
        terms = jnp.dot(gathered, final_projector, preferred_element_type=f32).astype(bf16)
        terms = lax.all_to_all(terms, "kv", split_axis=0, concat_axis=1, tiled=True)
        mixed = lax.psum_scatter(terms, "tp", scatter_dimension=1, tiled=True)
    return (mixed, taken)


def solution(mesh):
    row, per_head = P(("grp", "kv"), "tp"), P(("grp", "kv"), None, "tp")
    four = P(("grp", "kv"), None, "tp", None)
    weight = P("kv", "tp")
    state = P(("grp", "kv"), "tp", None, None)
    in_specs = (
        row, P(), weight, weight, weight, weight, P(), P(), P("tp"), P("tp"), per_head, P(),
        P("tp", "kv"), state, four, four, per_head, per_head, P(("grp", "kv")),
    )
    body = functools.partial(on_device, mesh.shape["kv"], mesh.shape["tp"])
    return jax.shard_map(body, mesh=mesh, in_specs=in_specs, out_specs=(row, state), check_vma=False)
```

```python
import functools

import jax
import jax.numpy as jnp
from jax import lax
from jax.experimental import pallas as pl
from jax.experimental.pallas import tpu as pltpu
from jax.sharding import PartitionSpec as P

DK = 128
P_SIZE = 4
SB = 8
TALL = SB * P_SIZE
epsilon = 1e-06
f32 = jnp.float32
bf16 = jnp.bfloat16


def lane_dot(a, b):
    return jnp.sum(a * b, axis=-1, keepdims=True)


def first_half():
    return lax.broadcasted_iota(jnp.int32, (8, DK), 0) < P_SIZE


def load_heads(heads, src, dst, factor=None):
    for h in range(heads):
        part = src[:, h * DK : (h + 1) * DK].astype(f32)
        dst[pl.ds(h * TALL, TALL), :] = part if factor is None else (part * factor).astype(bf16).astype(f32)


def tile(h, pair):
    return pl.ds(h * TALL + pair * 8, 8)


def proposal(h, p):
    return pl.ds(h * TALL + p, SB, stride=P_SIZE)


def rows_to_columns(wide):
    count = wide.shape[1]
    same = lax.broadcasted_iota(jnp.int32, (count, count), 0) == lax.broadcasted_iota(jnp.int32, (count, count), 1)
    return lax.dot_general(
        same.astype(f32), wide, (((1,), (1,)), ((), ())),
        precision=lax.Precision.HIGHEST, preferred_element_type=f32,
    )


def accepted_kernel(heads, s_ref, k_ref, v_ref, n_ref, o_ref, r_scr, u_scr, c_scr, kf, vf):
    load_heads(heads, k_ref, kf)
    load_heads(heads, v_ref, vf)
    low = first_half()
    for pair in range(SB // 2):
        for h in range(heads):
            at = tile(h, pair)
            lhs = kf[at, :].astype(bf16)
            r0 = jnp.dot(lhs, s_ref[2 * pair, h].astype(bf16), preferred_element_type=f32)
            r1 = jnp.dot(lhs, s_ref[2 * pair + 1, h].astype(bf16), preferred_element_type=f32)
            r_scr[at, :] = jnp.where(low, r0, r1)
    few = n_ref[...]
    span = P_SIZE * heads
    count = few[:, 2 * span : 2 * span + 1]
    for h in range(heads):
        scale = jnp.ones((SB, 1), f32)
        ks, us, norms = [], [], []
        for p in range(P_SIZE):
            at = proposal(h, p)
            col = slice(p * heads + h, p * heads + h + 1)
            key = kf[at, :]
            norm = lax.rsqrt(lane_dot(key, key) + epsilon)
            live = count > float(p)
            g = jnp.where(live, jnp.exp(few[:, p * heads + h : p * heads + h + 1]), 1.0)
            b = jnp.where(live, few[:, span + p * heads + h : span + p * heads + h + 1], 0.0)
            rec = (scale * norm) * r_scr[at, :]
            for ki, ui, ni in zip(ks, us, norms):
                rec = rec + (lane_dot(ki, key) * (ni * norm)) * ui
            us = [ui * g for ui in us]
            scale = scale * g
            us.append(b * (vf[at, :] - g * rec))
            ks.append(key)
            norms.append(norm)
        for p in range(P_SIZE):
            u_scr[proposal(h, p), :] = us[p] * norms[p]
        c_scr[pl.ds(h * SB, SB), :] = jnp.broadcast_to(scale, (SB, DK))
    for pair in range(SB // 2):
        for h in range(heads):
            at = tile(h, pair)
            key = kf[at, :]
            lhs = jnp.concatenate([key, key], axis=0).astype(bf16)
            u = u_scr[at, :]
            hi = u.astype(bf16).astype(f32)
            lo = u - hi
            for half in range(2):
                keep = low if half == 0 else jnp.logical_not(low)
                rhs = jnp.concatenate([jnp.where(keep, hi, 0.0), jnp.where(keep, lo, 0.0)], axis=0).astype(bf16)
                seq = 2 * pair + half
                add = lax.dot_general(lhs, rhs, (((0,), (0,)), ((), ())), preferred_element_type=f32)
                o_ref[seq, h] = c_scr[pl.ds(h * SB + seq, 1), :] * s_ref[seq, h] + add


def attend_kernel(heads, features, few_ref, extra_ref, rate_ref, offset_ref, w_ref, parts_hbm, state, o_ref, kept,
                  held, parts, thin, rk, rq, qf, kf, vf, zf, of, ins, outs, psem):
    rows = o_ref.shape[0]
    blocks = state.shape[0] // SB
    pull = pltpu.make_async_copy(parts_hbm, parts, psem)
    pull.start()

    def fetch(i):
        return pltpu.make_async_copy(state.at[pl.ds(i * SB, SB)], held.at[pl.ds(i * SB, SB)], ins.at[i])

    def put(i):
        return pltpu.make_async_copy(held.at[pl.ds(i * SB, SB)], kept.at[pl.ds(i * SB, SB)], outs.at[i])

    for i in range(blocks):
        fetch(i).start()
    few = rows_to_columns(few_ref[...])
    factor = lax.rsqrt(few[:, 2 * heads : 2 * heads + 1] / features + epsilon)
    seqs = extra_ref.shape[1]
    row = lax.broadcasted_iota(jnp.int32, (rows, seqs), 0)
    owner = jnp.right_shift(row, 2) == lax.broadcasted_iota(jnp.int32, (rows, seqs), 1)
    spread = lax.dot_general(
        owner.astype(f32), extra_ref[...], (((1,), (1,)), ((), ())),
        precision=lax.Precision.HIGHEST, preferred_element_type=f32,
    )
    turn = jnp.bitwise_and(lax.broadcasted_iota(jnp.int32, (rows, heads), 0), 3)
    extra = pick(turn, [spread[:, p * heads : (p + 1) * heads] for p in range(P_SIZE)])
    raised = few[:, :heads] * factor + offset_ref[...]
    soft = jnp.maximum(raised, 0.0) + jnp.log1p(jnp.exp(-jnp.abs(raised)))
    thin[:, :heads] = jnp.exp(extra - jnp.exp(rate_ref[...]) * soft)
    thin[:, heads : 2 * heads] = jax.nn.sigmoid(few[:, heads : 2 * heads] * factor)
    thin[:, 2 * heads : 2 * heads + 1] = factor
    pull.wait()
    low = first_half()
    gain = w_ref[...]

    def block(i, carry):
        base = i * TALL
        tall = pl.ds(base, TALL)
        fetch(i).wait()
        put(i).start()
        scaling = thin[tall, 2 * heads : 2 * heads + 1]
        for n, dst in enumerate((qf, kf, vf, zf)):
            load_heads(heads, parts.at[n, tall], dst, scaling)
        for pair in range(SB // 2):
            for h in range(heads):
                at = tile(h, pair)
                lhs = jnp.concatenate([kf[at, :], qf[at, :]], axis=0).astype(bf16)
                r0 = jnp.dot(lhs, held[i * SB + 2 * pair, h].astype(bf16), preferred_element_type=f32)
                r1 = jnp.dot(lhs, held[i * SB + 2 * pair + 1, h].astype(bf16), preferred_element_type=f32)
                rk[at, :] = jnp.where(low, r0[:8], r1[:8])
                rq[at, :] = jnp.where(low, r0[8:], r1[8:])
        for h in range(heads):
            scale = jnp.ones((SB, 1), f32)
            ks, us, norms = [], [], []
            for p in range(P_SIZE):
                at = proposal(h, p)
                scalars = thin[pl.ds(base + p, SB, stride=P_SIZE), :]
                key = kf[at, :]
                query = qf[at, :]
                norm = lax.rsqrt(lane_dot(key, key) + epsilon)
                qnorm = lax.rsqrt(lane_dot(query, query) + epsilon) * DK ** (-0.5)
                g = scalars[:, h : h + 1]
                rec = (scale * norm) * rk[at, :]
                for ki, ui, ni in zip(ks, us, norms):
                    rec = rec + (lane_dot(ki, key) * (ni * norm)) * ui
                us = [ui * g for ui in us]
                scale = scale * g
                us.append(scalars[:, heads + h : heads + h + 1] * (vf[at, :] - g * rec))
                ks.append(key)
                norms.append(norm)
                att = (scale * qnorm) * rq[at, :]
                for ki, ui, ni in zip(ks, us, norms):
                    att = att + (lane_dot(ki, query) * (ni * qnorm)) * ui
                gate = zf[at, :]
                mean = jnp.sum(att * att, axis=-1, keepdims=True) / DK
                of[at, :] = att * lax.rsqrt(mean + epsilon) * gain * (gate * jax.nn.sigmoid(gate))
        for h in range(heads):
            o_ref[tall, h * DK : (h + 1) * DK] = of[pl.ds(h * TALL, TALL), :].astype(bf16)
        return carry

    lax.fori_loop(0, blocks, block, 0)
    for i in range(blocks):
        put(i).wait()


def accepted(state, keys, values, few):
    seqs, heads = state.shape[:2]
    width = heads * DK
    rows = TALL
    tall = pl.BlockSpec((rows, width), lambda i: (i, 0))
    thin = pl.BlockSpec((SB, few.shape[1]), lambda i: (i, 0))
    block = pl.BlockSpec((SB, heads, DK, DK), lambda i: (i, 0, 0, 0))
    return pl.pallas_call(
        functools.partial(accepted_kernel, heads),
        grid=(seqs // SB,),
        in_specs=[block, tall, tall, thin],
        out_specs=block,
        out_shape=jax.ShapeDtypeStruct(state.shape, f32),
        scratch_shapes=[pltpu.VMEM((heads * n, DK), f32) for n in (TALL, TALL, SB, TALL, TALL)],
        cost_estimate=pl.CostEstimate(flops=10_000_000_000, bytes_accessed=2 * state.size * 4, transcendentals=0),
        name="accepted",
    )(state, keys, values, few)


def attend(features, state, parts, few, extra, rates, offset, gain):
    seqs, heads = state.shape[:2]
    rows, width = parts.shape[1:]
    blocks = seqs // SB
    vmem, hbm = pl.BlockSpec(memory_space=pltpu.VMEM), pl.BlockSpec(memory_space=pl.ANY)
    dma = pltpu.SemaphoreType.DMA
    return pl.pallas_call(
        functools.partial(attend_kernel, heads, features),
        in_specs=[vmem] * 5 + [hbm] * 2,
        out_specs=[vmem, hbm],
        out_shape=[jax.ShapeDtypeStruct((rows, width), bf16), jax.ShapeDtypeStruct(state.shape, f32)],
        scratch_shapes=[
            pltpu.VMEM(state.shape, f32),
            pltpu.VMEM(parts.shape, f32),
            pltpu.VMEM((rows, 2 * heads + 8), f32),
            *[pltpu.VMEM((heads * TALL, DK), f32)] * 7,
            dma((blocks,)), dma((blocks,)), dma,
        ],
        compiler_params=pltpu.CompilerParams(vmem_limit_bytes=40 * 2**20),
        cost_estimate=pl.CostEstimate(flops=5_000_000_000, bytes_accessed=state.size * 4, transcendentals=0),
        name="attend",
    )(few, extra, rates.reshape(1, heads), offset.reshape(1, heads), gain.reshape(1, DK), parts, state)


def pick(index, values):
    chosen = values[-1]
    for at, value in enumerate(values[:-1]):
        chosen = jnp.where(index == at, value, chosen)
    return chosen


def turned_slot(t):
    return pick(t, (0, 2, 1, 3))


def project_kernel(x_hbm, gain_hbm, keys_hbm, values_hbm, fade_hbm, pull_hbm, count_hbm, wf, ws, wq, wk, wv, wz, wo,
                   state, acc_out, few_ref, taken, f_out,
                   x_ref, gain_ref, keys, values, fade, pull, counts, fs, thin,
                   xpre, xbuf, gbuf, w, fbuf, acc, sbuf, abuf, bbuf, cbuf, esend, erecv, s_in, s_out,
                   r_scr, u_scr, c_scr, kf, vf,
                   lsem, xs, xp, xr, wsem, ss, ar, br, cr, es, er, ins, outs, fsem, fss, fzr, fys, fyr, fos, aos):
    k, t, g = lax.axis_index("kv"), lax.axis_index("tp"), lax.axis_index("grp")
    depth, width = w.shape[1], w.shape[2]
    rows = x_ref.shape[0]
    blocks = state.shape[0] // SB
    heads = state.shape[1]

    def remote(src, dst, send, recv, kv, tp, grp=g):
        return pltpu.make_async_remote_copy(
            src, dst, send, recv, device_id={"grp": grp, "kv": kv, "tp": tp}, device_id_type=pl.DeviceIdType.MESH
        )

    here = pl.ds(k * depth, depth)
    locals_ = [
        pltpu.make_async_copy(src, dst, lsem.at[n])
        for n, (src, dst) in enumerate(
            (
                (x_hbm, x_ref), (gain_hbm, gain_ref), (keys_hbm, keys), (values_hbm, values), (fade_hbm, fade),
                (pull_hbm, pull), (count_hbm, counts), (wf.at[:, here], fs.at[0]), (ws.at[:, here], fs.at[1]),
            )
        )
    ]
    for load in locals_:
        load.start()
    f_load = pltpu.make_async_copy(wo, fbuf.at[k], fsem)
    f_load.start()
    loads = [pltpu.make_async_copy(src, w.at[i], wsem.at[i]) for i, src in enumerate((wq, wk, wv, wz))]
    for load in loads:
        load.start()

    def fetch(i):
        return pltpu.make_async_copy(state.at[pl.ds(i * SB, SB)], s_in.at[i % 2], ins.at[i % 2])

    def put(i):
        return pltpu.make_async_copy(s_out.at[i % 2], taken.at[pl.ds(i * SB, SB)], outs.at[i % 2])

    fetch(0).start()

    beside = t + 1 - 2 * (t % 2)
    across = (t + 2) % 4
    corner = t % 2
    landing = 2 * (t // 2) + k % 2
    home = corner == k % 2
    top_kind = t // 2 == k // 2
    source = jnp.where(top_kind, k, (k + 2) % 4)
    near_src = jnp.where(k <= 1, corner, corner + 2)
    far_src = jnp.where(k <= 1, corner + 2, corner)
    barrier = pltpu.get_barrier_semaphore()

    def greet(kv, tp, grp=g):
        pl.semaphore_signal(
            barrier, inc=1, device_id={"grp": grp, "kv": kv, "tp": tp}, device_id_type=pl.DeviceIdType.MESH
        )

    greet(k, beside)
    greet(k, across)
    greet(k, t, 1 - g)
    for step in range(1, 4):
        greet((k + step) % 4, t)

    @pl.when(t != k)
    def _():
        greet(t, landing)

    @pl.when(across != k)
    def _():
        greet(across, landing)

    @pl.when(near_src != k)
    def _():
        greet(near_src, source)

    @pl.when(far_src != k)
    def _():
        greet(far_src, source)

    @pl.when(home)
    def _():
        pl.semaphore_wait(barrier, 8)

    @pl.when(jnp.logical_not(home))
    def _():
        pl.semaphore_wait(barrier, 10)

    half_tall = rows // 2
    top, bottom = pl.ds(0, half_tall), pl.ds(half_tall, half_tall)
    locals_[0].wait()

    @pl.when(t == k)
    def _():
        remote(x_ref.at[bottom], xbuf.at[k, bottom], xs.at[0], xr.at[k, 1], k, across).start()
        pltpu.make_async_copy(x_ref.at[top], xbuf.at[k, top], xr.at[k, 0]).start()

    @pl.when(t != k)
    def _():
        remote(x_ref.at[bottom], xpre, xs.at[0], xp, k, across).start()
        remote(x_ref.at[top], xbuf.at[k, top], xs.at[1], xr.at[k, 0], t, landing).start()

    @pl.when(across != k)
    def _():
        remote(xpre, xpre, xs.at[0], xp, k, across).wait_recv()
        remote(xpre, xbuf.at[k, bottom], xs.at[2], xr.at[k, 1], across, landing).start()

    kind = jnp.where(top_kind, 0, 1)
    direct = pl.ds(kind * half_tall, half_tall)
    crossed = pl.ds((1 - kind) * half_tall, half_tall)

    def piece(r, at, send, kd, tp):
        return remote(xbuf.at[r, at], xbuf.at[r, at], xs.at[send], xr.at[r, kd], k, tp)

    def spread(r, n):
        settled = jnp.logical_and(t == k, r == k)

        @pl.when(settled)
        def _():
            pltpu.make_async_copy(x_ref.at[top], xbuf.at[k, top], xr.at[k, 0]).wait()

        @pl.when(jnp.logical_not(settled))
        def _():
            piece(r, direct, 3, kind, across).wait_recv()

        piece(r, direct, 3 + n, kind, across).start()
        piece(r, direct, 5 + n, kind, beside).start()

    half_rows = fbuf.shape[1] // 2
    half = pl.ds(g * half_rows, half_rows)

    def f_pass(c, to, sem):
        return remote(fbuf.at[c, half], fbuf.at[c, half], fss.at[sem], fzr.at[c], to, t)

    def f_swap(c):
        return remote(fbuf.at[c, half], fbuf.at[c, half], fys.at[c], fyr.at[c], k, t, 1 - g)

    spread(near_src, 0)
    f_load.wait()

    @pl.when(k < 3)
    def _():
        f_pass(k, k + 1, 4).start()

    @pl.when(k > 0)
    def _():
        f_pass(k, k - 1, 5).start()

    spread(far_src, 1)
    for n, r in enumerate((near_src, far_src)):
        piece(r, crossed, 3, 1 - kind, across).wait_recv()
        piece(r, crossed, 7 + n, 1 - kind, beside).start()

    def f_forwards(c):
        return jnp.logical_or(jnp.logical_and(c < k, k < 3), jnp.logical_and(c > k, k > 0))

    def f_take(c):
        to = jnp.where(c < k, k + 1, k - 1)
        f_pass(c, k, c).wait_recv()

        @pl.when(f_forwards(c))
        def _():
            f_pass(c, to, c).start()

        f_swap(c).start()

    end = jnp.where(k <= 1, 0, 3)
    near = jnp.where(k <= 1, 1, 2)
    is_end = k == end
    inside = jnp.logical_not(is_end)
    f_order = (jnp.where(is_end, near, end), 3 - near, 3 - end)

    for load in locals_[1:]:
        load.wait()
    thin[...] = rows_to_columns(
        jnp.concatenate([fade[...], pull[...], jnp.broadcast_to(counts[...].astype(f32), (8, counts.shape[1]))], axis=0)
    )
    for load in loads:
        load.wait()
    for r in (1 - corner, 3 - corner):
        for kd in range(2):
            piece(r, pl.ds(kd * half_tall, half_tall), 3, kd, beside).wait_recv()

    nt = (((1,), (1,)), ((), ()))

    def prepare(r):
        floated = xbuf[r].astype(f32)
        gained = (floated * gain_ref[k]).astype(bf16)
        gbuf[r] = gained
        squares = floated * floated
        high = squares.astype(bf16)
        rest = (squares - high.astype(f32)).astype(bf16)
        ones = jnp.ones((8, depth), bf16)
        for n in range(2):
            every = lax.dot_general(fs[n], gained, nt, preferred_element_type=f32)
            esend[r, n * heads : (n + 1) * heads, :] = pick(t, [every[m * heads : (m + 1) * heads] for m in range(4)])
        esend[r, 2 * heads :, :] = lax.dot_general(ones, high, nt, preferred_element_type=f32) + lax.dot_general(
            ones, rest, nt, preferred_element_type=f32
        )

        @pl.when(r != k)
        def _():
            remote(esend.at[r], erecv.at[k], es.at[r], er.at[k], r, t).start()

    def product(r, c):
        return jnp.dot(gbuf[r], w[c], preferred_element_type=f32)

    def from_end(i):
        remote(abuf.at[i], abuf.at[i], ss.at[i], ar.at[i], k, beside).wait_recv()
        return abuf[i].astype(f32)

    def from_inner(i):
        remote(bbuf.at[i], bbuf.at[i], ss.at[i], br.at[i], k, beside).wait_recv()
        return bbuf[i].astype(f32)

    def accept(i):
        @pl.when(i + 1 < blocks)
        def _():
            fetch(i + 1).start()

        fetch(i).wait()

        @pl.when(i >= 2)
        def _():
            put(i - 2).wait()

        tall, few_rows = pl.ds(i * TALL, TALL), pl.ds(i * SB, SB)
        accepted_kernel(
            heads, s_in.at[i % 2], keys.at[tall], values.at[tall], thin.at[few_rows], s_out.at[i % 2],
            r_scr, u_scr, c_scr, kf, vf,
        )
        put(i).start()

    def step(i, carry):
        stage, c = i // 4, i % 4
        r = pick(stage, (3 - end, 3 - near, near))

        @pl.when(c == 0)
        def _():
            prepare(r)

        @pl.when(i == 2)
        def _():
            prepare(end)

        @pl.when(is_end)
        def _():
            sbuf[i] = product(r, c).astype(bf16)
            remote(sbuf.at[i], abuf.at[i], ss.at[i], ar.at[i], near, t).start()

        @pl.when(jnp.logical_and(inside, i == 1))
        def _():
            f_take(f_order[0])
            f_take(f_order[1])

        @pl.when(jnp.logical_and(inside, i == 5))
        def _():
            f_take(f_order[2])

        @pl.when(jnp.logical_and(is_end, i == 4))
        def _():
            f_take(f_order[0])

        @pl.when(jnp.logical_and(inside, i < 8))
        def _():
            part = product(r, c)
            sbuf[i] = (part + from_end(i)).astype(bf16)
            remote(sbuf.at[i], bbuf.at[i], ss.at[i], br.at[i], 3 - near, t).start()

        @pl.when(jnp.logical_and(inside, stage == 1))
        def _():
            part = product(end, c)
            sbuf[8 + c] = (part + from_inner(c)).astype(bf16)
            remote(sbuf.at[8 + c], cbuf.at[c], ss.at[8 + c], cr.at[c], end, t).start()

        @pl.when(jnp.logical_and(inside, stage == 2))
        def _():
            acc[c] = product(r, c) + from_inner(4 + c) + from_end(i)
            pltpu.make_async_copy(acc.at[c], acc_out.at[c], aos.at[c]).start()

        @pl.when(i % 2 == 0)
        def _():
            accept(i // 2)

        return carry

    lax.fori_loop(0, 12, step, 0)
    for i in range(max(blocks - 2, 0), blocks):
        put(i).wait()

    @pl.when(is_end)
    def _():
        f_take(f_order[1])

        def finish(c, carry):
            part = product(end, c)

            @pl.when(c == 1)
            def _():
                f_take(f_order[2])

            remote(cbuf.at[c], cbuf.at[c], ss.at[c], cr.at[c], k, beside).wait_recv()
            acc[c] = part + cbuf[c].astype(f32)
            pltpu.make_async_copy(acc.at[c], acc_out.at[c], aos.at[c]).start()
            return carry

        lax.fori_loop(0, 4, finish, 0)

    few_ref[...] = esend[k]
    for src in range(4):

        @pl.when(k != src)
        def _():
            remote(esend.at[src], erecv.at[src], es.at[src], er.at[src], k, beside).wait()
            few_ref[...] += erecv[src]
            remote(fbuf.at[src, half], fbuf.at[src, half], fys.at[src], fyr.at[src], k, beside).wait()

        pltpu.make_async_copy(fbuf.at[src], f_out.at[src], fos.at[src]).start()

    remote(x_ref.at[bottom], xpre, xs.at[0], xp, k, across).wait_send()

    @pl.when(t != k)
    def _():
        remote(x_ref.at[top], xbuf.at[k, top], xs.at[1], xr.at[k, 0], t, landing).wait_send()

    @pl.when(across != k)
    def _():
        remote(xpre, xbuf.at[k, bottom], xs.at[2], xr.at[k, 1], across, landing).wait_send()

    for n in range(6):
        piece(k, top, 3 + n, 0, beside).wait_send()

    @pl.when(k < 3)
    def _():
        f_pass(k, k, 4).wait_send()

    @pl.when(k > 0)
    def _():
        f_pass(k, k, 5).wait_send()

    for src in range(4):

        @pl.when(jnp.logical_and(k != src, f_forwards(src)))
        def _():
            f_pass(src, k, src).wait_send()

    for i in range(12):
        remote(sbuf.at[i], abuf.at[i], ss.at[i], ar.at[i], k, beside).wait_send()
    for src in range(4):
        pltpu.make_async_copy(fbuf.at[src], f_out.at[src], fos.at[src]).wait()
        pltpu.make_async_copy(acc.at[src], acc_out.at[src], aos.at[src]).wait()


def project(x, gain, weights, forgetting, strength, final, state, keys, values, fade, pull, counts):
    rows, depth = x.shape
    width = weights[0].shape[1]
    seqs, heads = state.shape[:2]
    few_rows = 2 * heads + 8
    vmem, hbm = pl.BlockSpec(memory_space=pltpu.VMEM), pl.BlockSpec(memory_space=pl.ANY)
    dma = pltpu.SemaphoreType.DMA
    gain = gain.reshape(-1, 1, depth)
    forgetting, strength = forgetting.T, strength.T

    def chunks(n):
        return pltpu.VMEM((n, rows, width), bf16)

    def like(a):
        return pltpu.VMEM(a.shape, a.dtype)

    return pl.pallas_call(
        project_kernel,
        in_specs=[hbm] * 15,
        out_specs=[hbm, vmem, hbm, hbm],
        out_shape=[
            jax.ShapeDtypeStruct((4, rows, width), f32),
            jax.ShapeDtypeStruct((few_rows, rows), f32),
            jax.ShapeDtypeStruct(state.shape, f32),
            jax.ShapeDtypeStruct((4,) + final.shape, bf16),
        ],
        scratch_shapes=[
            like(x), like(gain), like(keys), like(values), like(fade), like(pull), like(counts),
            pltpu.VMEM((2, forgetting.shape[0], depth), bf16),
            pltpu.VMEM((seqs, 2 * P_SIZE * heads + 8), f32),
            pltpu.VMEM((rows // 2, depth), bf16),
            pltpu.VMEM((4, rows, depth), bf16),
            pltpu.VMEM((4, rows, depth), bf16),
            pltpu.VMEM((4, depth, width), bf16),
            pltpu.VMEM((4,) + final.shape, bf16),
            pltpu.VMEM((4, rows, width), f32),
            chunks(12), chunks(12), chunks(8), chunks(4),
            pltpu.VMEM((4, few_rows, rows), f32),
            pltpu.VMEM((4, few_rows, rows), f32),
            pltpu.VMEM((2, SB) + state.shape[1:], f32),
            pltpu.VMEM((2, SB) + state.shape[1:], f32),
            *[pltpu.VMEM((heads * n, DK), f32) for n in (TALL, TALL, SB, TALL, TALL)],
            dma((9,)), dma((9,)), dma, dma((4, 2)), dma((4,)), dma((12,)), dma((12,)), dma((8,)), dma((4,)), dma((4,)),
            dma((4,)), dma((2,)), dma((2,)), dma, dma((6,)), dma((4,)), dma((4,)), dma((4,)), dma((4,)), dma((4,)),
        ],
        compiler_params=pltpu.CompilerParams(has_side_effects=True, collective_id=0, vmem_limit_bytes=56 * 2**20),
        name="project",
    )(x, gain, keys, values, fade, pull, counts, forgetting, strength, *weights, final, state)


PIECES = 3


def mix_kernel(flat_ref, f_hbm, o_ref, w, part, mate, cross, wsem, ms, mr, xs, xr):
    k, t, g = lax.axis_index("kv"), lax.axis_index("tp"), lax.axis_index("grp")
    rows = flat_ref.shape[0]
    piece = rows // PIECES
    beside = t + 1 - 2 * (t % 2)
    across = (t + 2) % 4
    order = ((beside + 2) % 4, across, beside, t)

    def remote(src, dst, send, recv, tp):
        return pltpu.make_async_remote_copy(
            src, dst, send, recv, device_id={"grp": g, "kv": k, "tp": tp}, device_id_type=pl.DeviceIdType.MESH
        )

    loads = [pltpu.make_async_copy(f_hbm.at[c], w.at[n], wsem.at[n]) for n, c in enumerate(order)]
    for load in loads:
        load.start()
    barrier = pltpu.get_barrier_semaphore()
    for peer in (beside, across):
        pl.semaphore_signal(
            barrier, inc=1, device_id={"grp": g, "kv": k, "tp": peer}, device_id_type=pl.DeviceIdType.MESH
        )
    pl.semaphore_wait(barrier, 2)

    def to_mate(n, s):
        at = pl.ds(s * piece, piece)
        return remote(part.at[2 * n, at], mate.at[n, at], ms.at[n, s], mr.at[n, s], beside)

    def to_cross(s):
        at = pl.ds(s * piece, piece)
        return remote(part.at[1, at], cross.at[at], xs.at[s], xr.at[s], across)

    def fill(n, s):
        at = pl.ds(s * piece, piece)
        return jnp.dot(flat_ref[at, :], w[n], preferred_element_type=f32).astype(bf16)

    loads[0].wait()
    for s in range(PIECES):
        part[0, s * piece : (s + 1) * piece, :] = fill(0, s)
        to_mate(0, s).start()
    loads[1].wait()
    for s in range(PIECES):
        at = slice(s * piece, (s + 1) * piece)
        mine = fill(1, s).astype(f32)
        to_mate(0, s).wait_recv()
        part[1, at, :] = (mine + mate[0, at, :].astype(f32)).astype(bf16)
        to_cross(s).start()
    loads[2].wait()
    for s in range(PIECES):
        part[2, s * piece : (s + 1) * piece, :] = fill(2, s)
        to_mate(1, s).start()
    loads[3].wait()
    for s in range(PIECES):
        part[3, s * piece : (s + 1) * piece, :] = fill(3, s)
    for s in range(PIECES):
        at = slice(s * piece, (s + 1) * piece)
        to_mate(1, s).wait_recv()
        to_cross(s).wait_recv()
        o_ref[at, :] = (
            part[3, at, :].astype(f32) + mate[1, at, :].astype(f32) + cross[at, :].astype(f32)
        ).astype(bf16)
    for s in range(PIECES):
        to_mate(0, s).wait_send()
        to_mate(1, s).wait_send()
        to_cross(s).wait_send()


def mix(flat, final):
    rows, width = flat.shape
    cols = final.shape[2]
    vmem, hbm = pl.BlockSpec(memory_space=pltpu.VMEM), pl.BlockSpec(memory_space=pl.ANY)
    dma = pltpu.SemaphoreType.DMA
    return pl.pallas_call(
        mix_kernel,
        in_specs=[vmem, hbm],
        out_specs=vmem,
        out_shape=jax.ShapeDtypeStruct((rows, cols), bf16),
        scratch_shapes=[
            pltpu.VMEM((4, width, cols), bf16),
            pltpu.VMEM((4, rows, cols), bf16),
            pltpu.VMEM((2, rows, cols), bf16),
            pltpu.VMEM((rows, cols), bf16),
            dma((4,)), dma((2, PIECES)), dma((2, PIECES)), dma((PIECES,)), dma((PIECES,)),
        ],
        compiler_params=pltpu.CompilerParams(has_side_effects=True, collective_id=1, vmem_limit_bytes=56 * 2**20),
        name="mix",
    )(flat, final)


def on_device(
    n_kv,
    n_tp,
    candidate_embeddings,
    incoming_rms_scaling,
    probe_projector,
    address_projector,
    content_projector,
    sigmoid_mask_matrix,
    forgetting_projector,
    strength_projector_matrix,
    channel_forgetting_rates,
    forgetting_offset,
    extra_forgetting,
    outgoing_rms_scaling,
    final_projector,
    memory_matrix,
    earlier_addresses,
    earlier_contents,
    earlier_strengths,
    earlier_forgetting,
    admitted_counts,
):
    rows, local_cols = candidate_embeddings.shape
    features = incoming_rms_scaling.shape[0]
    depth, width = probe_projector.shape
    heads = width // DK
    seqs = rows // P_SIZE
    k_index, t_index = lax.axis_index("kv"), lax.axis_index("tp")

    def thin(values):
        return values.transpose(1, 2, 0).reshape(P_SIZE * heads, seqs)

    weights = (probe_projector, address_projector, content_projector, sigmoid_mask_matrix)
    fade, pull, extra = thin(earlier_forgetting), thin(earlier_strengths), thin(extra_forgetting)
    earlier = (memory_matrix, earlier_addresses.reshape(rows, width), earlier_contents.reshape(rows, width))
    if n_kv == 4 and n_tp == 4:
        summed, few, taken, columns = project(
            candidate_embeddings, incoming_rms_scaling, weights, forgetting_projector, strength_projector_matrix,
            final_projector, *earlier, fade, pull, admitted_counts.reshape(1, seqs),
        )
    else:
        every = lax.all_gather(candidate_embeddings, "tp", axis=1, tiled=True)
        every = lax.all_to_all(every, "kv", split_axis=1, concat_axis=0, tiled=True)
        gain_part = lax.dynamic_slice_in_dim(incoming_rms_scaling, k_index * depth, depth)
        floated = every.astype(f32)
        gained = (floated * gain_part).astype(bf16)
        decay_cols = lax.dynamic_slice(forgetting_projector, (k_index * depth, t_index * heads), (depth, heads))
        beta_cols = lax.dynamic_slice(strength_projector_matrix, (k_index * depth, t_index * heads), (depth, heads))
        few = jnp.concatenate(
            [
                jnp.dot(gained, jnp.concatenate([decay_cols, beta_cols], axis=1), preferred_element_type=f32),
                jnp.sum(floated * floated, axis=1, keepdims=True),
            ],
            axis=1,
        )
        few = lax.psum_scatter(few, "kv", scatter_dimension=0, tiled=True)
        few = jnp.pad(few, ((0, 0), (0, 7))).T
        partial = jnp.stack([jnp.dot(gained, w, preferred_element_type=f32).astype(bf16) for w in weights])
        summed = lax.psum_scatter(partial, "kv", scatter_dimension=1, tiled=True).astype(f32)
        counts = admitted_counts.astype(f32).reshape(seqs, 1)
        taken = accepted(*earlier, jnp.concatenate([fade.T, pull.T, counts], axis=1))
    flat, taken = attend(
        features, taken, summed, few, extra, channel_forgetting_rates, forgetting_offset, outgoing_rms_scaling
    )
    if n_kv == 4 and n_tp == 4:
        mixed = mix(flat, columns)
    else:
        gathered = lax.all_gather(flat, "kv", axis=0, tiled=True)
        terms = jnp.dot(gathered, final_projector, preferred_element_type=f32).astype(bf16)
        terms = lax.all_to_all(terms, "kv", split_axis=0, concat_axis=1, tiled=True)
        mixed = lax.psum_scatter(terms, "tp", scatter_dimension=1, tiled=True)
    return (mixed, taken)


def solution(mesh):
    row, per_head = P(("grp", "kv"), "tp"), P(("grp", "kv"), None, "tp")
    four = P(("grp", "kv"), None, "tp", None)
    weight = P("kv", "tp")
    state = P(("grp", "kv"), "tp", None, None)
    in_specs = (
        row, P(), weight, weight, weight, weight, P(), P(), P("tp"), P("tp"), per_head, P(),
        P("tp", "kv"), state, four, four, per_head, per_head, P(("grp", "kv")),
    )
    body = functools.partial(on_device, mesh.shape["kv"], mesh.shape["tp"])
    return jax.shard_map(body, mesh=mesh, in_specs=in_specs, out_specs=(row, state), check_vma=False)
```

```python
import functools

import jax
import jax.numpy as jnp
from jax import lax
from jax.experimental import pallas as pl
from jax.experimental.pallas import tpu as pltpu
from jax.sharding import PartitionSpec as P

DK = 128
P_SIZE = 4
SB = 8
TALL = SB * P_SIZE
epsilon = 1e-06
LIMIT = 42 * 2**20
f32 = jnp.float32
bf16 = jnp.bfloat16


def lane_dot(a, b):
    return jnp.sum(a * b, axis=-1, keepdims=True)


def first_half():
    return lax.broadcasted_iota(jnp.int32, (8, DK), 0) < P_SIZE


def load_heads(heads, src, dst, factor=None):
    for h in range(heads):
        part = src[:, h * DK : (h + 1) * DK].astype(f32)
        dst[pl.ds(h * TALL, TALL), :] = part if factor is None else (part * factor).astype(bf16).astype(f32)


def tile(h, pair):
    return pl.ds(h * TALL + pair * 8, 8)


def proposal(h, p):
    return pl.ds(h * TALL + p, SB, stride=P_SIZE)


def rows_to_columns(wide):
    count = wide.shape[1]
    same = lax.broadcasted_iota(jnp.int32, (count, count), 0) == lax.broadcasted_iota(jnp.int32, (count, count), 1)
    return lax.dot_general(
        same.astype(f32), wide, (((1,), (1,)), ((), ())),
        precision=lax.Precision.HIGHEST, preferred_element_type=f32,
    )


def accepted_kernel(heads, s_ref, k_ref, v_ref, n_ref, o_ref, r_scr, u_scr, c_scr, kf, vf):
    load_heads(heads, k_ref, kf)
    load_heads(heads, v_ref, vf)
    low = first_half()
    for pair in range(SB // 2):
        for h in range(heads):
            at = tile(h, pair)
            lhs = kf[at, :].astype(bf16)
            r0 = jnp.dot(lhs, s_ref[2 * pair, h].astype(bf16), preferred_element_type=f32)
            r1 = jnp.dot(lhs, s_ref[2 * pair + 1, h].astype(bf16), preferred_element_type=f32)
            r_scr[at, :] = jnp.where(low, r0, r1)
    few = n_ref[...]
    span = P_SIZE * heads
    count = few[:, 2 * span : 2 * span + 1]
    for h in range(heads):
        scale = jnp.ones((SB, 1), f32)
        ks, us, norms = [], [], []
        for p in range(P_SIZE):
            at = proposal(h, p)
            col = slice(p * heads + h, p * heads + h + 1)
            key = kf[at, :]
            norm = lax.rsqrt(lane_dot(key, key) + epsilon)
            live = count > float(p)
            g = jnp.where(live, jnp.exp(few[:, p * heads + h : p * heads + h + 1]), 1.0)
            b = jnp.where(live, few[:, span + p * heads + h : span + p * heads + h + 1], 0.0)
            rec = (scale * norm) * r_scr[at, :]
            for ki, ui, ni in zip(ks, us, norms):
                rec = rec + (lane_dot(ki, key) * (ni * norm)) * ui
            us = [ui * g for ui in us]
            scale = scale * g
            us.append(b * (vf[at, :] - g * rec))
            ks.append(key)
            norms.append(norm)
        for p in range(P_SIZE):
            u_scr[proposal(h, p), :] = us[p] * norms[p]
        c_scr[pl.ds(h * SB, SB), :] = jnp.broadcast_to(scale, (SB, DK))
    for pair in range(SB // 2):
        for h in range(heads):
            at = tile(h, pair)
            key = kf[at, :]
            lhs = jnp.concatenate([key, key], axis=0).astype(bf16)
            u = u_scr[at, :]
            hi = u.astype(bf16).astype(f32)
            lo = u - hi
            for half in range(2):
                keep = low if half == 0 else jnp.logical_not(low)
                rhs = jnp.concatenate([jnp.where(keep, hi, 0.0), jnp.where(keep, lo, 0.0)], axis=0).astype(bf16)
                seq = 2 * pair + half
                add = lax.dot_general(lhs, rhs, (((0,), (0,)), ((), ())), preferred_element_type=f32)
                o_ref[seq, h] = c_scr[pl.ds(h * SB + seq, 1), :] * s_ref[seq, h] + add


def attend_kernel(heads, features, few_ref, extra_ref, rate_ref, offset_ref, w_ref, parts, state, o_ref, kept, thin, rk, rq, qf, kf, vf, zf, of, done):
    keep = pltpu.make_async_copy(state, kept, done)
    keep.start()
    rows = o_ref.shape[0]
    blocks = state.shape[0] // SB
    few = rows_to_columns(few_ref[...])
    factor = lax.rsqrt(few[:, 2 * heads : 2 * heads + 1] / features + epsilon)
    seqs = extra_ref.shape[1]
    row = lax.broadcasted_iota(jnp.int32, (rows, seqs), 0)
    owner = jnp.right_shift(row, 2) == lax.broadcasted_iota(jnp.int32, (rows, seqs), 1)
    spread = lax.dot_general(
        owner.astype(f32), extra_ref[...], (((1,), (1,)), ((), ())),
        precision=lax.Precision.HIGHEST, preferred_element_type=f32,
    )
    turn = jnp.bitwise_and(lax.broadcasted_iota(jnp.int32, (rows, heads), 0), 3)
    extra = pick(turn, [spread[:, p * heads : (p + 1) * heads] for p in range(P_SIZE)])
    raised = few[:, :heads] * factor + offset_ref[...]
    soft = jnp.maximum(raised, 0.0) + jnp.log1p(jnp.exp(-jnp.abs(raised)))
    thin[:, :heads] = jnp.exp(extra - jnp.exp(rate_ref[...]) * soft)
    thin[:, heads : 2 * heads] = jax.nn.sigmoid(few[:, heads : 2 * heads] * factor)
    thin[:, 2 * heads : 2 * heads + 1] = factor
    low = first_half()
    gain = w_ref[...]

    def block(i, carry):
        base = i * TALL
        tall = pl.ds(base, TALL)
        scaling = thin[tall, 2 * heads : 2 * heads + 1]
        for n, dst in enumerate((qf, kf, vf, zf)):
            load_heads(heads, parts.at[n, tall], dst, scaling)
        for pair in range(SB // 2):
            for h in range(heads):
                at = tile(h, pair)
                lhs = jnp.concatenate([kf[at, :], qf[at, :]], axis=0).astype(bf16)
                r0 = jnp.dot(lhs, state[i * SB + 2 * pair, h].astype(bf16), preferred_element_type=f32)
                r1 = jnp.dot(lhs, state[i * SB + 2 * pair + 1, h].astype(bf16), preferred_element_type=f32)
                rk[at, :] = jnp.where(low, r0[:8], r1[:8])
                rq[at, :] = jnp.where(low, r0[8:], r1[8:])
        for h in range(heads):
            scale = jnp.ones((SB, 1), f32)
            ks, us, norms = [], [], []
            for p in range(P_SIZE):
                at = proposal(h, p)
                scalars = thin[pl.ds(base + p, SB, stride=P_SIZE), :]
                key = kf[at, :]
                query = qf[at, :]
                norm = lax.rsqrt(lane_dot(key, key) + epsilon)
                qnorm = lax.rsqrt(lane_dot(query, query) + epsilon) * DK ** (-0.5)
                g = scalars[:, h : h + 1]
                rec = (scale * norm) * rk[at, :]
                for ki, ui, ni in zip(ks, us, norms):
                    rec = rec + (lane_dot(ki, key) * (ni * norm)) * ui
                us = [ui * g for ui in us]
                scale = scale * g
                us.append(scalars[:, heads + h : heads + h + 1] * (vf[at, :] - g * rec))
                ks.append(key)
                norms.append(norm)
                att = (scale * qnorm) * rq[at, :]
                for ki, ui, ni in zip(ks, us, norms):
                    att = att + (lane_dot(ki, query) * (ni * qnorm)) * ui
                gate = zf[at, :]
                mean = jnp.sum(att * att, axis=-1, keepdims=True) / DK
                of[at, :] = att * lax.rsqrt(mean + epsilon) * gain * (gate * jax.nn.sigmoid(gate))
        for h in range(heads):
            o_ref[tall, h * DK : (h + 1) * DK] = of[pl.ds(h * TALL, TALL), :].astype(bf16)
        return carry

    lax.fori_loop(0, blocks, block, 0)
    keep.wait()


def accepted(state, keys, values, few):
    seqs, heads = state.shape[:2]
    width = heads * DK
    rows = TALL
    tall = pl.BlockSpec((rows, width), lambda i: (i, 0))
    thin = pl.BlockSpec((SB, few.shape[1]), lambda i: (i, 0))
    block = pl.BlockSpec((SB, heads, DK, DK), lambda i: (i, 0, 0, 0))
    return pl.pallas_call(
        functools.partial(accepted_kernel, heads),
        grid=(seqs // SB,),
        in_specs=[block, tall, tall, thin],
        out_specs=block,
        out_shape=jax.ShapeDtypeStruct(state.shape, f32),
        scratch_shapes=[pltpu.VMEM((heads * n, DK), f32) for n in (TALL, TALL, SB, TALL, TALL)],
        cost_estimate=pl.CostEstimate(flops=10_000_000_000, bytes_accessed=2 * state.size * 4, transcendentals=0),
        name="accepted",
    )(state, keys, values, few)


def local(array):
    return pltpu.with_memory_space_constraint(array, pltpu.VMEM)


def attend(features, state, parts, few, extra, rates, offset, gain):
    seqs, heads = state.shape[:2]
    rows, width = parts.shape[1:]
    vmem = pl.BlockSpec(memory_space=pltpu.VMEM)
    return pl.pallas_call(
        functools.partial(attend_kernel, heads, features),
        in_specs=[vmem] * 7,
        out_specs=[vmem, pl.BlockSpec(memory_space=pl.ANY)],
        out_shape=[pltpu.VMEM((rows, width), bf16), jax.ShapeDtypeStruct(state.shape, f32)],
        scratch_shapes=[
            pltpu.VMEM((rows, 2 * heads + 8), f32),
            *[pltpu.VMEM((heads * TALL, DK), f32)] * 7,
            pltpu.SemaphoreType.DMA,
        ],
        compiler_params=pltpu.CompilerParams(vmem_limit_bytes=LIMIT),
        cost_estimate=pl.CostEstimate(flops=5_000_000_000, bytes_accessed=state.size * 4, transcendentals=0),
        name="attend",
    )(
        local(few), extra, rates.reshape(1, heads), offset.reshape(1, heads), gain.reshape(1, DK),
        local(parts), local(state),
    )


def pick(index, values):
    chosen = values[-1]
    for at, value in enumerate(values[:-1]):
        chosen = jnp.where(index == at, value, chosen)
    return chosen


def turned_slot(t):
    return pick(t, (0, 2, 1, 3))


def project_kernel(x_hbm, gain_hbm, keys_hbm, values_hbm, fade_hbm, pull_hbm, count_hbm, wf, ws, wq, wk, wv, wz, wo,
                   state, acc, few_ref, taken, fbuf,
                   x_ref, gain_ref, keys, values, fade, pull, counts, fs, thin,
                   xpre, xbuf, gbuf, w, sbuf, abuf, bbuf, cbuf, esend, erecv, s_in,
                   r_scr, u_scr, c_scr, kf, vf,
                   lsem, xs, xp, xr, wsem, ss, ar, br, cr, es, er, ins, fsem, fss, fzr, fys, fyr):
    k, t, g = lax.axis_index("kv"), lax.axis_index("tp"), lax.axis_index("grp")
    depth, width = w.shape[1], w.shape[2]
    rows = x_ref.shape[0]
    blocks = state.shape[0] // SB
    heads = state.shape[1]

    def remote(src, dst, send, recv, kv, tp, grp=g):
        return pltpu.make_async_remote_copy(
            src, dst, send, recv, device_id={"grp": grp, "kv": kv, "tp": tp}, device_id_type=pl.DeviceIdType.MESH
        )

    here = pl.ds(k * depth, depth)
    locals_ = [
        pltpu.make_async_copy(src, dst, lsem.at[n])
        for n, (src, dst) in enumerate(
            (
                (x_hbm, x_ref), (gain_hbm, gain_ref), (keys_hbm, keys), (values_hbm, values), (fade_hbm, fade),
                (pull_hbm, pull), (count_hbm, counts), (wf.at[:, here], fs.at[0]), (ws.at[:, here], fs.at[1]),
            )
        )
    ]
    for load in locals_:
        load.start()
    f_load = pltpu.make_async_copy(wo, fbuf.at[k], fsem)
    f_load.start()
    loads = [pltpu.make_async_copy(src, w.at[i], wsem.at[i]) for i, src in enumerate((wq, wk, wv, wz))]
    for load in loads:
        load.start()

    def fetch(i):
        return pltpu.make_async_copy(state.at[pl.ds(i * SB, SB)], s_in.at[i % 2], ins.at[i % 2])

    fetch(0).start()

    beside = t + 1 - 2 * (t % 2)
    across = (t + 2) % 4
    corner = t % 2
    landing = 2 * (t // 2) + k % 2
    home = corner == k % 2
    top_kind = t // 2 == k // 2
    source = jnp.where(top_kind, k, (k + 2) % 4)
    near_src = jnp.where(k <= 1, corner, corner + 2)
    far_src = jnp.where(k <= 1, corner + 2, corner)
    barrier = pltpu.get_barrier_semaphore()

    def greet(kv, tp, grp=g):
        pl.semaphore_signal(
            barrier, inc=1, device_id={"grp": grp, "kv": kv, "tp": tp}, device_id_type=pl.DeviceIdType.MESH
        )

    greet(k, beside)
    greet(k, across)
    greet(k, t, 1 - g)
    for step in range(1, 4):
        greet((k + step) % 4, t)

    @pl.when(t != k)
    def _():
        greet(t, landing)

    @pl.when(across != k)
    def _():
        greet(across, landing)

    @pl.when(near_src != k)
    def _():
        greet(near_src, source)

    @pl.when(far_src != k)
    def _():
        greet(far_src, source)

    @pl.when(home)
    def _():
        pl.semaphore_wait(barrier, 8)

    @pl.when(jnp.logical_not(home))
    def _():
        pl.semaphore_wait(barrier, 10)

    half_tall = rows // 2
    top, bottom = pl.ds(0, half_tall), pl.ds(half_tall, half_tall)
    locals_[0].wait()

    @pl.when(t == k)
    def _():
        remote(x_ref.at[bottom], xbuf.at[k, bottom], xs.at[0], xr.at[k, 1], k, across).start()
        pltpu.make_async_copy(x_ref.at[top], xbuf.at[k, top], xr.at[k, 0]).start()

    @pl.when(t != k)
    def _():
        remote(x_ref.at[bottom], xpre, xs.at[0], xp, k, across).start()
        remote(x_ref.at[top], xbuf.at[k, top], xs.at[1], xr.at[k, 0], t, landing).start()

    @pl.when(across != k)
    def _():
        remote(xpre, xpre, xs.at[0], xp, k, across).wait_recv()
        remote(xpre, xbuf.at[k, bottom], xs.at[2], xr.at[k, 1], across, landing).start()

    kind = jnp.where(top_kind, 0, 1)
    direct = pl.ds(kind * half_tall, half_tall)
    crossed = pl.ds((1 - kind) * half_tall, half_tall)

    def piece(r, at, send, kd, tp):
        return remote(xbuf.at[r, at], xbuf.at[r, at], xs.at[send], xr.at[r, kd], k, tp)

    def spread(r, n):
        settled = jnp.logical_and(t == k, r == k)

        @pl.when(settled)
        def _():
            pltpu.make_async_copy(x_ref.at[top], xbuf.at[k, top], xr.at[k, 0]).wait()

        @pl.when(jnp.logical_not(settled))
        def _():
            piece(r, direct, 3, kind, across).wait_recv()

        piece(r, direct, 3 + n, kind, across).start()
        piece(r, direct, 5 + n, kind, beside).start()

    half_rows = fbuf.shape[1] // 2
    half = pl.ds(g * half_rows, half_rows)

    def f_pass(c, to, sem):
        return remote(fbuf.at[c, half], fbuf.at[c, half], fss.at[sem], fzr.at[c], to, t)

    def f_swap(c):
        return remote(fbuf.at[c, half], fbuf.at[c, half], fys.at[c], fyr.at[c], k, t, 1 - g)

    spread(near_src, 0)
    spread(far_src, 1)
    f_load.wait()

    @pl.when(k < 3)
    def _():
        f_pass(k, k + 1, 4).start()

    @pl.when(k > 0)
    def _():
        f_pass(k, k - 1, 5).start()

    for n, r in enumerate((near_src, far_src)):
        piece(r, crossed, 3, 1 - kind, across).wait_recv()
        piece(r, crossed, 7 + n, 1 - kind, beside).start()

    def f_forwards(c):
        return jnp.logical_or(jnp.logical_and(c < k, k < 3), jnp.logical_and(c > k, k > 0))

    def f_take(c):
        to = jnp.where(c < k, k + 1, k - 1)
        f_pass(c, k, c).wait_recv()

        @pl.when(f_forwards(c))
        def _():
            f_pass(c, to, c).start()

        f_swap(c).start()

    end = jnp.where(k <= 1, 0, 3)
    near = jnp.where(k <= 1, 1, 2)
    is_end = k == end
    inside = jnp.logical_not(is_end)
    f_order = (jnp.where(is_end, near, end), 3 - near, 3 - end)

    for load in locals_[1:]:
        load.wait()
    thin[...] = rows_to_columns(
        jnp.concatenate([fade[...], pull[...], jnp.broadcast_to(counts[...].astype(f32), (8, counts.shape[1]))], axis=0)
    )
    for load in loads:
        load.wait()
    for r in (1 - corner, 3 - corner):
        for kd in range(2):
            piece(r, pl.ds(kd * half_tall, half_tall), 3, kd, beside).wait_recv()

    nt = (((1,), (1,)), ((), ()))

    def prepare(r):
        floated = xbuf[r].astype(f32)
        gained = (floated * gain_ref[k]).astype(bf16)
        gbuf[r] = gained
        squares = floated * floated
        high = squares.astype(bf16)
        rest = (squares - high.astype(f32)).astype(bf16)
        ones = jnp.ones((8, depth), bf16)
        for n in range(2):
            every = lax.dot_general(fs[n], gained, nt, preferred_element_type=f32)
            esend[r, n * heads : (n + 1) * heads, :] = pick(t, [every[m * heads : (m + 1) * heads] for m in range(4)])
        esend[r, 2 * heads :, :] = lax.dot_general(ones, high, nt, preferred_element_type=f32) + lax.dot_general(
            ones, rest, nt, preferred_element_type=f32
        )

        @pl.when(r != k)
        def _():
            remote(esend.at[r], erecv.at[k], es.at[r], er.at[k], r, t).start()

    def product(r, c):
        return jnp.dot(gbuf[r], w[c], preferred_element_type=f32)

    def from_end(i):
        remote(abuf.at[i], abuf.at[i], ss.at[i], ar.at[i], k, beside).wait_recv()
        return abuf[i].astype(f32)

    def from_inner(i):
        remote(bbuf.at[i], bbuf.at[i], ss.at[i], br.at[i], k, beside).wait_recv()
        return bbuf[i].astype(f32)

    def accept(i):
        @pl.when(i + 1 < blocks)
        def _():
            fetch(i + 1).start()

        fetch(i).wait()

        tall, few_rows = pl.ds(i * TALL, TALL), pl.ds(i * SB, SB)
        accepted_kernel(
            heads, s_in.at[i % 2], keys.at[tall], values.at[tall], thin.at[few_rows], taken.at[few_rows],
            r_scr, u_scr, c_scr, kf, vf,
        )

    def step(i, carry):
        stage, c = i // 4, i % 4
        r = pick(stage, (3 - end, 3 - near, near))

        @pl.when(c == 0)
        def _():
            prepare(r)

        @pl.when(i == 2)
        def _():
            prepare(end)

        @pl.when(is_end)
        def _():
            sbuf[i] = product(r, c).astype(bf16)
            remote(sbuf.at[i], abuf.at[i], ss.at[i], ar.at[i], near, t).start()

        @pl.when(jnp.logical_and(inside, i == 1))
        def _():
            f_take(f_order[0])
            f_take(f_order[1])

        @pl.when(jnp.logical_and(inside, i == 5))
        def _():
            f_take(f_order[2])

        @pl.when(jnp.logical_and(is_end, i == 4))
        def _():
            f_take(f_order[0])

        @pl.when(jnp.logical_and(inside, i < 8))
        def _():
            part = product(r, c)
            sbuf[i] = (part + from_end(i)).astype(bf16)
            remote(sbuf.at[i], bbuf.at[i], ss.at[i], br.at[i], 3 - near, t).start()

        @pl.when(jnp.logical_and(inside, stage == 1))
        def _():
            part = product(end, c)
            sbuf[8 + c] = (part + from_inner(c)).astype(bf16)
            remote(sbuf.at[8 + c], cbuf.at[c], ss.at[8 + c], cr.at[c], end, t).start()

        @pl.when(jnp.logical_and(inside, stage == 2))
        def _():
            acc[c] = product(r, c) + from_inner(4 + c) + from_end(i)

        @pl.when(i % 2 == 0)
        def _():
            accept(i // 2)

        return carry

    lax.fori_loop(0, 12, step, 0)

    @pl.when(is_end)
    def _():
        f_take(f_order[1])

        def finish(c, carry):
            part = product(end, c)

            @pl.when(c == 1)
            def _():
                f_take(f_order[2])

            remote(cbuf.at[c], cbuf.at[c], ss.at[c], cr.at[c], k, beside).wait_recv()
            acc[c] = part + cbuf[c].astype(f32)
            return carry

        lax.fori_loop(0, 4, finish, 0)

    few_ref[...] = esend[k]
    for src in range(4):

        @pl.when(k != src)
        def _():
            remote(esend.at[src], erecv.at[src], es.at[src], er.at[src], k, beside).wait()
            few_ref[...] += erecv[src]
            remote(fbuf.at[src, half], fbuf.at[src, half], fys.at[src], fyr.at[src], k, beside).wait()

    remote(x_ref.at[bottom], xpre, xs.at[0], xp, k, across).wait_send()

    @pl.when(t != k)
    def _():
        remote(x_ref.at[top], xbuf.at[k, top], xs.at[1], xr.at[k, 0], t, landing).wait_send()

    @pl.when(across != k)
    def _():
        remote(xpre, xbuf.at[k, bottom], xs.at[2], xr.at[k, 1], across, landing).wait_send()

    for n in range(6):
        piece(k, top, 3 + n, 0, beside).wait_send()

    @pl.when(k < 3)
    def _():
        f_pass(k, k, 4).wait_send()

    @pl.when(k > 0)
    def _():
        f_pass(k, k, 5).wait_send()

    for src in range(4):

        @pl.when(jnp.logical_and(k != src, f_forwards(src)))
        def _():
            f_pass(src, k, src).wait_send()

    for i in range(12):
        remote(sbuf.at[i], abuf.at[i], ss.at[i], ar.at[i], k, beside).wait_send()


def project(x, gain, weights, forgetting, strength, final, state, keys, values, fade, pull, counts):
    rows, depth = x.shape
    width = weights[0].shape[1]
    seqs, heads = state.shape[:2]
    few_rows = 2 * heads + 8
    vmem, hbm = pl.BlockSpec(memory_space=pltpu.VMEM), pl.BlockSpec(memory_space=pl.ANY)
    dma = pltpu.SemaphoreType.DMA
    gain = gain.reshape(-1, 1, depth)
    forgetting, strength = forgetting.T, strength.T

    def chunks(n):
        return pltpu.VMEM((n, rows, width), bf16)

    def like(a):
        return pltpu.VMEM(a.shape, a.dtype)

    return pl.pallas_call(
        project_kernel,
        in_specs=[hbm] * 15,
        out_specs=[vmem] * 4,
        out_shape=[
            pltpu.VMEM((4, rows, width), f32),
            pltpu.VMEM((few_rows, rows), f32),
            pltpu.VMEM(state.shape, f32),
            pltpu.VMEM((4,) + final.shape, bf16),
        ],
        scratch_shapes=[
            like(x), like(gain), like(keys), like(values), like(fade), like(pull), like(counts),
            pltpu.VMEM((2, forgetting.shape[0], depth), bf16),
            pltpu.VMEM((seqs, 2 * P_SIZE * heads + 8), f32),
            pltpu.VMEM((rows // 2, depth), bf16),
            pltpu.VMEM((4, rows, depth), bf16),
            pltpu.VMEM((4, rows, depth), bf16),
            pltpu.VMEM((4, depth, width), bf16),
            chunks(12), chunks(12), chunks(8), chunks(4),
            pltpu.VMEM((4, few_rows, rows), f32),
            pltpu.VMEM((4, few_rows, rows), f32),
            pltpu.VMEM((2, SB) + state.shape[1:], f32),
            *[pltpu.VMEM((heads * n, DK), f32) for n in (TALL, TALL, SB, TALL, TALL)],
            dma((9,)), dma((9,)), dma, dma((4, 2)), dma((4,)), dma((12,)), dma((12,)), dma((8,)), dma((4,)), dma((4,)),
            dma((4,)), dma((2,)), dma, dma((6,)), dma((4,)), dma((4,)), dma((4,)),
        ],
        compiler_params=pltpu.CompilerParams(has_side_effects=True, collective_id=0, vmem_limit_bytes=LIMIT),
        name="project",
    )(x, gain, keys, values, fade, pull, counts, forgetting, strength, *weights, final, state)


PIECES = 3


def mix_kernel(flat_ref, f_ref, o_ref, part, mate, cross, ms, mr, xs, xr):
    k, t, g = lax.axis_index("kv"), lax.axis_index("tp"), lax.axis_index("grp")
    rows = flat_ref.shape[0]
    piece = rows // PIECES
    beside = t + 1 - 2 * (t % 2)
    across = (t + 2) % 4
    order = ((beside + 2) % 4, across, beside, t)

    def remote(src, dst, send, recv, tp):
        return pltpu.make_async_remote_copy(
            src, dst, send, recv, device_id={"grp": g, "kv": k, "tp": tp}, device_id_type=pl.DeviceIdType.MESH
        )

    barrier = pltpu.get_barrier_semaphore()
    for peer in (beside, across):
        pl.semaphore_signal(
            barrier, inc=1, device_id={"grp": g, "kv": k, "tp": peer}, device_id_type=pl.DeviceIdType.MESH
        )
    pl.semaphore_wait(barrier, 2)

    def to_mate(n, s):
        at = pl.ds(s * piece, piece)
        return remote(part.at[2 * n, at], mate.at[n, at], ms.at[n, s], mr.at[n, s], beside)

    def to_cross(s):
        at = pl.ds(s * piece, piece)
        return remote(part.at[1, at], cross.at[at], xs.at[s], xr.at[s], across)

    def fill(n, s):
        at = pl.ds(s * piece, piece)
        return jnp.dot(flat_ref[at, :], f_ref[order[n]], preferred_element_type=f32).astype(bf16)

    for s in range(PIECES):
        part[0, s * piece : (s + 1) * piece, :] = fill(0, s)
        to_mate(0, s).start()
    for s in range(PIECES):
        at = slice(s * piece, (s + 1) * piece)
        mine = fill(1, s).astype(f32)
        to_mate(0, s).wait_recv()
        part[1, at, :] = (mine + mate[0, at, :].astype(f32)).astype(bf16)
        to_cross(s).start()
    for s in range(PIECES):
        part[2, s * piece : (s + 1) * piece, :] = fill(2, s)
        to_mate(1, s).start()
    for s in range(PIECES):
        part[3, s * piece : (s + 1) * piece, :] = fill(3, s)
    for s in range(PIECES):
        at = slice(s * piece, (s + 1) * piece)
        to_mate(1, s).wait_recv()
        to_cross(s).wait_recv()
        o_ref[at, :] = (
            part[3, at, :].astype(f32) + mate[1, at, :].astype(f32) + cross[at, :].astype(f32)
        ).astype(bf16)
    for s in range(PIECES):
        to_mate(0, s).wait_send()
        to_mate(1, s).wait_send()
        to_cross(s).wait_send()


def mix(flat, final):
    rows, width = flat.shape
    cols = final.shape[2]
    vmem, hbm = pl.BlockSpec(memory_space=pltpu.VMEM), pl.BlockSpec(memory_space=pl.ANY)
    dma = pltpu.SemaphoreType.DMA
    return pl.pallas_call(
        mix_kernel,
        in_specs=[vmem, vmem],
        out_specs=vmem,
        out_shape=jax.ShapeDtypeStruct((rows, cols), bf16),
        scratch_shapes=[
            pltpu.VMEM((4, rows, cols), bf16),
            pltpu.VMEM((2, rows, cols), bf16),
            pltpu.VMEM((rows, cols), bf16),
            dma((2, PIECES)), dma((2, PIECES)), dma((PIECES,)), dma((PIECES,)),
        ],
        compiler_params=pltpu.CompilerParams(has_side_effects=True, collective_id=1, vmem_limit_bytes=LIMIT),
        name="mix",
    )(local(flat), local(final))


def on_device(
    n_kv,
    n_tp,
    candidate_embeddings,
    incoming_rms_scaling,
    probe_projector,
    address_projector,
    content_projector,
    sigmoid_mask_matrix,
    forgetting_projector,
    strength_projector_matrix,
    channel_forgetting_rates,
    forgetting_offset,
    extra_forgetting,
    outgoing_rms_scaling,
    final_projector,
    memory_matrix,
    earlier_addresses,
    earlier_contents,
    earlier_strengths,
    earlier_forgetting,
    admitted_counts,
):
    rows, local_cols = candidate_embeddings.shape
    features = incoming_rms_scaling.shape[0]
    depth, width = probe_projector.shape
    heads = width // DK
    seqs = rows // P_SIZE
    k_index, t_index = lax.axis_index("kv"), lax.axis_index("tp")

    def thin(values):
        return values.transpose(1, 2, 0).reshape(P_SIZE * heads, seqs)

    weights = (probe_projector, address_projector, content_projector, sigmoid_mask_matrix)
    fade, pull, extra = thin(earlier_forgetting), thin(earlier_strengths), thin(extra_forgetting)
    earlier = (memory_matrix, earlier_addresses.reshape(rows, width), earlier_contents.reshape(rows, width))
    if n_kv == 4 and n_tp == 4:
        summed, few, taken, columns = project(
            candidate_embeddings, incoming_rms_scaling, weights, forgetting_projector, strength_projector_matrix,
            final_projector, *earlier, fade, pull, admitted_counts.reshape(1, seqs),
        )
    else:
        every = lax.all_gather(candidate_embeddings, "tp", axis=1, tiled=True)
        every = lax.all_to_all(every, "kv", split_axis=1, concat_axis=0, tiled=True)
        gain_part = lax.dynamic_slice_in_dim(incoming_rms_scaling, k_index * depth, depth)
        floated = every.astype(f32)
        gained = (floated * gain_part).astype(bf16)
        decay_cols = lax.dynamic_slice(forgetting_projector, (k_index * depth, t_index * heads), (depth, heads))
        beta_cols = lax.dynamic_slice(strength_projector_matrix, (k_index * depth, t_index * heads), (depth, heads))
        few = jnp.concatenate(
            [
                jnp.dot(gained, jnp.concatenate([decay_cols, beta_cols], axis=1), preferred_element_type=f32),
                jnp.sum(floated * floated, axis=1, keepdims=True),
            ],
            axis=1,
        )
        few = lax.psum_scatter(few, "kv", scatter_dimension=0, tiled=True)
        few = jnp.pad(few, ((0, 0), (0, 7))).T
        partial = jnp.stack([jnp.dot(gained, w, preferred_element_type=f32).astype(bf16) for w in weights])
        summed = lax.psum_scatter(partial, "kv", scatter_dimension=1, tiled=True).astype(f32)
        counts = admitted_counts.astype(f32).reshape(seqs, 1)
        taken = accepted(*earlier, jnp.concatenate([fade.T, pull.T, counts], axis=1))
    flat, taken = attend(
        features, taken, summed, few, extra, channel_forgetting_rates, forgetting_offset, outgoing_rms_scaling
    )
    if n_kv == 4 and n_tp == 4:
        mixed = mix(flat, columns)
    else:
        gathered = lax.all_gather(flat, "kv", axis=0, tiled=True)
        terms = jnp.dot(gathered, final_projector, preferred_element_type=f32).astype(bf16)
        terms = lax.all_to_all(terms, "kv", split_axis=0, concat_axis=1, tiled=True)
        mixed = lax.psum_scatter(terms, "tp", scatter_dimension=1, tiled=True)
    return (mixed, taken)


def solution(mesh):
    row, per_head = P(("grp", "kv"), "tp"), P(("grp", "kv"), None, "tp")
    four = P(("grp", "kv"), None, "tp", None)
    weight = P("kv", "tp")
    state = P(("grp", "kv"), "tp", None, None)
    in_specs = (
        row, P(), weight, weight, weight, weight, P(), P(), P("tp"), P("tp"), per_head, P(),
        P("tp", "kv"), state, four, four, per_head, per_head, P(("grp", "kv")),
    )
    body = functools.partial(on_device, mesh.shape["kv"], mesh.shape["tp"])
    return jax.shard_map(body, mesh=mesh, in_specs=in_specs, out_specs=(row, state), check_vma=False)
```

```python
import functools

import jax
import jax.numpy as jnp
from jax import lax
from jax.experimental import pallas as pl
from jax.experimental.pallas import tpu as pltpu
from jax.sharding import PartitionSpec as P

DK = 128
P_SIZE = 4
SB = 8
TALL = SB * P_SIZE
epsilon = 1e-06
LIMIT = 42 * 2**20
f32 = jnp.float32
bf16 = jnp.bfloat16


def lane_dot(a, b):
    return jnp.sum(a * b, axis=-1, keepdims=True)


def first_half():
    return lax.broadcasted_iota(jnp.int32, (8, DK), 0) < P_SIZE


def load_heads(heads, src, dst, factor=None):
    for h in range(heads):
        part = src[:, h * DK : (h + 1) * DK].astype(f32)
        dst[pl.ds(h * TALL, TALL), :] = part if factor is None else (part * factor).astype(bf16).astype(f32)


def tile(h, pair):
    return pl.ds(h * TALL + pair * 8, 8)


def proposal(h, p):
    return pl.ds(h * TALL + p, SB, stride=P_SIZE)


def rows_to_columns(wide):
    count = wide.shape[1]
    same = lax.broadcasted_iota(jnp.int32, (count, count), 0) == lax.broadcasted_iota(jnp.int32, (count, count), 1)
    return lax.dot_general(
        same.astype(f32), wide, (((1,), (1,)), ((), ())),
        precision=lax.Precision.HIGHEST, preferred_element_type=f32,
    )


def accepted_kernel(heads, s_ref, k_ref, v_ref, n_ref, o_ref, r_scr, u_scr, c_scr, kf, vf):
    load_heads(heads, k_ref, kf)
    load_heads(heads, v_ref, vf)
    low = first_half()
    for pair in range(SB // 2):
        for h in range(heads):
            at = tile(h, pair)
            lhs = kf[at, :].astype(bf16)
            r0 = jnp.dot(lhs, s_ref[2 * pair, h].astype(bf16), preferred_element_type=f32)
            r1 = jnp.dot(lhs, s_ref[2 * pair + 1, h].astype(bf16), preferred_element_type=f32)
            r_scr[at, :] = jnp.where(low, r0, r1)
    few = n_ref[...]
    span = P_SIZE * heads
    count = few[:, 2 * span : 2 * span + 1]
    for h in range(heads):
        scale = jnp.ones((SB, 1), f32)
        ks, us, norms = [], [], []
        for p in range(P_SIZE):
            at = proposal(h, p)
            col = slice(p * heads + h, p * heads + h + 1)
            key = kf[at, :]
            norm = lax.rsqrt(lane_dot(key, key) + epsilon)
            live = count > float(p)
            g = jnp.where(live, jnp.exp(few[:, p * heads + h : p * heads + h + 1]), 1.0)
            b = jnp.where(live, few[:, span + p * heads + h : span + p * heads + h + 1], 0.0)
            rec = (scale * norm) * r_scr[at, :]
            for ki, ui, ni in zip(ks, us, norms):
                rec = rec + (lane_dot(ki, key) * (ni * norm)) * ui
            us = [ui * g for ui in us]
            scale = scale * g
            us.append(b * (vf[at, :] - g * rec))
            ks.append(key)
            norms.append(norm)
        for p in range(P_SIZE):
            u_scr[proposal(h, p), :] = us[p] * norms[p]
        c_scr[pl.ds(h * SB, SB), :] = jnp.broadcast_to(scale, (SB, DK))
    for pair in range(SB // 2):
        for h in range(heads):
            at = tile(h, pair)
            key = kf[at, :]
            lhs = jnp.concatenate([key, key], axis=0).astype(bf16)
            u = u_scr[at, :]
            hi = u.astype(bf16).astype(f32)
            lo = u - hi
            for half in range(2):
                keep = low if half == 0 else jnp.logical_not(low)
                rhs = jnp.concatenate([jnp.where(keep, hi, 0.0), jnp.where(keep, lo, 0.0)], axis=0).astype(bf16)
                seq = 2 * pair + half
                add = lax.dot_general(lhs, rhs, (((0,), (0,)), ((), ())), preferred_element_type=f32)
                o_ref[seq, h] = c_scr[pl.ds(h * SB + seq, 1), :] * s_ref[seq, h] + add


def attend_items(items, scratch, load, factor, state_at, scalars, gain, emit):
    rk, rq, qf, kf, vf, zf, of = scratch
    low = first_half()
    for j, item in enumerate(items):
        for n, dst in enumerate((qf, kf, vf, zf)):
            dst[pl.ds(j * TALL, TALL), :] = (load(item, n) * factor(item)).astype(bf16).astype(f32)
    for pair in range(SB // 2):
        for j, item in enumerate(items):
            at = tile(j, pair)
            lhs = jnp.concatenate([kf[at, :], qf[at, :]], axis=0).astype(bf16)
            r0 = jnp.dot(lhs, state_at(item, 2 * pair).astype(bf16), preferred_element_type=f32)
            r1 = jnp.dot(lhs, state_at(item, 2 * pair + 1).astype(bf16), preferred_element_type=f32)
            rk[at, :] = jnp.where(low, r0[:8], r1[:8])
            rq[at, :] = jnp.where(low, r0[8:], r1[8:])
    for j, item in enumerate(items):
        scale = jnp.ones((SB, 1), f32)
        ks, us, norms = [], [], []
        for p in range(P_SIZE):
            at = proposal(j, p)
            g, strength = scalars(item, p)
            key = kf[at, :]
            query = qf[at, :]
            norm = lax.rsqrt(lane_dot(key, key) + epsilon)
            qnorm = lax.rsqrt(lane_dot(query, query) + epsilon) * DK ** (-0.5)
            rec = (scale * norm) * rk[at, :]
            for ki, ui, ni in zip(ks, us, norms):
                rec = rec + (lane_dot(ki, key) * (ni * norm)) * ui
            us = [ui * g for ui in us]
            scale = scale * g
            us.append(strength * (vf[at, :] - g * rec))
            ks.append(key)
            norms.append(norm)
            att = (scale * qnorm) * rq[at, :]
            for ki, ui, ni in zip(ks, us, norms):
                att = att + (lane_dot(ki, query) * (ni * qnorm)) * ui
            gate = zf[at, :]
            mean = jnp.sum(att * att, axis=-1, keepdims=True) / DK
            of[at, :] = att * lax.rsqrt(mean + epsilon) * gain * (gate * jax.nn.sigmoid(gate))
    for j, item in enumerate(items):
        emit(item, of[pl.ds(j * TALL, TALL), :].astype(bf16))


def small_terms(heads, features, few_wide, extra, rates, offset, thin):
    rows = few_wide.shape[1]
    few = rows_to_columns(few_wide)
    factor = lax.rsqrt(few[:, 2 * heads : 2 * heads + 1] / features + epsilon)
    seqs = extra.shape[1]
    row = lax.broadcasted_iota(jnp.int32, (rows, seqs), 0)
    owner = jnp.right_shift(row, 2) == lax.broadcasted_iota(jnp.int32, (rows, seqs), 1)
    spread = lax.dot_general(
        owner.astype(f32), extra, (((1,), (1,)), ((), ())),
        precision=lax.Precision.HIGHEST, preferred_element_type=f32,
    )
    turn = jnp.bitwise_and(lax.broadcasted_iota(jnp.int32, (rows, heads), 0), 3)
    struck = pick(turn, [spread[:, p * heads : (p + 1) * heads] for p in range(P_SIZE)])
    raised = few[:, :heads] * factor + offset
    soft = jnp.maximum(raised, 0.0) + jnp.log1p(jnp.exp(-jnp.abs(raised)))
    thin[:, :heads] = jnp.exp(struck - jnp.exp(rates) * soft)
    thin[:, heads : 2 * heads] = jax.nn.sigmoid(few[:, heads : 2 * heads] * factor)
    thin[:, 2 * heads : 2 * heads + 1] = factor


def attend_kernel(heads, features, few_ref, extra_ref, rate_ref, offset_ref, w_ref, parts, state, o_ref, kept, thin, *rest):
    scratch, done = rest[:-1], rest[-1]
    keep = pltpu.make_async_copy(state, kept, done)
    keep.start()
    small_terms(heads, features, few_ref[...], extra_ref[...], rate_ref[...], offset_ref[...], thin)

    def block(i, carry):
        base = i * TALL
        tall = pl.ds(base, TALL)

        def scalars(h, p):
            both = thin[pl.ds(base + p, SB, stride=P_SIZE), :]
            return both[:, h : h + 1], both[:, heads + h : heads + h + 1]

        def emit(h, value):
            o_ref[tall, h * DK : (h + 1) * DK] = value

        attend_items(
            range(heads), scratch,
            lambda h, n: parts[n, tall, h * DK : (h + 1) * DK],
            lambda h: thin[tall, 2 * heads : 2 * heads + 1],
            lambda h, seq: state[i * SB + seq, h],
            scalars, w_ref[...], emit,
        )
        return carry

    lax.fori_loop(0, state.shape[0] // SB, block, 0)
    keep.wait()


GROUP = 3


def attend_head(h, heads, blocks, scratch, parts_at, thin, state, gain, flat):
    def group(it, carry):
        def tall(j):
            return pl.ds((it * GROUP + j) * TALL, TALL)

        def scalars(j, p):
            both = thin[pl.ds((it * GROUP + j) * TALL + p, SB, stride=P_SIZE), :]
            return tuple(pick(h, [both[:, n + m : n + m + 1] for m in range(heads)]) for n in (0, heads))

        def emit(j, value):
            flat[tall(j), pl.ds(pl.multiple_of(h * DK, DK), DK)] = value

        attend_items(
            range(GROUP), scratch,
            lambda j, n: parts_at(tall(j), n),
            lambda j: thin[tall(j), 2 * heads : 2 * heads + 1],
            lambda j, seq: state[(it * GROUP + j) * SB + seq, h],
            scalars, gain, emit,
        )
        return carry

    lax.fori_loop(0, blocks // GROUP, group, 0)


def last_kernel(heads, thin, w_ref, parts, state, some, columns, o_ref, kept, flat, *rest):
    scratch, done = rest[:-1], rest[-1]
    keep = pltpu.make_async_copy(state, kept, done)
    keep.start()
    flat[...] = some[...]
    blocks = state.shape[0] // SB
    attend_head(
        heads - 1, heads, blocks, scratch, lambda at, n: parts[at, n * DK : (n + 1) * DK], thin, state, w_ref[...], flat
    )
    for c in range(columns.shape[0]):
        o_ref[c] = jnp.dot(flat[...], columns[c], preferred_element_type=f32).astype(bf16)
    keep.wait()


def accepted(state, keys, values, few):
    seqs, heads = state.shape[:2]
    width = heads * DK
    rows = TALL
    tall = pl.BlockSpec((rows, width), lambda i: (i, 0))
    thin = pl.BlockSpec((SB, few.shape[1]), lambda i: (i, 0))
    block = pl.BlockSpec((SB, heads, DK, DK), lambda i: (i, 0, 0, 0))
    return pl.pallas_call(
        functools.partial(accepted_kernel, heads),
        grid=(seqs // SB,),
        in_specs=[block, tall, tall, thin],
        out_specs=block,
        out_shape=jax.ShapeDtypeStruct(state.shape, f32),
        scratch_shapes=[pltpu.VMEM((heads * n, DK), f32) for n in (TALL, TALL, SB, TALL, TALL)],
        cost_estimate=pl.CostEstimate(flops=10_000_000_000, bytes_accessed=2 * state.size * 4, transcendentals=0),
        name="accepted",
    )(state, keys, values, few)


def local(array):
    return pltpu.with_memory_space_constraint(array, pltpu.VMEM)


def attend(features, state, parts, few, extra, rates, offset, gain):
    seqs, heads = state.shape[:2]
    rows, width = parts.shape[1:]
    vmem = pl.BlockSpec(memory_space=pltpu.VMEM)
    return pl.pallas_call(
        functools.partial(attend_kernel, heads, features),
        in_specs=[vmem] * 7,
        out_specs=[vmem, pl.BlockSpec(memory_space=pl.ANY)],
        out_shape=[pltpu.VMEM((rows, width), bf16), jax.ShapeDtypeStruct(state.shape, f32)],
        scratch_shapes=[
            pltpu.VMEM((rows, 2 * heads + 8), f32),
            *[pltpu.VMEM((heads * TALL, DK), f32)] * 7,
            pltpu.SemaphoreType.DMA,
        ],
        compiler_params=pltpu.CompilerParams(vmem_limit_bytes=LIMIT),
        cost_estimate=pl.CostEstimate(flops=5_000_000_000, bytes_accessed=state.size * 4, transcendentals=0),
        name="attend",
    )(
        local(few), extra, rates.reshape(1, heads), offset.reshape(1, heads), gain.reshape(1, DK),
        local(parts), local(state),
    )


def pick(index, values):
    chosen = values[-1]
    for at, value in enumerate(values[:-1]):
        chosen = jnp.where(index == at, value, chosen)
    return chosen


def last_head(thin, gain, parts, state, some, columns):
    seqs, heads = state.shape[:2]
    rows, width = some.shape
    vmem = pl.BlockSpec(memory_space=pltpu.VMEM)
    return pl.pallas_call(
        functools.partial(last_kernel, heads),
        in_specs=[vmem] * 6,
        out_specs=[vmem, pl.BlockSpec(memory_space=pl.ANY)],
        out_shape=[
            pltpu.VMEM((columns.shape[0], rows, columns.shape[2]), bf16),
            jax.ShapeDtypeStruct(state.shape, f32),
        ],
        scratch_shapes=[
            pltpu.VMEM((rows, width), bf16),
            *[pltpu.VMEM((GROUP * TALL, DK), f32)] * 7,
            pltpu.SemaphoreType.DMA,
        ],
        compiler_params=pltpu.CompilerParams(vmem_limit_bytes=LIMIT),
        cost_estimate=pl.CostEstimate(flops=5_000_000_000, bytes_accessed=state.size * 4, transcendentals=0),
        name="last_head",
    )(local(thin), gain.reshape(1, DK), local(parts), local(state), local(some), local(columns))


def turned_slot(t):
    return pick(t, (0, 2, 1, 3))


def project_kernel(x_hbm, gain_hbm, keys_hbm, values_hbm, fade_hbm, pull_hbm, count_hbm, extra_hbm, rate_hbm, offset_hbm,
                   outer_hbm, wf, ws, wq, wk, wv, wz, wo, state, last, small, taken, fbuf, flat,
                   x_ref, gain_ref, keys, values, fade, pull, counts, extra, rates, offset, outer, fs, thin, few_ref, acc,
                   xpre, xbuf, gbuf, w, sbuf, abuf, bbuf, cbuf, esend, erecv, s_in,
                   r_scr, u_scr, c_scr, kf, vf, a0, a1, a2, a3, a4, a5, a6,
                   lsem, xs, xp, xr, wsem, ss, ar, br, cr, es, er, ins, fsem, fss, fzr, fys, fyr):
    k, t, g = lax.axis_index("kv"), lax.axis_index("tp"), lax.axis_index("grp")
    depth, width = w.shape[1], w.shape[2]
    features = gain_ref.shape[0] * depth
    rows = x_ref.shape[0]
    blocks = state.shape[0] // SB
    heads = state.shape[1]

    def remote(src, dst, send, recv, kv, tp, grp=g):
        return pltpu.make_async_remote_copy(
            src, dst, send, recv, device_id={"grp": grp, "kv": kv, "tp": tp}, device_id_type=pl.DeviceIdType.MESH
        )

    here = pl.ds(k * depth, depth)
    locals_ = [
        pltpu.make_async_copy(src, dst, lsem.at[n])
        for n, (src, dst) in enumerate(
            (
                (x_hbm, x_ref), (gain_hbm, gain_ref), (keys_hbm, keys), (values_hbm, values), (fade_hbm, fade),
                (pull_hbm, pull), (count_hbm, counts), (extra_hbm, extra), (rate_hbm, rates), (offset_hbm, offset), (outer_hbm, outer),
                (wf.at[:, here], fs.at[0]), (ws.at[:, here], fs.at[1]),
            )
        )
    ]
    for load in locals_:
        load.start()
    f_load = pltpu.make_async_copy(wo, fbuf.at[k], fsem)
    f_load.start()
    loads = [
        pltpu.make_async_copy(
            src.at[:, pl.ds(h * DK, DK)], w.at[h, :, pl.ds(n * DK, DK)], wsem.at[h * 4 + n]
        )
        for h in range(heads)
        for n, src in enumerate((wq, wk, wv, wz))
    ]
    for load in loads:
        load.start()

    def fetch(i):
        return pltpu.make_async_copy(state.at[pl.ds(i * SB, SB)], s_in.at[i % 2], ins.at[i % 2])

    fetch(0).start()

    beside = t + 1 - 2 * (t % 2)
    across = (t + 2) % 4
    corner = t % 2
    landing = 2 * (t // 2) + k % 2
    home = corner == k % 2
    top_kind = t // 2 == k // 2
    source = jnp.where(top_kind, k, (k + 2) % 4)
    near_src = jnp.where(k <= 1, corner, corner + 2)
    far_src = jnp.where(k <= 1, corner + 2, corner)
    barrier = pltpu.get_barrier_semaphore()

    def greet(kv, tp, grp=g):
        pl.semaphore_signal(
            barrier, inc=1, device_id={"grp": grp, "kv": kv, "tp": tp}, device_id_type=pl.DeviceIdType.MESH
        )

    greet(k, beside)
    greet(k, across)
    greet(k, t, 1 - g)
    for step in range(1, 4):
        greet((k + step) % 4, t)

    @pl.when(t != k)
    def _():
        greet(t, landing)

    @pl.when(across != k)
    def _():
        greet(across, landing)

    @pl.when(near_src != k)
    def _():
        greet(near_src, source)

    @pl.when(far_src != k)
    def _():
        greet(far_src, source)

    @pl.when(home)
    def _():
        pl.semaphore_wait(barrier, 8)

    @pl.when(jnp.logical_not(home))
    def _():
        pl.semaphore_wait(barrier, 10)

    half_tall = rows // 2
    top, bottom = pl.ds(0, half_tall), pl.ds(half_tall, half_tall)
    locals_[0].wait()

    @pl.when(t == k)
    def _():
        remote(x_ref.at[bottom], xbuf.at[k, bottom], xs.at[0], xr.at[k, 1], k, across).start()
        pltpu.make_async_copy(x_ref.at[top], xbuf.at[k, top], xr.at[k, 0]).start()

    @pl.when(t != k)
    def _():
        remote(x_ref.at[bottom], xpre, xs.at[0], xp, k, across).start()
        remote(x_ref.at[top], xbuf.at[k, top], xs.at[1], xr.at[k, 0], t, landing).start()

    @pl.when(across != k)
    def _():
        remote(xpre, xpre, xs.at[0], xp, k, across).wait_recv()
        remote(xpre, xbuf.at[k, bottom], xs.at[2], xr.at[k, 1], across, landing).start()

    kind = jnp.where(top_kind, 0, 1)
    direct = pl.ds(kind * half_tall, half_tall)
    crossed = pl.ds((1 - kind) * half_tall, half_tall)

    def piece(r, at, send, kd, tp):
        return remote(xbuf.at[r, at], xbuf.at[r, at], xs.at[send], xr.at[r, kd], k, tp)

    def spread(r, n):
        settled = jnp.logical_and(t == k, r == k)

        @pl.when(settled)
        def _():
            pltpu.make_async_copy(x_ref.at[top], xbuf.at[k, top], xr.at[k, 0]).wait()

        @pl.when(jnp.logical_not(settled))
        def _():
            piece(r, direct, 3, kind, across).wait_recv()

        piece(r, direct, 3 + n, kind, across).start()
        piece(r, direct, 5 + n, kind, beside).start()

    half_rows = fbuf.shape[1] // 2
    half = pl.ds(g * half_rows, half_rows)

    def f_pass(c, to, sem):
        return remote(fbuf.at[c, half], fbuf.at[c, half], fss.at[sem], fzr.at[c], to, t)

    def f_swap(c):
        return remote(fbuf.at[c, half], fbuf.at[c, half], fys.at[c], fyr.at[c], k, t, 1 - g)

    spread(near_src, 0)
    spread(far_src, 1)
    f_load.wait()

    @pl.when(k < 3)
    def _():
        f_pass(k, k + 1, 4).start()

    @pl.when(k > 0)
    def _():
        f_pass(k, k - 1, 5).start()

    for n, r in enumerate((near_src, far_src)):
        piece(r, crossed, 3, 1 - kind, across).wait_recv()
        piece(r, crossed, 7 + n, 1 - kind, beside).start()

    def f_forwards(c):
        return jnp.logical_or(jnp.logical_and(c < k, k < 3), jnp.logical_and(c > k, k > 0))

    def f_take(c):
        to = jnp.where(c < k, k + 1, k - 1)
        f_pass(c, k, c).wait_recv()

        @pl.when(f_forwards(c))
        def _():
            f_pass(c, to, c).start()

        f_swap(c).start()

    end = jnp.where(k <= 1, 0, 3)
    near = jnp.where(k <= 1, 1, 2)
    is_end = k == end
    inside = jnp.logical_not(is_end)
    f_order = (jnp.where(is_end, near, end), 3 - near, 3 - end)

    for load in locals_[1:]:
        load.wait()
    thin[...] = rows_to_columns(
        jnp.concatenate([fade[...], pull[...], jnp.broadcast_to(counts[...].astype(f32), (8, counts.shape[1]))], axis=0)
    )
    for load in loads:
        load.wait()
    for r in (1 - corner, 3 - corner):
        for kd in range(2):
            piece(r, pl.ds(kd * half_tall, half_tall), 3, kd, beside).wait_recv()

    nt = (((1,), (1,)), ((), ()))

    def prepare(r):
        floated = xbuf[r].astype(f32)
        gained = (floated * gain_ref[k]).astype(bf16)
        gbuf[r] = gained
        squares = floated * floated
        high = squares.astype(bf16)
        rest = (squares - high.astype(f32)).astype(bf16)
        ones = jnp.ones((8, depth), bf16)
        for n in range(2):
            every = lax.dot_general(fs[n], gained, nt, preferred_element_type=f32)
            esend[r, n * heads : (n + 1) * heads, :] = pick(t, [every[m * heads : (m + 1) * heads] for m in range(4)])
        esend[r, 2 * heads :, :] = lax.dot_general(ones, high, nt, preferred_element_type=f32) + lax.dot_general(
            ones, rest, nt, preferred_element_type=f32
        )

        @pl.when(r != k)
        def _():
            remote(esend.at[r], erecv.at[k], es.at[r], er.at[k], r, t).start()

    def product(r, c):
        return jnp.dot(gbuf[r], w[c], preferred_element_type=f32)

    def from_end(i):
        remote(abuf.at[i], abuf.at[i], ss.at[i], ar.at[i], k, beside).wait_recv()
        return abuf[i].astype(f32)

    def from_inner(i):
        remote(bbuf.at[i], bbuf.at[i], ss.at[i], br.at[i], k, beside).wait_recv()
        return bbuf[i].astype(f32)

    def accept(i):
        @pl.when(i + 1 < blocks)
        def _():
            fetch(i + 1).start()

        fetch(i).wait()

        tall, few_rows = pl.ds(i * TALL, TALL), pl.ds(i * SB, SB)
        accepted_kernel(
            heads, s_in.at[i % 2], keys.at[tall], values.at[tall], thin.at[few_rows], taken.at[few_rows],
            r_scr, u_scr, c_scr, kf, vf,
        )

    def accept_all():
        def one(i, carry):
            accept(i)
            return carry

        lax.fori_loop(0, blocks, one, 0)

    chunk_head, chunk_stage = (0, 1, 0, 0, 2, 1, 1, 3, 2, 3, 2, 3), (0, 0, 1, 2, 0, 1, 2, 0, 1, 1, 2, 2)
    prepared = (3 - end, end, 3 - near, near)

    def settle_small():
        few_ref[...] = esend[k]
        for src in range(4):

            @pl.when(k != src)
            def _():
                remote(esend.at[src], erecv.at[src], es.at[src], er.at[src], k, beside).wait()
                few_ref[...] += erecv[src]

        small_terms(heads, features, few_ref[...], extra[...], rates[...], offset[...], small)

    def attention(h):
        attend_head(
            h, heads, blocks, (a0, a1, a2, a3, a4, a5, a6),
            lambda at, n: acc[h, at, n * DK : (n + 1) * DK], small, taken, outer[...], flat,
        )

    @pl.when(inside)
    def _():
        def one(i, carry):
            prepare(pick(i, prepared))
            return carry

        lax.fori_loop(0, 4, one, 0)
        f_take(f_order[0])
        f_take(f_order[1])
        accept_all()

    def step(i, carry):
        h, stage = pick(i, chunk_head), pick(i, chunk_stage)
        r = pick(stage, (3 - end, 3 - near, near))

        @pl.when(jnp.logical_and(is_end, i < 4))
        def _():
            prepare(pick(i, prepared))

        @pl.when(is_end)
        def _():
            sbuf[i] = product(r, h).astype(bf16)
            remote(sbuf.at[i], abuf.at[i], ss.at[i], ar.at[i], near, t).start()

        @pl.when(jnp.logical_and(inside, stage < 2))
        def _():
            part = product(r, h)
            sbuf[i] = (part + from_end(i)).astype(bf16)
            remote(sbuf.at[i], bbuf.at[i], ss.at[i], br.at[i], 3 - near, t).start()

        @pl.when(jnp.logical_and(inside, i == 2))
        def _():
            f_take(f_order[2])

        back = jnp.logical_or(jnp.logical_or(i == 2, i == 3), jnp.logical_or(i == 6, i == 9))

        @pl.when(jnp.logical_and(inside, back))
        def _():
            m = jnp.where(i == 2, 0, i // 3)
            part = product(end, m)
            sbuf[12 + m] = (part + from_inner(pick(m, (0, 1, 4, 7)))).astype(bf16)
            remote(sbuf.at[12 + m], cbuf.at[m], ss.at[12 + m], cr.at[m], end, t).start()

        @pl.when(jnp.logical_and(inside, i == 4))
        def _():
            settle_small()

        ready = jnp.logical_or(jnp.logical_or(i == 4, i == 7), i == 10)

        @pl.when(jnp.logical_and(inside, ready))
        def _():
            m = i // 3 - 1
            acc[m] = product(near, m) + from_inner(pick(m, (2, 5, 8))) + from_end(pick(m, (3, 6, 10)))
            attention(m)

        @pl.when(jnp.logical_and(inside, i == 11))
        def _():
            last[...] = product(near, 3) + from_inner(9) + from_end(11)

        return carry

    lax.fori_loop(0, 12, step, 0)

    @pl.when(is_end)
    def _():
        f_take(f_order[0])
        accept_all()
        settle_small()
        f_take(f_order[1])

        def returned(m):
            part = product(end, m)
            remote(cbuf.at[m], cbuf.at[m], ss.at[m], cr.at[m], k, beside).wait_recv()
            return part + cbuf[m].astype(f32)

        def finish(m, carry):
            acc[m] = returned(m)
            attention(m)

            @pl.when(m == 1)
            def _():
                f_take(f_order[2])

            return carry

        lax.fori_loop(0, 3, finish, 0)
        last[...] = returned(3)

    for src in range(4):

        @pl.when(k != src)
        def _():
            remote(fbuf.at[src, half], fbuf.at[src, half], fys.at[src], fyr.at[src], k, beside).wait()

    remote(x_ref.at[bottom], xpre, xs.at[0], xp, k, across).wait_send()

    @pl.when(t != k)
    def _():
        remote(x_ref.at[top], xbuf.at[k, top], xs.at[1], xr.at[k, 0], t, landing).wait_send()

    @pl.when(across != k)
    def _():
        remote(xpre, xbuf.at[k, bottom], xs.at[2], xr.at[k, 1], across, landing).wait_send()

    for n in range(6):
        piece(k, top, 3 + n, 0, beside).wait_send()

    @pl.when(k < 3)
    def _():
        f_pass(k, k, 4).wait_send()

    @pl.when(k > 0)
    def _():
        f_pass(k, k, 5).wait_send()

    for src in range(4):

        @pl.when(jnp.logical_and(k != src, f_forwards(src)))
        def _():
            f_pass(src, k, src).wait_send()

    for i in range(12):

        @pl.when(is_end if chunk_stage[i] == 2 else k >= 0)
        def _():
            remote(sbuf.at[i], abuf.at[i], ss.at[i], ar.at[i], k, beside).wait_send()

    for m in range(4):

        @pl.when(inside)
        def _():
            remote(sbuf.at[12 + m], cbuf.at[m], ss.at[12 + m], cr.at[m], end, t).wait_send()


def project(x, gain, weights, forgetting, strength, final, state, keys, values, fade, pull, counts, extra, rates, offset, outer):
    rows, depth = x.shape
    width = weights[0].shape[1]
    seqs, heads = state.shape[:2]
    few_rows = 2 * heads + 8
    vmem, hbm = pl.BlockSpec(memory_space=pltpu.VMEM), pl.BlockSpec(memory_space=pl.ANY)
    dma = pltpu.SemaphoreType.DMA
    gain = gain.reshape(-1, 1, depth)
    rates, offset, outer = rates.reshape(1, heads), offset.reshape(1, heads), outer.reshape(1, DK)
    forgetting, strength = forgetting.T, strength.T

    def chunks(n):
        return pltpu.VMEM((n, rows, width), bf16)

    def like(a):
        return pltpu.VMEM(a.shape, a.dtype)

    return pl.pallas_call(
        project_kernel,
        in_specs=[hbm] * 19,
        out_specs=[vmem] * 5,
        out_shape=[
            pltpu.VMEM((rows, width), f32),
            pltpu.VMEM((rows, few_rows), f32),
            pltpu.VMEM(state.shape, f32),
            pltpu.VMEM((4,) + final.shape, bf16),
            pltpu.VMEM((rows, width), bf16),
        ],
        scratch_shapes=[
            like(x), like(gain), like(keys), like(values), like(fade), like(pull), like(counts),
            like(extra), like(rates), like(offset), like(outer),
            pltpu.VMEM((2, forgetting.shape[0], depth), bf16),
            pltpu.VMEM((seqs, 2 * P_SIZE * heads + 8), f32),
            pltpu.VMEM((few_rows, rows), f32),
            pltpu.VMEM((3, rows, width), f32),
            pltpu.VMEM((rows // 2, depth), bf16),
            pltpu.VMEM((4, rows, depth), bf16),
            pltpu.VMEM((4, rows, depth), bf16),
            pltpu.VMEM((4, depth, width), bf16),
            chunks(16), chunks(12), chunks(12), chunks(4),
            pltpu.VMEM((4, few_rows, rows), f32),
            pltpu.VMEM((4, few_rows, rows), f32),
            pltpu.VMEM((2, SB) + state.shape[1:], f32),
            *[pltpu.VMEM((heads * n, DK), f32) for n in (TALL, TALL, SB, TALL, TALL)],
            *[pltpu.VMEM((GROUP * TALL, DK), f32)] * 7,
            dma((13,)), dma((9,)), dma, dma((4, 2)), dma((16,)), dma((16,)), dma((12,)), dma((12,)), dma((4,)), dma((4,)),
            dma((4,)), dma((2,)), dma, dma((6,)), dma((4,)), dma((4,)), dma((4,)),
        ],
        compiler_params=pltpu.CompilerParams(has_side_effects=True, collective_id=0, vmem_limit_bytes=LIMIT),
        name="project",
    )(x, gain, keys, values, fade, pull, counts, extra, rates, offset, outer, forgetting, strength, *weights, final, state)


PIECES = 3


def mix_kernel(part, o_ref, mate, sent, cross, ms, mr, xs, xr):
    k, t, g = lax.axis_index("kv"), lax.axis_index("tp"), lax.axis_index("grp")
    rows = part.shape[1]
    piece = rows // PIECES
    beside = t + 1 - 2 * (t % 2)
    across = (t + 2) % 4
    order = ((beside + 2) % 4, beside)

    def remote(src, dst, send, recv, tp):
        return pltpu.make_async_remote_copy(
            src, dst, send, recv, device_id={"grp": g, "kv": k, "tp": tp}, device_id_type=pl.DeviceIdType.MESH
        )

    barrier = pltpu.get_barrier_semaphore()
    for peer in (beside, across):
        pl.semaphore_signal(
            barrier, inc=1, device_id={"grp": g, "kv": k, "tp": peer}, device_id_type=pl.DeviceIdType.MESH
        )
    pl.semaphore_wait(barrier, 2)

    def to_mate(n, s):
        at = pl.ds(s * piece, piece)
        return remote(part.at[order[n], at], mate.at[n, at], ms.at[n, s], mr.at[n, s], beside)

    def to_cross(s):
        at = pl.ds(s * piece, piece)
        return remote(sent.at[at], cross.at[at], xs.at[s], xr.at[s], across)

    for n in range(2):
        for s in range(PIECES):
            to_mate(n, s).start()
    for s in range(PIECES):
        at = slice(s * piece, (s + 1) * piece)
        to_mate(0, s).wait_recv()
        sent[at, :] = (part[across, at, :].astype(f32) + mate[0, at, :].astype(f32)).astype(bf16)
        to_cross(s).start()
    for s in range(PIECES):
        at = slice(s * piece, (s + 1) * piece)
        to_mate(1, s).wait_recv()
        to_cross(s).wait_recv()
        o_ref[at, :] = (
            part[t, at, :].astype(f32) + mate[1, at, :].astype(f32) + cross[at, :].astype(f32)
        ).astype(bf16)
    for s in range(PIECES):
        to_mate(0, s).wait_send()
        to_mate(1, s).wait_send()
        to_cross(s).wait_send()


def mix(part):
    rows, cols = part.shape[1:]
    vmem = pl.BlockSpec(memory_space=pltpu.VMEM)
    dma = pltpu.SemaphoreType.DMA
    return pl.pallas_call(
        mix_kernel,
        in_specs=[vmem],
        out_specs=vmem,
        out_shape=jax.ShapeDtypeStruct((rows, cols), bf16),
        scratch_shapes=[
            pltpu.VMEM((2, rows, cols), bf16),
            pltpu.VMEM((rows, cols), bf16),
            pltpu.VMEM((rows, cols), bf16),
            dma((2, PIECES)), dma((2, PIECES)), dma((PIECES,)), dma((PIECES,)),
        ],
        compiler_params=pltpu.CompilerParams(has_side_effects=True, collective_id=1, vmem_limit_bytes=LIMIT),
        name="mix",
    )(local(part))


def on_device(
    n_kv,
    n_tp,
    candidate_embeddings,
    incoming_rms_scaling,
    probe_projector,
    address_projector,
    content_projector,
    sigmoid_mask_matrix,
    forgetting_projector,
    strength_projector_matrix,
    channel_forgetting_rates,
    forgetting_offset,
    extra_forgetting,
    outgoing_rms_scaling,
    final_projector,
    memory_matrix,
    earlier_addresses,
    earlier_contents,
    earlier_strengths,
    earlier_forgetting,
    admitted_counts,
):
    rows, local_cols = candidate_embeddings.shape
    features = incoming_rms_scaling.shape[0]
    depth, width = probe_projector.shape
    heads = width // DK
    seqs = rows // P_SIZE
    k_index, t_index = lax.axis_index("kv"), lax.axis_index("tp")

    def thin(values):
        return values.transpose(1, 2, 0).reshape(P_SIZE * heads, seqs)

    weights = (probe_projector, address_projector, content_projector, sigmoid_mask_matrix)
    fade, pull, extra = thin(earlier_forgetting), thin(earlier_strengths), thin(extra_forgetting)
    earlier = (memory_matrix, earlier_addresses.reshape(rows, width), earlier_contents.reshape(rows, width))
    if n_kv == 4 and n_tp == 4:
        last, small, taken, columns, flat = project(
            candidate_embeddings, incoming_rms_scaling, weights, forgetting_projector, strength_projector_matrix,
            final_projector, *earlier, fade, pull, admitted_counts.reshape(1, seqs), extra,
            channel_forgetting_rates, forgetting_offset, outgoing_rms_scaling,
        )
        part, taken = last_head(small, outgoing_rms_scaling, last, taken, flat, columns)
        mixed = mix(part)
    else:
        every = lax.all_gather(candidate_embeddings, "tp", axis=1, tiled=True)
        every = lax.all_to_all(every, "kv", split_axis=1, concat_axis=0, tiled=True)
        gain_part = lax.dynamic_slice_in_dim(incoming_rms_scaling, k_index * depth, depth)
        floated = every.astype(f32)
        gained = (floated * gain_part).astype(bf16)
        decay_cols = lax.dynamic_slice(forgetting_projector, (k_index * depth, t_index * heads), (depth, heads))
        beta_cols = lax.dynamic_slice(strength_projector_matrix, (k_index * depth, t_index * heads), (depth, heads))
        few = jnp.concatenate(
            [
                jnp.dot(gained, jnp.concatenate([decay_cols, beta_cols], axis=1), preferred_element_type=f32),
                jnp.sum(floated * floated, axis=1, keepdims=True),
            ],
            axis=1,
        )
        few = lax.psum_scatter(few, "kv", scatter_dimension=0, tiled=True)
        few = jnp.pad(few, ((0, 0), (0, 7))).T
        partial = jnp.stack([jnp.dot(gained, w, preferred_element_type=f32).astype(bf16) for w in weights])
        summed = lax.psum_scatter(partial, "kv", scatter_dimension=1, tiled=True).astype(f32)
        counts = admitted_counts.astype(f32).reshape(seqs, 1)
        taken = accepted(*earlier, jnp.concatenate([fade.T, pull.T, counts], axis=1))
        flat, taken = attend(
            features, taken, summed, few, extra, channel_forgetting_rates, forgetting_offset, outgoing_rms_scaling
        )
        gathered = lax.all_gather(flat, "kv", axis=0, tiled=True)
        terms = jnp.dot(gathered, final_projector, preferred_element_type=f32).astype(bf16)
        terms = lax.all_to_all(terms, "kv", split_axis=0, concat_axis=1, tiled=True)
        mixed = lax.psum_scatter(terms, "tp", scatter_dimension=1, tiled=True)
    return (mixed, taken)


def solution(mesh):
    row, per_head = P(("grp", "kv"), "tp"), P(("grp", "kv"), None, "tp")
    four = P(("grp", "kv"), None, "tp", None)
    weight = P("kv", "tp")
    state = P(("grp", "kv"), "tp", None, None)
    in_specs = (
        row, P(), weight, weight, weight, weight, P(), P(), P("tp"), P("tp"), per_head, P(),
        P("tp", "kv"), state, four, four, per_head, per_head, P(("grp", "kv")),
    )
    body = functools.partial(on_device, mesh.shape["kv"], mesh.shape["tp"])
    return jax.shard_map(body, mesh=mesh, in_specs=in_specs, out_specs=(row, state), check_vma=False)
```

```python
import functools

import jax
import jax.numpy as jnp
from jax import lax
from jax.experimental import pallas as pl
from jax.experimental.pallas import tpu as pltpu
from jax.sharding import PartitionSpec as P

DK = 128
P_SIZE = 4
SB = 8
TALL = SB * P_SIZE
epsilon = 1e-06
LIMIT = 42 * 2**20
f32 = jnp.float32
bf16 = jnp.bfloat16


def lane_dot(a, b):
    return jnp.sum(a * b, axis=-1, keepdims=True)


def first_half():
    return lax.broadcasted_iota(jnp.int32, (8, DK), 0) < P_SIZE


def load_heads(heads, src, dst, factor=None):
    if len(src.shape) == 4:
        block = src[...].astype(f32)
        for h in range(heads):
            dst[pl.ds(h * TALL, TALL), :] = block[:, :, h, :].reshape(TALL, DK)
        return
    for h in range(heads):
        part = src[:, h * DK : (h + 1) * DK].astype(f32)
        dst[pl.ds(h * TALL, TALL), :] = part if factor is None else (part * factor).astype(bf16).astype(f32)


def tile(h, pair):
    return pl.ds(h * TALL + pair * 8, 8)


def proposal(h, p):
    return pl.ds(h * TALL + p, SB, stride=P_SIZE)


def rows_to_columns(wide):
    count = wide.shape[1]
    same = lax.broadcasted_iota(jnp.int32, (count, count), 0) == lax.broadcasted_iota(jnp.int32, (count, count), 1)
    return lax.dot_general(
        same.astype(f32), wide, (((1,), (1,)), ((), ())),
        precision=lax.Precision.HIGHEST, preferred_element_type=f32,
    )


def accepted_kernel(heads, s_ref, k_ref, v_ref, n_ref, o_ref, r_scr, u_scr, c_scr, kf, vf):
    load_heads(heads, k_ref, kf)
    load_heads(heads, v_ref, vf)
    low = first_half()
    for pair in range(SB // 2):
        for h in range(heads):
            at = tile(h, pair)
            lhs = kf[at, :].astype(bf16)
            r0 = jnp.dot(lhs, s_ref[2 * pair, h].astype(bf16), preferred_element_type=f32)
            r1 = jnp.dot(lhs, s_ref[2 * pair + 1, h].astype(bf16), preferred_element_type=f32)
            r_scr[at, :] = jnp.where(low, r0, r1)
    few = n_ref[...]
    span = P_SIZE * heads
    count = few[:, 2 * span : 2 * span + 1]
    for h in range(heads):
        scale = jnp.ones((SB, 1), f32)
        ks, us, norms = [], [], []
        for p in range(P_SIZE):
            at = proposal(h, p)
            col = slice(p * heads + h, p * heads + h + 1)
            key = kf[at, :]
            norm = lax.rsqrt(lane_dot(key, key) + epsilon)
            live = count > float(p)
            g = jnp.where(live, jnp.exp(few[:, p * heads + h : p * heads + h + 1]), 1.0)
            b = jnp.where(live, few[:, span + p * heads + h : span + p * heads + h + 1], 0.0)
            rec = (scale * norm) * r_scr[at, :]
            for ki, ui, ni in zip(ks, us, norms):
                rec = rec + (lane_dot(ki, key) * (ni * norm)) * ui
            us = [ui * g for ui in us]
            scale = scale * g
            us.append(b * (vf[at, :] - g * rec))
            ks.append(key)
            norms.append(norm)
        for p in range(P_SIZE):
            u_scr[proposal(h, p), :] = us[p] * norms[p]
        c_scr[pl.ds(h * SB, SB), :] = jnp.broadcast_to(scale, (SB, DK))
    for pair in range(SB // 2):
        for h in range(heads):
            at = tile(h, pair)
            key = kf[at, :]
            lhs = jnp.concatenate([key, key], axis=0).astype(bf16)
            u = u_scr[at, :]
            hi = u.astype(bf16).astype(f32)
            lo = u - hi
            for half in range(2):
                keep = low if half == 0 else jnp.logical_not(low)
                rhs = jnp.concatenate([jnp.where(keep, hi, 0.0), jnp.where(keep, lo, 0.0)], axis=0).astype(bf16)
                seq = 2 * pair + half
                add = lax.dot_general(lhs, rhs, (((0,), (0,)), ((), ())), preferred_element_type=f32)
                o_ref[seq, h] = c_scr[pl.ds(h * SB + seq, 1), :] * s_ref[seq, h] + add


def attend_items(items, scratch, load, factor, state_at, scalars, gain, emit):
    rk, rq, qf, kf, vf, zf, of = scratch
    low = first_half()
    for j, item in enumerate(items):
        for n, dst in enumerate((qf, kf, vf, zf)):
            dst[pl.ds(j * TALL, TALL), :] = (load(item, n) * factor(item)).astype(bf16).astype(f32)
    for pair in range(SB // 2):
        for j, item in enumerate(items):
            at = tile(j, pair)
            lhs = jnp.concatenate([kf[at, :], qf[at, :]], axis=0).astype(bf16)
            r0 = jnp.dot(lhs, state_at(item, 2 * pair).astype(bf16), preferred_element_type=f32)
            r1 = jnp.dot(lhs, state_at(item, 2 * pair + 1).astype(bf16), preferred_element_type=f32)
            rk[at, :] = jnp.where(low, r0[:8], r1[:8])
            rq[at, :] = jnp.where(low, r0[8:], r1[8:])
    for j, item in enumerate(items):
        scale = jnp.ones((SB, 1), f32)
        ks, us, norms = [], [], []
        for p in range(P_SIZE):
            at = proposal(j, p)
            g, strength = scalars(item, p)
            key = kf[at, :]
            query = qf[at, :]
            norm = lax.rsqrt(lane_dot(key, key) + epsilon)
            qnorm = lax.rsqrt(lane_dot(query, query) + epsilon) * DK ** (-0.5)
            rec = (scale * norm) * rk[at, :]
            for ki, ui, ni in zip(ks, us, norms):
                rec = rec + (lane_dot(ki, key) * (ni * norm)) * ui
            us = [ui * g for ui in us]
            scale = scale * g
            us.append(strength * (vf[at, :] - g * rec))
            ks.append(key)
            norms.append(norm)
            att = (scale * qnorm) * rq[at, :]
            for ki, ui, ni in zip(ks, us, norms):
                att = att + (lane_dot(ki, query) * (ni * qnorm)) * ui
            gate = zf[at, :]
            mean = jnp.sum(att * att, axis=-1, keepdims=True) / DK
            of[at, :] = att * lax.rsqrt(mean + epsilon) * gain * (gate * jax.nn.sigmoid(gate))
    for j, item in enumerate(items):
        emit(item, of[pl.ds(j * TALL, TALL), :].astype(bf16))


def small_terms(heads, features, few_wide, extra, rates, offset, thin):
    rows = few_wide.shape[1]
    few = rows_to_columns(few_wide)
    factor = lax.rsqrt(few[:, 2 * heads : 2 * heads + 1] / features + epsilon)
    seqs = extra.shape[1]
    row = lax.broadcasted_iota(jnp.int32, (rows, seqs), 0)
    owner = jnp.right_shift(row, 2) == lax.broadcasted_iota(jnp.int32, (rows, seqs), 1)
    spread = lax.dot_general(
        owner.astype(f32), extra, (((1,), (1,)), ((), ())),
        precision=lax.Precision.HIGHEST, preferred_element_type=f32,
    )
    turn = jnp.bitwise_and(lax.broadcasted_iota(jnp.int32, (rows, heads), 0), 3)
    struck = pick(turn, [spread[:, p * heads : (p + 1) * heads] for p in range(P_SIZE)])
    raised = few[:, :heads] * factor + offset
    soft = jnp.maximum(raised, 0.0) + jnp.log1p(jnp.exp(-jnp.abs(raised)))
    thin[:, :heads] = jnp.exp(struck - jnp.exp(rates) * soft)
    thin[:, heads : 2 * heads] = jax.nn.sigmoid(few[:, heads : 2 * heads] * factor)
    thin[:, 2 * heads : 2 * heads + 1] = factor


def attend_kernel(heads, features, few_ref, extra_ref, rate_ref, offset_ref, w_ref, parts, state, o_ref, kept, thin, *rest):
    scratch, done = rest[:-1], rest[-1]
    keep = pltpu.make_async_copy(state, kept, done)
    keep.start()
    small_terms(heads, features, few_ref[...], extra_ref[...], rate_ref[...], offset_ref[...], thin)

    def block(i, carry):
        base = i * TALL
        tall = pl.ds(base, TALL)

        def scalars(h, p):
            both = thin[pl.ds(base + p, SB, stride=P_SIZE), :]
            return both[:, h : h + 1], both[:, heads + h : heads + h + 1]

        def emit(h, value):
            o_ref[tall, h * DK : (h + 1) * DK] = value

        attend_items(
            range(heads), scratch,
            lambda h, n: parts[n, tall, h * DK : (h + 1) * DK],
            lambda h: thin[tall, 2 * heads : 2 * heads + 1],
            lambda h, seq: state[i * SB + seq, h],
            scalars, w_ref[...], emit,
        )
        return carry

    lax.fori_loop(0, state.shape[0] // SB, block, 0)
    keep.wait()


GROUP = 3


def attend_head(h, heads, blocks, scratch, parts_at, thin, state, gain, flat):
    def group(it, carry):
        def tall(j):
            return pl.ds((it * GROUP + j) * TALL, TALL)

        def scalars(j, p):
            both = thin[pl.ds((it * GROUP + j) * TALL + p, SB, stride=P_SIZE), :]
            return both[:, h : h + 1], both[:, heads + h : heads + h + 1]

        def emit(j, value):
            flat[tall(j), h * DK : (h + 1) * DK] = value

        attend_items(
            range(GROUP), scratch,
            lambda j, n: parts_at(tall(j), n),
            lambda j: thin[tall(j), 2 * heads : 2 * heads + 1],
            lambda j, seq: state[(it * GROUP + j) * SB + seq, h],
            scalars, gain, emit,
        )
        return carry

    lax.fori_loop(0, blocks // GROUP, group, 0)


def last_kernel(heads, thin, w_ref, parts, state, some, columns, o_ref, kept, flat, *rest):
    scratch, done = rest[:-1], rest[-1]
    keep = pltpu.make_async_copy(state, kept, done)
    keep.start()
    flat[...] = some[...]
    blocks = state.shape[0] // SB
    attend_head(
        heads - 1, heads, blocks, scratch, lambda at, n: parts[at, n * DK : (n + 1) * DK], thin, state, w_ref[...], flat
    )
    for c in range(columns.shape[0]):
        o_ref[c] = jnp.dot(flat[...], columns[c], preferred_element_type=f32).astype(bf16)
    keep.wait()


def accepted(state, keys, values, few):
    seqs, heads = state.shape[:2]
    width = heads * DK
    rows = TALL
    tall = pl.BlockSpec((rows, width), lambda i: (i, 0))
    thin = pl.BlockSpec((SB, few.shape[1]), lambda i: (i, 0))
    block = pl.BlockSpec((SB, heads, DK, DK), lambda i: (i, 0, 0, 0))
    return pl.pallas_call(
        functools.partial(accepted_kernel, heads),
        grid=(seqs // SB,),
        in_specs=[block, tall, tall, thin],
        out_specs=block,
        out_shape=jax.ShapeDtypeStruct(state.shape, f32),
        scratch_shapes=[pltpu.VMEM((heads * n, DK), f32) for n in (TALL, TALL, SB, TALL, TALL)],
        cost_estimate=pl.CostEstimate(flops=10_000_000_000, bytes_accessed=2 * state.size * 4, transcendentals=0),
        name="accepted",
    )(state, keys, values, few)


def local(array):
    return pltpu.with_memory_space_constraint(array, pltpu.VMEM)


def attend(features, state, parts, few, extra, rates, offset, gain):
    seqs, heads = state.shape[:2]
    rows, width = parts.shape[1:]
    vmem = pl.BlockSpec(memory_space=pltpu.VMEM)
    return pl.pallas_call(
        functools.partial(attend_kernel, heads, features),
        in_specs=[vmem] * 7,
        out_specs=[vmem, pl.BlockSpec(memory_space=pl.ANY)],
        out_shape=[pltpu.VMEM((rows, width), bf16), jax.ShapeDtypeStruct(state.shape, f32)],
        scratch_shapes=[
            pltpu.VMEM((rows, 2 * heads + 8), f32),
            *[pltpu.VMEM((heads * TALL, DK), f32)] * 7,
            pltpu.SemaphoreType.DMA,
        ],
        compiler_params=pltpu.CompilerParams(vmem_limit_bytes=LIMIT),
        cost_estimate=pl.CostEstimate(flops=5_000_000_000, bytes_accessed=state.size * 4, transcendentals=0),
        name="attend",
    )(
        local(few), extra, rates.reshape(1, heads), offset.reshape(1, heads), gain.reshape(1, DK),
        local(parts), local(state),
    )


def pick(index, values):
    chosen = values[-1]
    for at, value in enumerate(values[:-1]):
        chosen = jnp.where(index == at, value, chosen)
    return chosen


def last_head(thin, gain, parts, state, some, columns):
    seqs, heads = state.shape[:2]
    rows, width = some.shape
    vmem = pl.BlockSpec(memory_space=pltpu.VMEM)
    return pl.pallas_call(
        functools.partial(last_kernel, heads),
        in_specs=[vmem] * 6,
        out_specs=[vmem, pl.BlockSpec(memory_space=pl.ANY)],
        out_shape=[
            pltpu.VMEM((columns.shape[0], rows, columns.shape[2]), bf16),
            jax.ShapeDtypeStruct(state.shape, f32),
        ],
        scratch_shapes=[
            pltpu.VMEM((rows, width), bf16),
            *[pltpu.VMEM((GROUP * TALL, DK), f32)] * 7,
            pltpu.SemaphoreType.DMA,
        ],
        compiler_params=pltpu.CompilerParams(vmem_limit_bytes=LIMIT),
        cost_estimate=pl.CostEstimate(flops=5_000_000_000, bytes_accessed=state.size * 4, transcendentals=0),
        name="last_head",
    )(local(thin), gain.reshape(1, DK), local(parts), local(state), local(some), local(columns))


def turned_slot(t):
    return pick(t, (0, 2, 1, 3))


def project_kernel(x_hbm, gain_hbm, keys_hbm, values_hbm, fade_hbm, pull_hbm, count_hbm, extra_hbm, rate_hbm, offset_hbm,
                   outer_hbm, wf, ws, wq, wk, wv, wz, wo, state, last, small, taken, fbuf, flat,
                   x_ref, gain_ref, keys, values, fade, pull, counts, extra, rates, offset, outer, fs, thin, few_ref, acc,
                   xpre, xbuf, gbuf, w, sbuf, abuf, bbuf, cbuf, esend, erecv, s_in,
                   r_scr, u_scr, c_scr, kf, vf, a0, a1, a2, a3, a4, a5, a6,
                   lsem, xs, xp, xr, wsem, ss, ar, br, cr, es, er, ins, fsem, fss, fzr, fys, fyr):
    k, t, g = lax.axis_index("kv"), lax.axis_index("tp"), lax.axis_index("grp")
    depth, width = w.shape[1], w.shape[2]
    features = gain_ref.shape[0] * depth
    rows = x_ref.shape[0]
    blocks = state.shape[0] // SB
    heads = state.shape[1]

    def remote(src, dst, send, recv, kv, tp, grp=g):
        return pltpu.make_async_remote_copy(
            src, dst, send, recv, device_id={"grp": grp, "kv": kv, "tp": tp}, device_id_type=pl.DeviceIdType.MESH
        )

    here = pl.ds(k * depth, depth)
    locals_ = [
        pltpu.make_async_copy(src, dst, lsem.at[n])
        for n, (src, dst) in enumerate(
            (
                (x_hbm, x_ref), (gain_hbm, gain_ref), (keys_hbm, keys), (values_hbm, values), (fade_hbm, fade),
                (pull_hbm, pull), (count_hbm, counts), (extra_hbm, extra), (rate_hbm, rates), (offset_hbm, offset), (outer_hbm, outer),
                (wf.at[:, here], fs.at[0]), (ws.at[:, here], fs.at[1]),
            )
        )
    ]
    for load in locals_:
        load.start()
    f_load = pltpu.make_async_copy(wo, fbuf.at[k], fsem)
    f_load.start()
    loads = [
        pltpu.make_async_copy(
            src.at[:, pl.ds(h * DK, DK)], w.at[h, :, pl.ds(n * DK, DK)], wsem.at[h * 4 + n]
        )
        for h in range(heads)
        for n, src in enumerate((wq, wk, wv, wz))
    ]
    for load in loads:
        load.start()

    def fetch(i):
        return pltpu.make_async_copy(state.at[pl.ds(i * SB, SB)], s_in.at[i % 2], ins.at[i % 2])

    fetch(0).start()

    beside = t + 1 - 2 * (t % 2)
    across = (t + 2) % 4
    corner = t % 2
    landing = 2 * (t // 2) + k % 2
    home = corner == k % 2
    top_kind = t // 2 == k // 2
    source = jnp.where(top_kind, k, (k + 2) % 4)
    near_src = jnp.where(k <= 1, corner, corner + 2)
    far_src = jnp.where(k <= 1, corner + 2, corner)
    barrier = pltpu.get_barrier_semaphore()

    def greet(kv, tp, grp=g):
        pl.semaphore_signal(
            barrier, inc=1, device_id={"grp": grp, "kv": kv, "tp": tp}, device_id_type=pl.DeviceIdType.MESH
        )

    greet(k, beside)
    greet(k, across)
    greet(k, t, 1 - g)
    for step in range(1, 4):
        greet((k + step) % 4, t)

    @pl.when(t != k)
    def _():
        greet(t, landing)

    @pl.when(across != k)
    def _():
        greet(across, landing)

    @pl.when(near_src != k)
    def _():
        greet(near_src, source)

    @pl.when(far_src != k)
    def _():
        greet(far_src, source)

    @pl.when(home)
    def _():
        pl.semaphore_wait(barrier, 8)

    @pl.when(jnp.logical_not(home))
    def _():
        pl.semaphore_wait(barrier, 10)

    quarter = rows // 4
    locals_[0].wait()

    def part(q):
        return pl.ds(q * quarter, quarter)

    def forward(q):
        return remote(xpre.at[q], xbuf.at[k, part(2 + q)], xs.at[4 + q], xr.at[k, 2 + q], across, landing)

    def outward(q):
        return remote(x_ref.at[part(q)], xbuf.at[k, part(q)], xs.at[2 + q], xr.at[k, q], t, landing)

    def settled_copy(q):
        return pltpu.make_async_copy(x_ref.at[part(q)], xbuf.at[k, part(q)], xr.at[k, q])

    def sideways(q):
        return remote(x_ref.at[part(2 + q)], xpre.at[q], xs.at[q], xp.at[q], k, across)

    @pl.when(t == k)
    def _():
        for q in range(2):
            remote(x_ref.at[part(2 + q)], xbuf.at[k, part(2 + q)], xs.at[q], xr.at[k, 2 + q], k, across).start()
        for q in range(2):
            settled_copy(q).start()

    @pl.when(t != k)
    def _():
        for q in range(2):
            sideways(q).start()
        for q in range(2):
            outward(q).start()

    @pl.when(across != k)
    def _():
        for q in range(2):
            sideways(q).wait_recv()
            forward(q).start()

    kind = jnp.where(top_kind, 0, 1)

    def piece(r, q, send, tp):
        at = pl.ds(q * quarter, quarter)
        return remote(xbuf.at[r, at], xbuf.at[r, at], xs.at[send], xr.at[r, q], k, tp)

    def spread(r, n, q):
        settled = jnp.logical_and(t == k, r == k)

        @pl.when(settled)
        def _():
            settled_copy(q).wait()

        @pl.when(jnp.logical_not(settled))
        def _():
            piece(r, 2 * kind + q, 6, across).wait_recv()

        piece(r, 2 * kind + q, 6 + n, across).start()
        piece(r, 2 * kind + q, 10 + n, beside).start()

    half_rows = fbuf.shape[1] // 2
    half = pl.ds(g * half_rows, half_rows)

    def f_pass(c, to, sem):
        return remote(fbuf.at[c, half], fbuf.at[c, half], fss.at[sem], fzr.at[c], to, t)

    def f_swap(c):
        return remote(fbuf.at[c, half], fbuf.at[c, half], fys.at[c], fyr.at[c], k, t, 1 - g)

    for q in range(2):
        spread(near_src, 2 * q, q)
        spread(far_src, 2 * q + 1, q)
    f_load.wait()

    @pl.when(k < 3)
    def _():
        f_pass(k, k + 1, 4).start()

    @pl.when(k > 0)
    def _():
        f_pass(k, k - 1, 5).start()

    for q in range(2):
        for n, r in enumerate((near_src, far_src)):
            piece(r, 2 - 2 * kind + q, 6, across).wait_recv()
            piece(r, 2 - 2 * kind + q, 14 + 2 * q + n, beside).start()

    def f_forwards(c):
        return jnp.logical_or(jnp.logical_and(c < k, k < 3), jnp.logical_and(c > k, k > 0))

    def f_take(c):
        to = jnp.where(c < k, k + 1, k - 1)
        f_pass(c, k, c).wait_recv()

        @pl.when(f_forwards(c))
        def _():
            f_pass(c, to, c).start()

        f_swap(c).start()

    end = jnp.where(k <= 1, 0, 3)
    near = jnp.where(k <= 1, 1, 2)
    is_end = k == end
    inside = jnp.logical_not(is_end)
    f_order = (jnp.where(is_end, near, end), 3 - near, 3 - end)

    for load in locals_[1:]:
        load.wait()
    thin[...] = rows_to_columns(
        jnp.concatenate([fade[...], pull[...], jnp.broadcast_to(counts[...].astype(f32), (8, counts.shape[1]))], axis=0)
    )
    for load in loads:
        load.wait()
    for r in (1 - corner, 3 - corner):
        for q in range(4):
            piece(r, q, 6, beside).wait_recv()

    nt = (((1,), (1,)), ((), ()))

    def prepare(r):
        floated = xbuf[r].astype(f32)
        gained = (floated * gain_ref[k]).astype(bf16)
        gbuf[r] = gained
        squares = floated * floated
        high = squares.astype(bf16)
        rest = (squares - high.astype(f32)).astype(bf16)
        ones = jnp.ones((8, depth), bf16)
        for n in range(2):
            every = lax.dot_general(fs[n], gained, nt, preferred_element_type=f32)
            esend[r, n * heads : (n + 1) * heads, :] = pick(t, [every[m * heads : (m + 1) * heads] for m in range(4)])
        esend[r, 2 * heads :, :] = lax.dot_general(ones, high, nt, preferred_element_type=f32) + lax.dot_general(
            ones, rest, nt, preferred_element_type=f32
        )

        @pl.when(r != k)
        def _():
            remote(esend.at[r], erecv.at[k], es.at[r], er.at[k], r, t).start()

    def product(r, c):
        return jnp.dot(gbuf[r], w[c], preferred_element_type=f32)

    def from_end(i):
        remote(abuf.at[i], abuf.at[i], ss.at[i], ar.at[i], k, beside).wait_recv()
        return abuf[i].astype(f32)

    def from_inner(i):
        remote(bbuf.at[i], bbuf.at[i], ss.at[i], br.at[i], k, beside).wait_recv()
        return bbuf[i].astype(f32)

    def accept(i):
        @pl.when(i + 1 < blocks)
        def _():
            fetch(i + 1).start()

        fetch(i).wait()

        few_rows = pl.ds(i * SB, SB)
        accepted_kernel(
            heads, s_in.at[i % 2], keys.at[few_rows], values.at[few_rows], thin.at[few_rows], taken.at[few_rows],
            r_scr, u_scr, c_scr, kf, vf,
        )

    def accept_all():
        def one(i, carry):
            accept(i)
            return carry

        lax.fori_loop(0, blocks, one, 0)

    chunk_head, chunk_stage = (0, 1, 0, 0, 2, 1, 1, 3, 2, 3, 2, 3), (0, 0, 1, 2, 0, 1, 2, 0, 1, 1, 2, 2)
    prepared = (3 - end, end, 3 - near, near)

    def settle_small():
        few_ref[...] = esend[k]
        for src in range(4):

            @pl.when(k != src)
            def _():
                remote(esend.at[src], erecv.at[src], es.at[src], er.at[src], k, beside).wait()
                few_ref[...] += erecv[src]

        small_terms(heads, features, few_ref[...], extra[...], rates[...], offset[...], small)

    def attention(h):
        attend_head(
            h, heads, blocks, (a0, a1, a2, a3, a4, a5, a6),
            lambda at, n: acc[h, at, n * DK : (n + 1) * DK], small, taken, outer[...], flat,
        )

    @pl.when(inside)
    def _():
        def one(i, carry):
            prepare(pick(i, prepared))
            return carry

        lax.fori_loop(0, 4, one, 0)
        accept_all()
        f_take(f_order[0])
        f_take(f_order[1])

    def step(i, carry):
        h, stage = pick(i, chunk_head), pick(i, chunk_stage)
        r = pick(stage, (3 - end, 3 - near, near))

        @pl.when(jnp.logical_and(is_end, i < 4))
        def _():
            prepare(pick(i, prepared))

        @pl.when(is_end)
        def _():
            sbuf[i] = product(r, h).astype(bf16)
            remote(sbuf.at[i], abuf.at[i], ss.at[i], ar.at[i], near, t).start()

        @pl.when(jnp.logical_and(inside, stage < 2))
        def _():
            part = product(r, h)
            sbuf[i] = (part + from_end(i)).astype(bf16)
            remote(sbuf.at[i], bbuf.at[i], ss.at[i], br.at[i], 3 - near, t).start()

        @pl.when(jnp.logical_and(inside, i == 2))
        def _():
            f_take(f_order[2])

        back = jnp.logical_or(jnp.logical_or(i == 2, i == 3), jnp.logical_or(i == 6, i == 9))

        @pl.when(jnp.logical_and(inside, back))
        def _():
            m = jnp.where(i == 2, 0, i // 3)
            part = product(end, m)
            sbuf[12 + m] = (part + from_inner(pick(m, (0, 1, 4, 7)))).astype(bf16)
            remote(sbuf.at[12 + m], cbuf.at[m], ss.at[12 + m], cr.at[m], end, t).start()

        @pl.when(jnp.logical_and(inside, i == 4))
        def _():
            settle_small()

        ready = jnp.logical_or(jnp.logical_or(i == 4, i == 7), i == 10)

        @pl.when(jnp.logical_and(inside, ready))
        def _():
            m = i // 3 - 1
            acc[m] = product(near, m) + from_inner(pick(m, (2, 5, 8))) + from_end(pick(m, (3, 6, 10)))

        for m in range(3):

            @pl.when(jnp.logical_and(inside, i == 4 + 3 * m))
            def _():
                attention(m)

        @pl.when(jnp.logical_and(inside, i == 11))
        def _():
            last[...] = product(near, 3) + from_inner(9) + from_end(11)

        return carry

    lax.fori_loop(0, 12, step, 0)

    @pl.when(is_end)
    def _():
        f_take(f_order[0])
        accept_all()
        settle_small()
        f_take(f_order[1])

        def returned(m):
            part = product(end, m)
            remote(cbuf.at[m], cbuf.at[m], ss.at[m], cr.at[m], k, beside).wait_recv()
            return part + cbuf[m].astype(f32)

        for m in range(3):
            acc[m] = returned(m)
            attention(m)
            if m == 1:
                f_take(f_order[2])
        last[...] = returned(3)

    for src in range(4):

        @pl.when(k != src)
        def _():
            remote(fbuf.at[src, half], fbuf.at[src, half], fys.at[src], fyr.at[src], k, beside).wait()

    for q in range(2):
        sideways(q).wait_send()

    @pl.when(t != k)
    def _():
        for q in range(2):
            outward(q).wait_send()

    @pl.when(across != k)
    def _():
        for q in range(2):
            forward(q).wait_send()

    for n in range(12):
        piece(k, 0, 6 + n, beside).wait_send()

    @pl.when(k < 3)
    def _():
        f_pass(k, k, 4).wait_send()

    @pl.when(k > 0)
    def _():
        f_pass(k, k, 5).wait_send()

    for src in range(4):

        @pl.when(jnp.logical_and(k != src, f_forwards(src)))
        def _():
            f_pass(src, k, src).wait_send()

    for i in range(12):

        @pl.when(is_end if chunk_stage[i] == 2 else k >= 0)
        def _():
            remote(sbuf.at[i], abuf.at[i], ss.at[i], ar.at[i], k, beside).wait_send()

    for m in range(4):

        @pl.when(inside)
        def _():
            remote(sbuf.at[12 + m], cbuf.at[m], ss.at[12 + m], cr.at[m], end, t).wait_send()


def project(x, gain, weights, forgetting, strength, final, state, keys, values, fade, pull, counts, extra, rates, offset, outer):
    rows, depth = x.shape
    width = weights[0].shape[1]
    seqs, heads = state.shape[:2]
    few_rows = 2 * heads + 8
    vmem, hbm = pl.BlockSpec(memory_space=pltpu.VMEM), pl.BlockSpec(memory_space=pl.ANY)
    dma = pltpu.SemaphoreType.DMA
    gain = gain.reshape(-1, 1, depth)
    rates, offset, outer = rates.reshape(1, heads), offset.reshape(1, heads), outer.reshape(1, DK)
    forgetting, strength = forgetting.T, strength.T

    def chunks(n):
        return pltpu.VMEM((n, rows, width), bf16)

    def like(a):
        return pltpu.VMEM(a.shape, a.dtype)

    return pl.pallas_call(
        project_kernel,
        in_specs=[hbm] * 19,
        out_specs=[vmem] * 5,
        out_shape=[
            pltpu.VMEM((rows, width), f32),
            pltpu.VMEM((rows, few_rows), f32),
            pltpu.VMEM(state.shape, f32),
            pltpu.VMEM((4,) + final.shape, bf16),
            pltpu.VMEM((rows, width), bf16),
        ],
        scratch_shapes=[
            like(x), like(gain), like(keys), like(values), like(fade), like(pull), like(counts),
            like(extra), like(rates), like(offset), like(outer),
            pltpu.VMEM((2, forgetting.shape[0], depth), bf16),
            pltpu.VMEM((seqs, 2 * P_SIZE * heads + 8), f32),
            pltpu.VMEM((few_rows, rows), f32),
            pltpu.VMEM((3, rows, width), f32),
            pltpu.VMEM((2, rows // 4, depth), bf16),
            pltpu.VMEM((4, rows, depth), bf16),
            pltpu.VMEM((4, rows, depth), bf16),
            pltpu.VMEM((4, depth, width), bf16),
            chunks(16), chunks(12), chunks(12), chunks(4),
            pltpu.VMEM((4, few_rows, rows), f32),
            pltpu.VMEM((4, few_rows, rows), f32),
            pltpu.VMEM((2, SB) + state.shape[1:], f32),
            *[pltpu.VMEM((heads * n, DK), f32) for n in (TALL, TALL, SB, TALL, TALL)],
            *[pltpu.VMEM((GROUP * TALL, DK), f32)] * 7,
            dma((13,)), dma((18,)), dma((2,)), dma((4, 4)), dma((16,)), dma((16,)), dma((12,)), dma((12,)), dma((4,)), dma((4,)),
            dma((4,)), dma((2,)), dma, dma((6,)), dma((4,)), dma((4,)), dma((4,)),
        ],
        compiler_params=pltpu.CompilerParams(has_side_effects=True, collective_id=0, vmem_limit_bytes=LIMIT),
        name="project",
    )(x, gain, keys, values, fade, pull, counts, extra, rates, offset, outer, forgetting, strength, *weights, final, state)


PIECES = 3


def mix_kernel(part, o_ref, mate, sent, cross, ms, mr, xs, xr):
    k, t, g = lax.axis_index("kv"), lax.axis_index("tp"), lax.axis_index("grp")
    rows = part.shape[1]
    piece = rows // PIECES
    beside = t + 1 - 2 * (t % 2)
    across = (t + 2) % 4
    order = ((beside + 2) % 4, beside)

    def remote(src, dst, send, recv, tp):
        return pltpu.make_async_remote_copy(
            src, dst, send, recv, device_id={"grp": g, "kv": k, "tp": tp}, device_id_type=pl.DeviceIdType.MESH
        )

    barrier = pltpu.get_barrier_semaphore()
    for peer in (beside, across):
        pl.semaphore_signal(
            barrier, inc=1, device_id={"grp": g, "kv": k, "tp": peer}, device_id_type=pl.DeviceIdType.MESH
        )
    pl.semaphore_wait(barrier, 2)

    def to_mate(n, s):
        at = pl.ds(s * piece, piece)
        return remote(part.at[order[n], at], mate.at[n, at], ms.at[n, s], mr.at[n, s], beside)

    def to_cross(s):
        at = pl.ds(s * piece, piece)
        return remote(sent.at[at], cross.at[at], xs.at[s], xr.at[s], across)

    for n in range(2):
        for s in range(PIECES):
            to_mate(n, s).start()
    for s in range(PIECES):
        at = slice(s * piece, (s + 1) * piece)
        to_mate(0, s).wait_recv()
        sent[at, :] = (part[across, at, :].astype(f32) + mate[0, at, :].astype(f32)).astype(bf16)
        to_cross(s).start()
    for s in range(PIECES):
        at = slice(s * piece, (s + 1) * piece)
        to_mate(1, s).wait_recv()
        to_cross(s).wait_recv()
        o_ref[at, :] = (
            part[t, at, :].astype(f32) + mate[1, at, :].astype(f32) + cross[at, :].astype(f32)
        ).astype(bf16)
    for s in range(PIECES):
        to_mate(0, s).wait_send()
        to_mate(1, s).wait_send()
        to_cross(s).wait_send()


def mix(part):
    rows, cols = part.shape[1:]
    vmem = pl.BlockSpec(memory_space=pltpu.VMEM)
    dma = pltpu.SemaphoreType.DMA
    return pl.pallas_call(
        mix_kernel,
        in_specs=[vmem],
        out_specs=vmem,
        out_shape=jax.ShapeDtypeStruct((rows, cols), bf16),
        scratch_shapes=[
            pltpu.VMEM((2, rows, cols), bf16),
            pltpu.VMEM((rows, cols), bf16),
            pltpu.VMEM((rows, cols), bf16),
            dma((2, PIECES)), dma((2, PIECES)), dma((PIECES,)), dma((PIECES,)),
        ],
        compiler_params=pltpu.CompilerParams(has_side_effects=True, collective_id=1, vmem_limit_bytes=LIMIT),
        name="mix",
    )(local(part))


def on_device(
    n_kv,
    n_tp,
    candidate_embeddings,
    incoming_rms_scaling,
    probe_projector,
    address_projector,
    content_projector,
    sigmoid_mask_matrix,
    forgetting_projector,
    strength_projector_matrix,
    channel_forgetting_rates,
    forgetting_offset,
    extra_forgetting,
    outgoing_rms_scaling,
    final_projector,
    memory_matrix,
    earlier_addresses,
    earlier_contents,
    earlier_strengths,
    earlier_forgetting,
    admitted_counts,
):
    rows, local_cols = candidate_embeddings.shape
    features = incoming_rms_scaling.shape[0]
    depth, width = probe_projector.shape
    heads = width // DK
    seqs = rows // P_SIZE
    k_index, t_index = lax.axis_index("kv"), lax.axis_index("tp")

    def thin(values):
        return values.transpose(1, 2, 0).reshape(P_SIZE * heads, seqs)

    weights = (probe_projector, address_projector, content_projector, sigmoid_mask_matrix)
    fade, pull, extra = thin(earlier_forgetting), thin(earlier_strengths), thin(extra_forgetting)
    if n_kv == 4 and n_tp == 4:
        last, small, taken, columns, flat = project(
            candidate_embeddings, incoming_rms_scaling, weights, forgetting_projector, strength_projector_matrix,
            final_projector, memory_matrix, earlier_addresses, earlier_contents, fade, pull, admitted_counts.reshape(1, seqs), extra,
            channel_forgetting_rates, forgetting_offset, outgoing_rms_scaling,
        )
        part, taken = last_head(small, outgoing_rms_scaling, last, taken, flat, columns)
        mixed = mix(part)
    else:
        every = lax.all_gather(candidate_embeddings, "tp", axis=1, tiled=True)
        every = lax.all_to_all(every, "kv", split_axis=1, concat_axis=0, tiled=True)
        gain_part = lax.dynamic_slice_in_dim(incoming_rms_scaling, k_index * depth, depth)
        floated = every.astype(f32)
        gained = (floated * gain_part).astype(bf16)
        decay_cols = lax.dynamic_slice(forgetting_projector, (k_index * depth, t_index * heads), (depth, heads))
        beta_cols = lax.dynamic_slice(strength_projector_matrix, (k_index * depth, t_index * heads), (depth, heads))
        few = jnp.concatenate(
            [
                jnp.dot(gained, jnp.concatenate([decay_cols, beta_cols], axis=1), preferred_element_type=f32),
                jnp.sum(floated * floated, axis=1, keepdims=True),
            ],
            axis=1,
        )
        few = lax.psum_scatter(few, "kv", scatter_dimension=0, tiled=True)
        few = jnp.pad(few, ((0, 0), (0, 7))).T
        partial = jnp.stack([jnp.dot(gained, w, preferred_element_type=f32).astype(bf16) for w in weights])
        summed = lax.psum_scatter(partial, "kv", scatter_dimension=1, tiled=True).astype(f32)
        counts = admitted_counts.astype(f32).reshape(seqs, 1)
        keys, values = earlier_addresses.reshape(rows, width), earlier_contents.reshape(rows, width)
        taken = accepted(memory_matrix, keys, values, jnp.concatenate([fade.T, pull.T, counts], axis=1))
        flat, taken = attend(
            features, taken, summed, few, extra, channel_forgetting_rates, forgetting_offset, outgoing_rms_scaling
        )
        gathered = lax.all_gather(flat, "kv", axis=0, tiled=True)
        terms = jnp.dot(gathered, final_projector, preferred_element_type=f32).astype(bf16)
        terms = lax.all_to_all(terms, "kv", split_axis=0, concat_axis=1, tiled=True)
        mixed = lax.psum_scatter(terms, "tp", scatter_dimension=1, tiled=True)
    return (mixed, taken)


def solution(mesh):
    row, per_head = P(("grp", "kv"), "tp"), P(("grp", "kv"), None, "tp")
    four = P(("grp", "kv"), None, "tp", None)
    weight = P("kv", "tp")
    state = P(("grp", "kv"), "tp", None, None)
    in_specs = (
        row, P(), weight, weight, weight, weight, P(), P(), P("tp"), P("tp"), per_head, P(),
        P("tp", "kv"), state, four, four, per_head, per_head, P(("grp", "kv")),
    )
    body = functools.partial(on_device, mesh.shape["kv"], mesh.shape["tp"])
    return jax.shard_map(body, mesh=mesh, in_specs=in_specs, out_specs=(row, state), check_vma=False)
```

```python
import functools

import jax
import jax.numpy as jnp
from jax import lax
from jax.experimental import pallas as pl
from jax.experimental.pallas import tpu as pltpu
from jax.sharding import PartitionSpec as P

DK = 128
P_SIZE = 4
SB = 8
TALL = SB * P_SIZE
epsilon = 1e-06
LIMIT = 42 * 2**20
f32 = jnp.float32
bf16 = jnp.bfloat16


def lane_dot(a, b):
    return jnp.sum(a * b, axis=-1, keepdims=True)


def first_half():
    return lax.broadcasted_iota(jnp.int32, (8, DK), 0) < P_SIZE


def load_heads(heads, src, dst, factor=None):
    if len(src.shape) == 4:
        block = src[...].astype(f32)
        for h in range(heads):
            dst[pl.ds(h * TALL, TALL), :] = block[:, :, h, :].reshape(TALL, DK)
        return
    for h in range(heads):
        part = src[:, h * DK : (h + 1) * DK].astype(f32)
        dst[pl.ds(h * TALL, TALL), :] = part if factor is None else (part * factor).astype(bf16).astype(f32)


def tile(h, pair):
    return pl.ds(h * TALL + pair * 8, 8)


def proposal(h, p):
    return pl.ds(h * TALL + p, SB, stride=P_SIZE)


def rows_to_columns(wide):
    count = wide.shape[1]
    same = lax.broadcasted_iota(jnp.int32, (count, count), 0) == lax.broadcasted_iota(jnp.int32, (count, count), 1)
    return lax.dot_general(
        same.astype(f32), wide, (((1,), (1,)), ((), ())),
        precision=lax.Precision.HIGHEST, preferred_element_type=f32,
    )


def accepted_kernel(heads, s_ref, k_ref, v_ref, n_ref, o_ref, r_scr, u_scr, c_scr, kf, vf):
    load_heads(heads, k_ref, kf)
    load_heads(heads, v_ref, vf)
    low = first_half()
    for pair in range(SB // 2):
        for h in range(heads):
            at = tile(h, pair)
            lhs = kf[at, :].astype(bf16)
            r0 = jnp.dot(lhs, s_ref[2 * pair, h].astype(bf16), preferred_element_type=f32)
            r1 = jnp.dot(lhs, s_ref[2 * pair + 1, h].astype(bf16), preferred_element_type=f32)
            r_scr[at, :] = jnp.where(low, r0, r1)
    few = n_ref[...]
    span = P_SIZE * heads
    count = few[:, 2 * span : 2 * span + 1]
    for h in range(heads):
        scale = jnp.ones((SB, 1), f32)
        ks, us, norms = [], [], []
        for p in range(P_SIZE):
            at = proposal(h, p)
            col = slice(p * heads + h, p * heads + h + 1)
            key = kf[at, :]
            norm = lax.rsqrt(lane_dot(key, key) + epsilon)
            live = count > float(p)
            g = jnp.where(live, jnp.exp(few[:, p * heads + h : p * heads + h + 1]), 1.0)
            b = jnp.where(live, few[:, span + p * heads + h : span + p * heads + h + 1], 0.0)
            rec = (scale * norm) * r_scr[at, :]
            for ki, ui, ni in zip(ks, us, norms):
                rec = rec + (lane_dot(ki, key) * (ni * norm)) * ui
            us = [ui * g for ui in us]
            scale = scale * g
            us.append(b * (vf[at, :] - g * rec))
            ks.append(key)
            norms.append(norm)
        for p in range(P_SIZE):
            u_scr[proposal(h, p), :] = us[p] * norms[p]
        c_scr[pl.ds(h * SB, SB), :] = jnp.broadcast_to(scale, (SB, DK))
    for pair in range(SB // 2):
        for h in range(heads):
            at = tile(h, pair)
            key = kf[at, :]
            lhs = jnp.concatenate([key, key], axis=0).astype(bf16)
            u = u_scr[at, :]
            hi = u.astype(bf16).astype(f32)
            lo = u - hi
            for half in range(2):
                keep = low if half == 0 else jnp.logical_not(low)
                rhs = jnp.concatenate([jnp.where(keep, hi, 0.0), jnp.where(keep, lo, 0.0)], axis=0).astype(bf16)
                seq = 2 * pair + half
                add = lax.dot_general(lhs, rhs, (((0,), (0,)), ((), ())), preferred_element_type=f32)
                o_ref[seq, h] = c_scr[pl.ds(h * SB + seq, 1), :] * s_ref[seq, h] + add


def attend_items(items, scratch, load, factor, state_at, scalars, gain, emit):
    rk, rq, qf, kf, vf, zf, of = scratch
    low = first_half()
    for j, item in enumerate(items):
        for n, dst in enumerate((qf, kf, vf, zf)):
            dst[pl.ds(j * TALL, TALL), :] = (load(item, n) * factor(item)).astype(bf16).astype(f32)
    for pair in range(SB // 2):
        for j, item in enumerate(items):
            at = tile(j, pair)
            lhs = jnp.concatenate([kf[at, :], qf[at, :]], axis=0).astype(bf16)
            r0 = jnp.dot(lhs, state_at(item, 2 * pair).astype(bf16), preferred_element_type=f32)
            r1 = jnp.dot(lhs, state_at(item, 2 * pair + 1).astype(bf16), preferred_element_type=f32)
            rk[at, :] = jnp.where(low, r0[:8], r1[:8])
            rq[at, :] = jnp.where(low, r0[8:], r1[8:])
    for j, item in enumerate(items):
        scale = jnp.ones((SB, 1), f32)
        ks, us, norms = [], [], []
        for p in range(P_SIZE):
            at = proposal(j, p)
            g, strength = scalars(item, p)
            key = kf[at, :]
            query = qf[at, :]
            norm = lax.rsqrt(lane_dot(key, key) + epsilon)
            qnorm = lax.rsqrt(lane_dot(query, query) + epsilon) * DK ** (-0.5)
            rec = (scale * norm) * rk[at, :]
            for ki, ui, ni in zip(ks, us, norms):
                rec = rec + (lane_dot(ki, key) * (ni * norm)) * ui
            us = [ui * g for ui in us]
            scale = scale * g
            us.append(strength * (vf[at, :] - g * rec))
            ks.append(key)
            norms.append(norm)
            att = (scale * qnorm) * rq[at, :]
            for ki, ui, ni in zip(ks, us, norms):
                att = att + (lane_dot(ki, query) * (ni * qnorm)) * ui
            gate = zf[at, :]
            mean = jnp.sum(att * att, axis=-1, keepdims=True) / DK
            of[at, :] = att * lax.rsqrt(mean + epsilon) * gain * (gate * jax.nn.sigmoid(gate))
    for j, item in enumerate(items):
        emit(item, of[pl.ds(j * TALL, TALL), :].astype(bf16))


def small_terms(heads, features, few_wide, extra, rates, offset, thin):
    rows = few_wide.shape[1]
    few = rows_to_columns(few_wide)
    factor = lax.rsqrt(few[:, 2 * heads : 2 * heads + 1] / features + epsilon)
    seqs = extra.shape[1]
    row = lax.broadcasted_iota(jnp.int32, (rows, seqs), 0)
    owner = jnp.right_shift(row, 2) == lax.broadcasted_iota(jnp.int32, (rows, seqs), 1)
    spread = lax.dot_general(
        owner.astype(f32), extra, (((1,), (1,)), ((), ())),
        precision=lax.Precision.HIGHEST, preferred_element_type=f32,
    )
    turn = jnp.bitwise_and(lax.broadcasted_iota(jnp.int32, (rows, heads), 0), 3)
    struck = pick(turn, [spread[:, p * heads : (p + 1) * heads] for p in range(P_SIZE)])
    raised = few[:, :heads] * factor + offset
    soft = jnp.maximum(raised, 0.0) + jnp.log1p(jnp.exp(-jnp.abs(raised)))
    thin[:, :heads] = jnp.exp(struck - jnp.exp(rates) * soft)
    thin[:, heads : 2 * heads] = jax.nn.sigmoid(few[:, heads : 2 * heads] * factor)
    thin[:, 2 * heads : 2 * heads + 1] = factor


def attend_kernel(heads, features, few_ref, extra_ref, rate_ref, offset_ref, w_ref, parts, state, o_ref, kept, thin, *rest):
    scratch, done = rest[:-1], rest[-1]
    keep = pltpu.make_async_copy(state, kept, done)
    keep.start()
    small_terms(heads, features, few_ref[...], extra_ref[...], rate_ref[...], offset_ref[...], thin)

    def block(i, carry):
        base = i * TALL
        tall = pl.ds(base, TALL)

        def scalars(h, p):
            both = thin[pl.ds(base + p, SB, stride=P_SIZE), :]
            return both[:, h : h + 1], both[:, heads + h : heads + h + 1]

        def emit(h, value):
            o_ref[tall, h * DK : (h + 1) * DK] = value

        attend_items(
            range(heads), scratch,
            lambda h, n: parts[n, tall, h * DK : (h + 1) * DK],
            lambda h: thin[tall, 2 * heads : 2 * heads + 1],
            lambda h, seq: state[i * SB + seq, h],
            scalars, w_ref[...], emit,
        )
        return carry

    lax.fori_loop(0, state.shape[0] // SB, block, 0)
    keep.wait()


GROUP = 3


def attend_head(h, heads, blocks, scratch, parts_at, thin, state, gain, flat):
    def group(it, carry):
        def tall(j):
            return pl.ds((it * GROUP + j) * TALL, TALL)

        def scalars(j, p):
            both = thin[pl.ds((it * GROUP + j) * TALL + p, SB, stride=P_SIZE), :]
            return both[:, h : h + 1], both[:, heads + h : heads + h + 1]

        def emit(j, value):
            flat[tall(j), h * DK : (h + 1) * DK] = value

        attend_items(
            range(GROUP), scratch,
            lambda j, n: parts_at(tall(j), n),
            lambda j: thin[tall(j), 2 * heads : 2 * heads + 1],
            lambda j, seq: state[(it * GROUP + j) * SB + seq, h],
            scalars, gain, emit,
        )
        return carry

    lax.fori_loop(0, blocks // GROUP, group, 0)


def last_kernel(heads, thin, w_ref, parts, state, some, columns, o_ref, kept, flat, *rest):
    scratch, done = rest[:-1], rest[-1]
    keep = pltpu.make_async_copy(state, kept, done)
    keep.start()
    flat[...] = some[...]
    blocks = state.shape[0] // SB
    attend_head(
        heads - 1, heads, blocks, scratch, lambda at, n: parts[at, n * DK : (n + 1) * DK], thin, state, w_ref[...], flat
    )
    for c in range(columns.shape[0]):
        o_ref[c] = jnp.dot(flat[...], columns[c], preferred_element_type=f32).astype(bf16)
    keep.wait()


def accepted(state, keys, values, few):
    seqs, heads = state.shape[:2]
    width = heads * DK
    rows = TALL
    tall = pl.BlockSpec((rows, width), lambda i: (i, 0))
    thin = pl.BlockSpec((SB, few.shape[1]), lambda i: (i, 0))
    block = pl.BlockSpec((SB, heads, DK, DK), lambda i: (i, 0, 0, 0))
    return pl.pallas_call(
        functools.partial(accepted_kernel, heads),
        grid=(seqs // SB,),
        in_specs=[block, tall, tall, thin],
        out_specs=block,
        out_shape=jax.ShapeDtypeStruct(state.shape, f32),
        scratch_shapes=[pltpu.VMEM((heads * n, DK), f32) for n in (TALL, TALL, SB, TALL, TALL)],
        cost_estimate=pl.CostEstimate(flops=10_000_000_000, bytes_accessed=2 * state.size * 4, transcendentals=0),
        name="accepted",
    )(state, keys, values, few)


def local(array):
    return pltpu.with_memory_space_constraint(array, pltpu.VMEM)


def attend(features, state, parts, few, extra, rates, offset, gain):
    seqs, heads = state.shape[:2]
    rows, width = parts.shape[1:]
    vmem = pl.BlockSpec(memory_space=pltpu.VMEM)
    return pl.pallas_call(
        functools.partial(attend_kernel, heads, features),
        in_specs=[vmem] * 7,
        out_specs=[vmem, pl.BlockSpec(memory_space=pl.ANY)],
        out_shape=[pltpu.VMEM((rows, width), bf16), jax.ShapeDtypeStruct(state.shape, f32)],
        scratch_shapes=[
            pltpu.VMEM((rows, 2 * heads + 8), f32),
            *[pltpu.VMEM((heads * TALL, DK), f32)] * 7,
            pltpu.SemaphoreType.DMA,
        ],
        compiler_params=pltpu.CompilerParams(vmem_limit_bytes=LIMIT),
        cost_estimate=pl.CostEstimate(flops=5_000_000_000, bytes_accessed=state.size * 4, transcendentals=0),
        name="attend",
    )(
        local(few), extra, rates.reshape(1, heads), offset.reshape(1, heads), gain.reshape(1, DK),
        local(parts), local(state),
    )


def pick(index, values):
    chosen = values[-1]
    for at, value in enumerate(values[:-1]):
        chosen = jnp.where(index == at, value, chosen)
    return chosen


def last_head(thin, gain, parts, state, some, columns):
    seqs, heads = state.shape[:2]
    rows, width = some.shape
    vmem = pl.BlockSpec(memory_space=pltpu.VMEM)
    return pl.pallas_call(
        functools.partial(last_kernel, heads),
        in_specs=[vmem] * 6,
        out_specs=[vmem, pl.BlockSpec(memory_space=pl.ANY)],
        out_shape=[
            pltpu.VMEM((columns.shape[0], rows, columns.shape[2]), bf16),
            jax.ShapeDtypeStruct(state.shape, f32),
        ],
        scratch_shapes=[
            pltpu.VMEM((rows, width), bf16),
            *[pltpu.VMEM((GROUP * TALL, DK), f32)] * 7,
            pltpu.SemaphoreType.DMA,
        ],
        compiler_params=pltpu.CompilerParams(vmem_limit_bytes=LIMIT),
        cost_estimate=pl.CostEstimate(flops=5_000_000_000, bytes_accessed=state.size * 4, transcendentals=0),
        name="last_head",
    )(local(thin), gain.reshape(1, DK), local(parts), local(state), local(some), local(columns))


def turned_slot(t):
    return pick(t, (0, 2, 1, 3))


def project_kernel(x_hbm, gain_hbm, keys_hbm, values_hbm, fade_hbm, pull_hbm, count_hbm, extra_hbm, rate_hbm, offset_hbm,
                   outer_hbm, wf, ws, wq, wk, wv, wz, wo, state, last, small, taken, fbuf, flat,
                   x_ref, gain_ref, keys, values, fade, pull, counts, extra, rates, offset, outer, fs, thin, few_ref, acc,
                   xpre, xbuf, gbuf, w, sbuf, abuf, bbuf, cbuf, esend, erecv, s_in,
                   r_scr, u_scr, c_scr, kf, vf, a0, a1, a2, a3, a4, a5, a6,
                   lsem, xs, xp, xr, wsem, ss, ar, br, cr, es, er, ins, fsem, fss, fzr, fys, fyr):
    k, t, g = lax.axis_index("kv"), lax.axis_index("tp"), lax.axis_index("grp")
    depth, width = w.shape[1], w.shape[2]
    features = gain_ref.shape[0] * depth
    rows = x_ref.shape[0]
    blocks = state.shape[0] // SB
    heads = state.shape[1]

    def remote(src, dst, send, recv, kv, tp, grp=g):
        return pltpu.make_async_remote_copy(
            src, dst, send, recv, device_id={"grp": grp, "kv": kv, "tp": tp}, device_id_type=pl.DeviceIdType.MESH
        )

    here = pl.ds(k * depth, depth)
    locals_ = [
        pltpu.make_async_copy(src, dst, lsem.at[n])
        for n, (src, dst) in enumerate(
            (
                (x_hbm, x_ref), (gain_hbm, gain_ref), (keys_hbm, keys), (values_hbm, values), (fade_hbm, fade),
                (pull_hbm, pull), (count_hbm, counts), (extra_hbm, extra), (rate_hbm, rates), (offset_hbm, offset), (outer_hbm, outer),
                (wf.at[:, here], fs.at[0]), (ws.at[:, here], fs.at[1]),
            )
        )
    ]
    for load in locals_:
        load.start()
    f_load = pltpu.make_async_copy(wo, fbuf.at[k], fsem)
    f_load.start()
    loads = [
        pltpu.make_async_copy(
            src.at[:, pl.ds(h * DK, DK)], w.at[h, :, pl.ds(n * DK, DK)], wsem.at[h * 4 + n]
        )
        for h in range(heads)
        for n, src in enumerate((wq, wk, wv, wz))
    ]
    for load in loads:
        load.start()

    def fetch(i):
        return pltpu.make_async_copy(state.at[pl.ds(i * SB, SB)], s_in.at[i % 2], ins.at[i % 2])

    fetch(0).start()

    beside = t + 1 - 2 * (t % 2)
    across = (t + 2) % 4
    corner = t % 2
    landing = 2 * (t // 2) + k % 2
    home = corner == k % 2
    top_kind = t // 2 == k // 2
    source = jnp.where(top_kind, k, (k + 2) % 4)
    near_src = jnp.where(k <= 1, corner, corner + 2)
    far_src = jnp.where(k <= 1, corner + 2, corner)
    barrier = pltpu.get_barrier_semaphore()

    def greet(kv, tp, grp=g):
        pl.semaphore_signal(
            barrier, inc=1, device_id={"grp": grp, "kv": kv, "tp": tp}, device_id_type=pl.DeviceIdType.MESH
        )

    greet(k, beside)
    greet(k, across)
    greet(k, t, 1 - g)
    for step in range(1, 4):
        greet((k + step) % 4, t)

    @pl.when(t != k)
    def _():
        greet(t, landing)

    @pl.when(across != k)
    def _():
        greet(across, landing)

    @pl.when(near_src != k)
    def _():
        greet(near_src, source)

    @pl.when(far_src != k)
    def _():
        greet(far_src, source)

    @pl.when(home)
    def _():
        pl.semaphore_wait(barrier, 8)

    @pl.when(jnp.logical_not(home))
    def _():
        pl.semaphore_wait(barrier, 10)

    quarter = rows // 4
    locals_[0].wait()

    def part(q):
        return pl.ds(q * quarter, quarter)

    def forward(q):
        return remote(xpre.at[q], xbuf.at[k, part(2 + q)], xs.at[4 + q], xr.at[k, 2 + q], across, landing)

    def outward(q):
        return remote(x_ref.at[part(q)], xbuf.at[k, part(q)], xs.at[2 + q], xr.at[k, q], t, landing)

    def settled_copy(q):
        return pltpu.make_async_copy(x_ref.at[part(q)], xbuf.at[k, part(q)], xr.at[k, q])

    def sideways(q):
        return remote(x_ref.at[part(2 + q)], xpre.at[q], xs.at[q], xp.at[q], k, across)

    @pl.when(t == k)
    def _():
        for q in range(2):
            remote(x_ref.at[part(2 + q)], xbuf.at[k, part(2 + q)], xs.at[q], xr.at[k, 2 + q], k, across).start()
        for q in range(2):
            settled_copy(q).start()

    @pl.when(t != k)
    def _():
        for q in range(2):
            sideways(q).start()
        for q in range(2):
            outward(q).start()

    @pl.when(across != k)
    def _():
        for q in range(2):
            sideways(q).wait_recv()
            forward(q).start()

    end = jnp.where(k <= 1, 0, 3)
    near = jnp.where(k <= 1, 1, 2)
    is_end = k == end
    inside = jnp.logical_not(is_end)
    kind = jnp.where(top_kind, 0, 1)

    def piece(r, q, send, tp):
        at = pl.ds(q * quarter, quarter)
        return remote(xbuf.at[r, at], xbuf.at[r, at], xs.at[send], xr.at[r, q], k, tp)

    def spread(r, n, q):
        settled = jnp.logical_and(t == k, r == k)

        @pl.when(settled)
        def _():
            settled_copy(q).wait()

        @pl.when(jnp.logical_not(settled))
        def _():
            piece(r, 2 * kind + q, 6, across).wait_recv()

        piece(r, 2 * kind + q, 6 + n, across).start()
        piece(r, 2 * kind + q, 10 + n, beside).start()

    half_rows = fbuf.shape[1] // 2
    half = pl.ds(g * half_rows, half_rows)

    def f_pass(c, to, sem):
        return remote(fbuf.at[c, half], fbuf.at[c, half], fss.at[sem], fzr.at[c], to, t)

    def f_swap(c):
        return remote(fbuf.at[c, half], fbuf.at[c, half], fys.at[c], fyr.at[c], k, t, 1 - g)

    def f_begin():
        f_load.wait()

        @pl.when(k < 3)
        def _():
            f_pass(k, k + 1, 4).start()

        @pl.when(k > 0)
        def _():
            f_pass(k, k - 1, 5).start()

    pl.when(is_end)(f_begin)
    for q in range(2):
        spread(far_src, 2 * q + 1, q)
        spread(near_src, 2 * q, q)
    pl.when(inside)(f_begin)
    def cross_in(n, r):
        for q in range(2):
            piece(r, 2 - 2 * kind + q, 6, across).wait_recv()
            piece(r, 2 - 2 * kind + q, 14 + 2 * q + n, beside).start()

    def beside_in(r):
        for q in range(4):
            piece(r, q, 6, beside).wait_recv()

    near_mate = jnp.where(k <= 1, 1 - corner, 3 - corner)
    far_mate = jnp.where(k <= 1, 3 - corner, 1 - corner)
    cross_in(1, far_src)

    def f_forwards(c):
        return jnp.logical_or(jnp.logical_and(c < k, k < 3), jnp.logical_and(c > k, k > 0))

    def f_take(c):
        to = jnp.where(c < k, k + 1, k - 1)
        f_pass(c, k, c).wait_recv()

        @pl.when(f_forwards(c))
        def _():
            f_pass(c, to, c).start()

        f_swap(c).start()

    f_order = (jnp.where(is_end, near, end), 3 - near, 3 - end)

    for load in locals_[1:]:
        load.wait()
    thin[...] = rows_to_columns(
        jnp.concatenate([fade[...], pull[...], jnp.broadcast_to(counts[...].astype(f32), (8, counts.shape[1]))], axis=0)
    )
    for load in loads:
        load.wait()

    @pl.when(jnp.logical_or(inside, far_mate == 3 - end))
    def _():
        beside_in(far_mate)

    @pl.when(inside)
    def _():
        cross_in(0, near_src)
        beside_in(near_mate)

    nt = (((1,), (1,)), ((), ()))

    def prepare(r):
        floated = xbuf[r].astype(f32)
        gained = (floated * gain_ref[k]).astype(bf16)
        gbuf[r] = gained
        squares = floated * floated
        high = squares.astype(bf16)
        rest = (squares - high.astype(f32)).astype(bf16)
        ones = jnp.ones((8, depth), bf16)
        for n in range(2):
            every = lax.dot_general(fs[n], gained, nt, preferred_element_type=f32)
            esend[r, n * heads : (n + 1) * heads, :] = pick(t, [every[m * heads : (m + 1) * heads] for m in range(4)])
        esend[r, 2 * heads :, :] = lax.dot_general(ones, high, nt, preferred_element_type=f32) + lax.dot_general(
            ones, rest, nt, preferred_element_type=f32
        )

        @pl.when(r != k)
        def _():
            remote(esend.at[r], erecv.at[k], es.at[r], er.at[k], r, t).start()

    def product(r, c):
        return jnp.dot(gbuf[r], w[c], preferred_element_type=f32)

    def from_end(i):
        remote(abuf.at[i], abuf.at[i], ss.at[i], ar.at[i], k, beside).wait_recv()
        return abuf[i].astype(f32)

    def from_inner(i):
        remote(bbuf.at[i], bbuf.at[i], ss.at[i], br.at[i], k, beside).wait_recv()
        return bbuf[i].astype(f32)

    def accept(i):
        @pl.when(i + 1 < blocks)
        def _():
            fetch(i + 1).start()

        fetch(i).wait()

        few_rows = pl.ds(i * SB, SB)
        accepted_kernel(
            heads, s_in.at[i % 2], keys.at[few_rows], values.at[few_rows], thin.at[few_rows], taken.at[few_rows],
            r_scr, u_scr, c_scr, kf, vf,
        )

    def accept_some(low, high):
        def one(i, carry):
            accept(i)
            return carry

        lax.fori_loop(low, high, one, 0)

    chunk_head, chunk_stage = (0, 1, 0, 0, 2, 1, 1, 3, 2, 3, 2, 3), (0, 0, 1, 2, 0, 1, 2, 0, 1, 1, 2, 2)
    prepared = (3 - end, end, 3 - near, near)
    late = (3 - end, end, 3 - near, near, end)

    def settle_small():
        few_ref[...] = esend[k]
        for src in range(4):

            @pl.when(k != src)
            def _():
                remote(esend.at[src], erecv.at[src], es.at[src], er.at[src], k, beside).wait()
                few_ref[...] += erecv[src]

        small_terms(heads, features, few_ref[...], extra[...], rates[...], offset[...], small)

    def attention(h):
        attend_head(
            h, heads, blocks, (a0, a1, a2, a3, a4, a5, a6),
            lambda at, n: acc[h, at, n * DK : (n + 1) * DK], small, taken, outer[...], flat,
        )

    @pl.when(inside)
    def _():
        def one(i, carry):
            prepare(pick(i, prepared))
            return carry

        lax.fori_loop(0, 4, one, 0)
        accept_some(0, blocks // 2)
        f_take(f_order[0])
        f_take(f_order[1])

    def step(i, carry):
        h, stage = pick(i, chunk_head), pick(i, chunk_stage)
        r = pick(stage, (3 - end, 3 - near, near))

        @pl.when(jnp.logical_and(is_end, i == 2))
        def _():
            cross_in(0, near_src)

            @pl.when(far_mate != 3 - end)
            def _():
                beside_in(far_mate)

            beside_in(near_mate)

        @pl.when(jnp.logical_and(is_end, jnp.logical_and(i < 5, i != 1)))
        def _():
            prepare(pick(i, late))

        @pl.when(is_end)
        def _():
            sbuf[i] = product(r, h).astype(bf16)
            remote(sbuf.at[i], abuf.at[i], ss.at[i], ar.at[i], near, t).start()

        @pl.when(jnp.logical_and(inside, stage < 2))
        def _():
            part = product(r, h)
            sbuf[i] = (part + from_end(i)).astype(bf16)
            remote(sbuf.at[i], bbuf.at[i], ss.at[i], br.at[i], 3 - near, t).start()

        @pl.when(jnp.logical_and(inside, i == 0))
        def _():
            accept_some(blocks // 2, blocks * 2 // 3)

        @pl.when(jnp.logical_and(inside, i == 1))
        def _():
            accept_some(blocks * 2 // 3, blocks)

        @pl.when(jnp.logical_and(inside, i == 3))
        def _():
            f_take(f_order[2])

        back = jnp.logical_or(jnp.logical_or(i == 3, i == 4), jnp.logical_or(i == 6, i == 9))

        @pl.when(jnp.logical_and(inside, back))
        def _():
            m = jnp.where(i <= 4, i - 3, i // 3)
            part = product(end, m)
            sbuf[12 + m] = (part + from_inner(pick(m, (0, 1, 4, 7)))).astype(bf16)
            remote(sbuf.at[12 + m], cbuf.at[m], ss.at[12 + m], cr.at[m], end, t).start()

        @pl.when(jnp.logical_and(inside, i == 5))
        def _():
            settle_small()

        ready = jnp.logical_or(jnp.logical_or(i == 5, i == 8), i == 10)

        @pl.when(jnp.logical_and(inside, ready))
        def _():
            m = i // 3 - 1
            acc[m] = product(near, m) + from_inner(pick(m, (2, 5, 8))) + from_end(pick(m, (3, 6, 10)))

        for m in range(3):

            @pl.when(jnp.logical_and(inside, i == (5, 8, 10)[m]))
            def _():
                attention(m)

        @pl.when(jnp.logical_and(inside, i == 11))
        def _():
            last[...] = product(near, 3) + from_inner(9) + from_end(11)

        return carry

    lax.fori_loop(0, 12, step, 0)

    @pl.when(is_end)
    def _():
        f_take(f_order[0])
        accept_some(0, blocks)
        settle_small()
        f_take(f_order[1])

        def returned(m):
            part = product(end, m)
            remote(cbuf.at[m], cbuf.at[m], ss.at[m], cr.at[m], k, beside).wait_recv()
            return part + cbuf[m].astype(f32)

        for m in range(3):
            acc[m] = returned(m)
            attention(m)
            if m == 0:
                f_take(f_order[2])
        last[...] = returned(3)

    for src in range(4):

        @pl.when(k != src)
        def _():
            remote(fbuf.at[src, half], fbuf.at[src, half], fys.at[src], fyr.at[src], k, beside).wait()

    for q in range(2):
        sideways(q).wait_send()

    @pl.when(t != k)
    def _():
        for q in range(2):
            outward(q).wait_send()

    @pl.when(across != k)
    def _():
        for q in range(2):
            forward(q).wait_send()

    for n in range(12):
        piece(k, 0, 6 + n, beside).wait_send()

    @pl.when(k < 3)
    def _():
        f_pass(k, k, 4).wait_send()

    @pl.when(k > 0)
    def _():
        f_pass(k, k, 5).wait_send()

    for src in range(4):

        @pl.when(jnp.logical_and(k != src, f_forwards(src)))
        def _():
            f_pass(src, k, src).wait_send()

    for i in range(12):

        @pl.when(is_end if chunk_stage[i] == 2 else k >= 0)
        def _():
            remote(sbuf.at[i], abuf.at[i], ss.at[i], ar.at[i], k, beside).wait_send()

    for m in range(4):

        @pl.when(inside)
        def _():
            remote(sbuf.at[12 + m], cbuf.at[m], ss.at[12 + m], cr.at[m], end, t).wait_send()


def project(x, gain, weights, forgetting, strength, final, state, keys, values, fade, pull, counts, extra, rates, offset, outer):
    rows, depth = x.shape
    width = weights[0].shape[1]
    seqs, heads = state.shape[:2]
    few_rows = 2 * heads + 8
    vmem, hbm = pl.BlockSpec(memory_space=pltpu.VMEM), pl.BlockSpec(memory_space=pl.ANY)
    dma = pltpu.SemaphoreType.DMA
    gain = gain.reshape(-1, 1, depth)
    rates, offset, outer = rates.reshape(1, heads), offset.reshape(1, heads), outer.reshape(1, DK)
    forgetting, strength = forgetting.T, strength.T

    def chunks(n):
        return pltpu.VMEM((n, rows, width), bf16)

    def like(a):
        return pltpu.VMEM(a.shape, a.dtype)

    return pl.pallas_call(
        project_kernel,
        in_specs=[hbm] * 19,
        out_specs=[vmem] * 5,
        out_shape=[
            pltpu.VMEM((rows, width), f32),
            pltpu.VMEM((rows, few_rows), f32),
            pltpu.VMEM(state.shape, f32),
            pltpu.VMEM((4,) + final.shape, bf16),
            pltpu.VMEM((rows, width), bf16),
        ],
        scratch_shapes=[
            like(x), like(gain), like(keys), like(values), like(fade), like(pull), like(counts),
            like(extra), like(rates), like(offset), like(outer),
            pltpu.VMEM((2, forgetting.shape[0], depth), bf16),
            pltpu.VMEM((seqs, 2 * P_SIZE * heads + 8), f32),
            pltpu.VMEM((few_rows, rows), f32),
            pltpu.VMEM((3, rows, width), f32),
            pltpu.VMEM((2, rows // 4, depth), bf16),
            pltpu.VMEM((4, rows, depth), bf16),
            pltpu.VMEM((4, rows, depth), bf16),
            pltpu.VMEM((4, depth, width), bf16),
            chunks(16), chunks(12), chunks(12), chunks(4),
            pltpu.VMEM((4, few_rows, rows), f32),
            pltpu.VMEM((4, few_rows, rows), f32),
            pltpu.VMEM((2, SB) + state.shape[1:], f32),
            *[pltpu.VMEM((heads * n, DK), f32) for n in (TALL, TALL, SB, TALL, TALL)],
            *[pltpu.VMEM((GROUP * TALL, DK), f32)] * 7,
            dma((13,)), dma((18,)), dma((2,)), dma((4, 4)), dma((16,)), dma((16,)), dma((12,)), dma((12,)), dma((4,)), dma((4,)),
            dma((4,)), dma((2,)), dma, dma((6,)), dma((4,)), dma((4,)), dma((4,)),
        ],
        compiler_params=pltpu.CompilerParams(has_side_effects=True, collective_id=0, vmem_limit_bytes=LIMIT),
        name="project",
    )(x, gain, keys, values, fade, pull, counts, extra, rates, offset, outer, forgetting, strength, *weights, final, state)


PIECES = 3


def mix_kernel(part, o_ref, mate, sent, cross, ms, mr, xs, xr):
    k, t, g = lax.axis_index("kv"), lax.axis_index("tp"), lax.axis_index("grp")
    rows = part.shape[1]
    piece = rows // PIECES
    beside = t + 1 - 2 * (t % 2)
    across = (t + 2) % 4
    order = ((beside + 2) % 4, beside)

    def remote(src, dst, send, recv, tp):
        return pltpu.make_async_remote_copy(
            src, dst, send, recv, device_id={"grp": g, "kv": k, "tp": tp}, device_id_type=pl.DeviceIdType.MESH
        )

    barrier = pltpu.get_barrier_semaphore()
    for peer in (beside, across):
        pl.semaphore_signal(
            barrier, inc=1, device_id={"grp": g, "kv": k, "tp": peer}, device_id_type=pl.DeviceIdType.MESH
        )
    pl.semaphore_wait(barrier, 2)

    def to_mate(n, s):
        at = pl.ds(s * piece, piece)
        return remote(part.at[order[n], at], mate.at[n, at], ms.at[n, s], mr.at[n, s], beside)

    def to_cross(s):
        at = pl.ds(s * piece, piece)
        return remote(sent.at[at], cross.at[at], xs.at[s], xr.at[s], across)

    for n in range(2):
        for s in range(PIECES):
            to_mate(n, s).start()
    for s in range(PIECES):
        at = slice(s * piece, (s + 1) * piece)
        to_mate(0, s).wait_recv()
        sent[at, :] = (part[across, at, :].astype(f32) + mate[0, at, :].astype(f32)).astype(bf16)
        to_cross(s).start()
    for s in range(PIECES):
        at = slice(s * piece, (s + 1) * piece)
        to_mate(1, s).wait_recv()
        to_cross(s).wait_recv()
        o_ref[at, :] = (
            part[t, at, :].astype(f32) + mate[1, at, :].astype(f32) + cross[at, :].astype(f32)
        ).astype(bf16)
    for s in range(PIECES):
        to_mate(0, s).wait_send()
        to_mate(1, s).wait_send()
        to_cross(s).wait_send()


def mix(part):
    rows, cols = part.shape[1:]
    vmem = pl.BlockSpec(memory_space=pltpu.VMEM)
    dma = pltpu.SemaphoreType.DMA
    return pl.pallas_call(
        mix_kernel,
        in_specs=[vmem],
        out_specs=vmem,
        out_shape=jax.ShapeDtypeStruct((rows, cols), bf16),
        scratch_shapes=[
            pltpu.VMEM((2, rows, cols), bf16),
            pltpu.VMEM((rows, cols), bf16),
            pltpu.VMEM((rows, cols), bf16),
            dma((2, PIECES)), dma((2, PIECES)), dma((PIECES,)), dma((PIECES,)),
        ],
        compiler_params=pltpu.CompilerParams(has_side_effects=True, collective_id=1, vmem_limit_bytes=LIMIT),
        name="mix",
    )(local(part))


def on_device(
    n_kv,
    n_tp,
    candidate_embeddings,
    incoming_rms_scaling,
    probe_projector,
    address_projector,
    content_projector,
    sigmoid_mask_matrix,
    forgetting_projector,
    strength_projector_matrix,
    channel_forgetting_rates,
    forgetting_offset,
    extra_forgetting,
    outgoing_rms_scaling,
    final_projector,
    memory_matrix,
    earlier_addresses,
    earlier_contents,
    earlier_strengths,
    earlier_forgetting,
    admitted_counts,
):
    rows, local_cols = candidate_embeddings.shape
    features = incoming_rms_scaling.shape[0]
    depth, width = probe_projector.shape
    heads = width // DK
    seqs = rows // P_SIZE
    k_index, t_index = lax.axis_index("kv"), lax.axis_index("tp")

    def thin(values):
        return values.transpose(1, 2, 0).reshape(P_SIZE * heads, seqs)

    weights = (probe_projector, address_projector, content_projector, sigmoid_mask_matrix)
    fade, pull, extra = thin(earlier_forgetting), thin(earlier_strengths), thin(extra_forgetting)
    if n_kv == 4 and n_tp == 4:
        last, small, taken, columns, flat = project(
            candidate_embeddings, incoming_rms_scaling, weights, forgetting_projector, strength_projector_matrix,
            final_projector, memory_matrix, earlier_addresses, earlier_contents, fade, pull, admitted_counts.reshape(1, seqs), extra,
            channel_forgetting_rates, forgetting_offset, outgoing_rms_scaling,
        )
        part, taken = last_head(small, outgoing_rms_scaling, last, taken, flat, columns)
        mixed = mix(part)
    else:
        every = lax.all_gather(candidate_embeddings, "tp", axis=1, tiled=True)
        every = lax.all_to_all(every, "kv", split_axis=1, concat_axis=0, tiled=True)
        gain_part = lax.dynamic_slice_in_dim(incoming_rms_scaling, k_index * depth, depth)
        floated = every.astype(f32)
        gained = (floated * gain_part).astype(bf16)
        decay_cols = lax.dynamic_slice(forgetting_projector, (k_index * depth, t_index * heads), (depth, heads))
        beta_cols = lax.dynamic_slice(strength_projector_matrix, (k_index * depth, t_index * heads), (depth, heads))
        few = jnp.concatenate(
            [
                jnp.dot(gained, jnp.concatenate([decay_cols, beta_cols], axis=1), preferred_element_type=f32),
                jnp.sum(floated * floated, axis=1, keepdims=True),
            ],
            axis=1,
        )
        few = lax.psum_scatter(few, "kv", scatter_dimension=0, tiled=True)
        few = jnp.pad(few, ((0, 0), (0, 7))).T
        partial = jnp.stack([jnp.dot(gained, w, preferred_element_type=f32).astype(bf16) for w in weights])
        summed = lax.psum_scatter(partial, "kv", scatter_dimension=1, tiled=True).astype(f32)
        counts = admitted_counts.astype(f32).reshape(seqs, 1)
        keys, values = earlier_addresses.reshape(rows, width), earlier_contents.reshape(rows, width)
        taken = accepted(memory_matrix, keys, values, jnp.concatenate([fade.T, pull.T, counts], axis=1))
        flat, taken = attend(
            features, taken, summed, few, extra, channel_forgetting_rates, forgetting_offset, outgoing_rms_scaling
        )
        gathered = lax.all_gather(flat, "kv", axis=0, tiled=True)
        terms = jnp.dot(gathered, final_projector, preferred_element_type=f32).astype(bf16)
        terms = lax.all_to_all(terms, "kv", split_axis=0, concat_axis=1, tiled=True)
        mixed = lax.psum_scatter(terms, "tp", scatter_dimension=1, tiled=True)
    return (mixed, taken)


def solution(mesh):
    row, per_head = P(("grp", "kv"), "tp"), P(("grp", "kv"), None, "tp")
    four = P(("grp", "kv"), None, "tp", None)
    weight = P("kv", "tp")
    state = P(("grp", "kv"), "tp", None, None)
    in_specs = (
        row, P(), weight, weight, weight, weight, P(), P(), P("tp"), P("tp"), per_head, P(),
        P("tp", "kv"), state, four, four, per_head, per_head, P(("grp", "kv")),
    )
    body = functools.partial(on_device, mesh.shape["kv"], mesh.shape["tp"])
    return jax.shard_map(body, mesh=mesh, in_specs=in_specs, out_specs=(row, state), check_vma=False)
```

```python
import functools

import jax
import jax.numpy as jnp
from jax import lax
from jax.experimental import pallas as pl
from jax.experimental.pallas import tpu as pltpu
from jax.sharding import PartitionSpec as P

DK = 128
P_SIZE = 4
SB = 8
TALL = SB * P_SIZE
epsilon = 1e-06
LIMIT = 42 * 2**20
f32 = jnp.float32
bf16 = jnp.bfloat16


def lane_dot(a, b):
    return jnp.sum(a * b, axis=-1, keepdims=True)


def first_half():
    return lax.broadcasted_iota(jnp.int32, (8, DK), 0) < P_SIZE


def load_heads(heads, src, dst, factor=None):
    if len(src.shape) == 4:
        block = src[...].astype(f32)
        for h in range(heads):
            dst[pl.ds(h * TALL, TALL), :] = block[:, :, h, :].reshape(TALL, DK)
        return
    for h in range(heads):
        part = src[:, h * DK : (h + 1) * DK].astype(f32)
        dst[pl.ds(h * TALL, TALL), :] = part if factor is None else (part * factor).astype(bf16).astype(f32)


def tile(h, pair):
    return pl.ds(h * TALL + pair * 8, 8)


def proposal(h, p):
    return pl.ds(h * TALL + p, SB, stride=P_SIZE)


def rows_to_columns(wide):
    count = wide.shape[1]
    same = lax.broadcasted_iota(jnp.int32, (count, count), 0) == lax.broadcasted_iota(jnp.int32, (count, count), 1)
    return lax.dot_general(
        same.astype(f32), wide, (((1,), (1,)), ((), ())),
        precision=lax.Precision.HIGHEST, preferred_element_type=f32,
    )


def accepted_kernel(heads, s_ref, k_ref, v_ref, n_ref, o_ref, r_scr, u_scr, c_scr, kf, vf):
    load_heads(heads, k_ref, kf)
    load_heads(heads, v_ref, vf)
    low = first_half()
    for pair in range(SB // 2):
        for h in range(heads):
            at = tile(h, pair)
            lhs = kf[at, :].astype(bf16)
            r0 = jnp.dot(lhs, s_ref[2 * pair, h].astype(bf16), preferred_element_type=f32)
            r1 = jnp.dot(lhs, s_ref[2 * pair + 1, h].astype(bf16), preferred_element_type=f32)
            r_scr[at, :] = jnp.where(low, r0, r1)
    few = n_ref[...]
    span = P_SIZE * heads
    count = few[:, 2 * span : 2 * span + 1]
    for h in range(heads):
        scale = jnp.ones((SB, 1), f32)
        ks, us, norms = [], [], []
        for p in range(P_SIZE):
            at = proposal(h, p)
            col = slice(p * heads + h, p * heads + h + 1)
            key = kf[at, :]
            norm = lax.rsqrt(lane_dot(key, key) + epsilon)
            live = count > float(p)
            g = jnp.where(live, jnp.exp(few[:, p * heads + h : p * heads + h + 1]), 1.0)
            b = jnp.where(live, few[:, span + p * heads + h : span + p * heads + h + 1], 0.0)
            rec = (scale * norm) * r_scr[at, :]
            for ki, ui, ni in zip(ks, us, norms):
                rec = rec + (lane_dot(ki, key) * (ni * norm)) * ui
            us = [ui * g for ui in us]
            scale = scale * g
            us.append(b * (vf[at, :] - g * rec))
            ks.append(key)
            norms.append(norm)
        for p in range(P_SIZE):
            u_scr[proposal(h, p), :] = us[p] * norms[p]
        c_scr[pl.ds(h * SB, SB), :] = jnp.broadcast_to(scale, (SB, DK))
    for pair in range(SB // 2):
        for h in range(heads):
            at = tile(h, pair)
            key = kf[at, :]
            lhs = jnp.concatenate([key, key], axis=0).astype(bf16)
            u = u_scr[at, :]
            hi = u.astype(bf16).astype(f32)
            lo = u - hi
            for half in range(2):
                keep = low if half == 0 else jnp.logical_not(low)
                rhs = jnp.concatenate([jnp.where(keep, hi, 0.0), jnp.where(keep, lo, 0.0)], axis=0).astype(bf16)
                seq = 2 * pair + half
                add = lax.dot_general(lhs, rhs, (((0,), (0,)), ((), ())), preferred_element_type=f32)
                o_ref[seq, h] = c_scr[pl.ds(h * SB + seq, 1), :] * s_ref[seq, h] + add


def attend_items(items, scratch, load, factor, state_at, scalars, gain, emit):
    rk, rq, qf, kf, vf, zf, of = scratch
    low = first_half()
    for j, item in enumerate(items):
        for n, dst in enumerate((qf, kf, vf, zf)):
            dst[pl.ds(j * TALL, TALL), :] = (load(item, n) * factor(item)).astype(bf16).astype(f32)
    for pair in range(SB // 2):
        for j, item in enumerate(items):
            at = tile(j, pair)
            lhs = jnp.concatenate([kf[at, :], qf[at, :]], axis=0).astype(bf16)
            r0 = jnp.dot(lhs, state_at(item, 2 * pair).astype(bf16), preferred_element_type=f32)
            r1 = jnp.dot(lhs, state_at(item, 2 * pair + 1).astype(bf16), preferred_element_type=f32)
            rk[at, :] = jnp.where(low, r0[:8], r1[:8])
            rq[at, :] = jnp.where(low, r0[8:], r1[8:])
    for j, item in enumerate(items):
        scale = jnp.ones((SB, 1), f32)
        ks, us, norms = [], [], []
        for p in range(P_SIZE):
            at = proposal(j, p)
            g, strength = scalars(item, p)
            key = kf[at, :]
            query = qf[at, :]
            norm = lax.rsqrt(lane_dot(key, key) + epsilon)
            qnorm = lax.rsqrt(lane_dot(query, query) + epsilon) * DK ** (-0.5)
            rec = (scale * norm) * rk[at, :]
            for ki, ui, ni in zip(ks, us, norms):
                rec = rec + (lane_dot(ki, key) * (ni * norm)) * ui
            us = [ui * g for ui in us]
            scale = scale * g
            us.append(strength * (vf[at, :] - g * rec))
            ks.append(key)
            norms.append(norm)
            att = (scale * qnorm) * rq[at, :]
            for ki, ui, ni in zip(ks, us, norms):
                att = att + (lane_dot(ki, query) * (ni * qnorm)) * ui
            gate = zf[at, :]
            mean = jnp.sum(att * att, axis=-1, keepdims=True) / DK
            of[at, :] = att * lax.rsqrt(mean + epsilon) * gain * (gate * jax.nn.sigmoid(gate))
    for j, item in enumerate(items):
        emit(item, of[pl.ds(j * TALL, TALL), :].astype(bf16))


def small_terms(heads, features, few_wide, extra, rates, offset, thin):
    rows = few_wide.shape[1]
    few = rows_to_columns(few_wide)
    factor = lax.rsqrt(few[:, 2 * heads : 2 * heads + 1] / features + epsilon)
    seqs = extra.shape[1]
    row = lax.broadcasted_iota(jnp.int32, (rows, seqs), 0)
    owner = jnp.right_shift(row, 2) == lax.broadcasted_iota(jnp.int32, (rows, seqs), 1)
    spread = lax.dot_general(
        owner.astype(f32), extra, (((1,), (1,)), ((), ())),
        precision=lax.Precision.HIGHEST, preferred_element_type=f32,
    )
    turn = jnp.bitwise_and(lax.broadcasted_iota(jnp.int32, (rows, heads), 0), 3)
    struck = pick(turn, [spread[:, p * heads : (p + 1) * heads] for p in range(P_SIZE)])
    raised = few[:, :heads] * factor + offset
    soft = jnp.maximum(raised, 0.0) + jnp.log1p(jnp.exp(-jnp.abs(raised)))
    thin[:, :heads] = jnp.exp(struck - jnp.exp(rates) * soft)
    thin[:, heads : 2 * heads] = jax.nn.sigmoid(few[:, heads : 2 * heads] * factor)
    thin[:, 2 * heads : 2 * heads + 1] = factor


def attend_kernel(heads, features, few_ref, extra_ref, rate_ref, offset_ref, w_ref, parts, state, o_ref, kept, thin, *rest):
    scratch, done = rest[:-1], rest[-1]
    keep = pltpu.make_async_copy(state, kept, done)
    keep.start()
    small_terms(heads, features, few_ref[...], extra_ref[...], rate_ref[...], offset_ref[...], thin)

    def block(i, carry):
        base = i * TALL
        tall = pl.ds(base, TALL)

        def scalars(h, p):
            both = thin[pl.ds(base + p, SB, stride=P_SIZE), :]
            return both[:, h : h + 1], both[:, heads + h : heads + h + 1]

        def emit(h, value):
            o_ref[tall, h * DK : (h + 1) * DK] = value

        attend_items(
            range(heads), scratch,
            lambda h, n: parts[n, tall, h * DK : (h + 1) * DK],
            lambda h: thin[tall, 2 * heads : 2 * heads + 1],
            lambda h, seq: state[i * SB + seq, h],
            scalars, w_ref[...], emit,
        )
        return carry

    lax.fori_loop(0, state.shape[0] // SB, block, 0)
    keep.wait()


GROUP = 3


def attend_head(h, heads, blocks, scratch, parts_at, thin, state, gain, flat):
    def group(it, carry):
        def tall(j):
            return pl.ds((it * GROUP + j) * TALL, TALL)

        def scalars(j, p):
            both = thin[pl.ds((it * GROUP + j) * TALL + p, SB, stride=P_SIZE), :]
            return both[:, h : h + 1], both[:, heads + h : heads + h + 1]

        def emit(j, value):
            flat[tall(j), h * DK : (h + 1) * DK] = value

        attend_items(
            range(GROUP), scratch,
            lambda j, n: parts_at(tall(j), n),
            lambda j: thin[tall(j), 2 * heads : 2 * heads + 1],
            lambda j, seq: state[(it * GROUP + j) * SB + seq, h],
            scalars, gain, emit,
        )
        return carry

    lax.fori_loop(0, blocks // GROUP, group, 0)


def last_kernel(heads, thin, w_ref, parts, state, some, columns, o_ref, kept, flat, *rest):
    scratch, done = rest[:-1], rest[-1]
    keep = pltpu.make_async_copy(state, kept, done)
    keep.start()
    flat[...] = some[...]
    blocks = state.shape[0] // SB
    attend_head(
        heads - 1, heads, blocks, scratch, lambda at, n: parts[at, n * DK : (n + 1) * DK], thin, state, w_ref[...], flat
    )
    for c in range(columns.shape[0]):
        o_ref[c] = jnp.dot(flat[...], columns[c], preferred_element_type=f32).astype(bf16)
    keep.wait()


def accepted(state, keys, values, few):
    seqs, heads = state.shape[:2]
    width = heads * DK
    rows = TALL
    tall = pl.BlockSpec((rows, width), lambda i: (i, 0))
    thin = pl.BlockSpec((SB, few.shape[1]), lambda i: (i, 0))
    block = pl.BlockSpec((SB, heads, DK, DK), lambda i: (i, 0, 0, 0))
    return pl.pallas_call(
        functools.partial(accepted_kernel, heads),
        grid=(seqs // SB,),
        in_specs=[block, tall, tall, thin],
        out_specs=block,
        out_shape=jax.ShapeDtypeStruct(state.shape, f32),
        scratch_shapes=[pltpu.VMEM((heads * n, DK), f32) for n in (TALL, TALL, SB, TALL, TALL)],
        cost_estimate=pl.CostEstimate(flops=10_000_000_000, bytes_accessed=2 * state.size * 4, transcendentals=0),
        name="accepted",
    )(state, keys, values, few)


def local(array):
    return pltpu.with_memory_space_constraint(array, pltpu.VMEM)


def attend(features, state, parts, few, extra, rates, offset, gain):
    seqs, heads = state.shape[:2]
    rows, width = parts.shape[1:]
    vmem = pl.BlockSpec(memory_space=pltpu.VMEM)
    return pl.pallas_call(
        functools.partial(attend_kernel, heads, features),
        in_specs=[vmem] * 7,
        out_specs=[vmem, pl.BlockSpec(memory_space=pl.ANY)],
        out_shape=[pltpu.VMEM((rows, width), bf16), jax.ShapeDtypeStruct(state.shape, f32)],
        scratch_shapes=[
            pltpu.VMEM((rows, 2 * heads + 8), f32),
            *[pltpu.VMEM((heads * TALL, DK), f32)] * 7,
            pltpu.SemaphoreType.DMA,
        ],
        compiler_params=pltpu.CompilerParams(vmem_limit_bytes=LIMIT),
        cost_estimate=pl.CostEstimate(flops=5_000_000_000, bytes_accessed=state.size * 4, transcendentals=0),
        name="attend",
    )(
        local(few), extra, rates.reshape(1, heads), offset.reshape(1, heads), gain.reshape(1, DK),
        local(parts), local(state),
    )


def pick(index, values):
    chosen = values[-1]
    for at, value in enumerate(values[:-1]):
        chosen = jnp.where(index == at, value, chosen)
    return chosen


def last_head(thin, gain, parts, state, some, columns):
    seqs, heads = state.shape[:2]
    rows, width = some.shape
    vmem = pl.BlockSpec(memory_space=pltpu.VMEM)
    return pl.pallas_call(
        functools.partial(last_kernel, heads),
        in_specs=[vmem] * 6,
        out_specs=[vmem, pl.BlockSpec(memory_space=pl.ANY)],
        out_shape=[
            pltpu.VMEM((columns.shape[0], rows, columns.shape[2]), bf16),
            jax.ShapeDtypeStruct(state.shape, f32),
        ],
        scratch_shapes=[
            pltpu.VMEM((rows, width), bf16),
            *[pltpu.VMEM((GROUP * TALL, DK), f32)] * 7,
            pltpu.SemaphoreType.DMA,
        ],
        compiler_params=pltpu.CompilerParams(vmem_limit_bytes=LIMIT),
        cost_estimate=pl.CostEstimate(flops=5_000_000_000, bytes_accessed=state.size * 4, transcendentals=0),
        name="last_head",
    )(local(thin), gain.reshape(1, DK), local(parts), local(state), local(some), local(columns))


def turned_slot(t):
    return pick(t, (0, 2, 1, 3))


def project_kernel(x_hbm, gain_hbm, keys_hbm, values_hbm, fade_hbm, pull_hbm, count_hbm, extra_hbm, rate_hbm, offset_hbm,
                   outer_hbm, wf, ws, wq, wk, wv, wz, wo, state, last, small, taken, fbuf, flat,
                   x_ref, gain_ref, keys, values, fade, pull, counts, extra, rates, offset, outer, fs, thin, few_ref, acc,
                   xpre, xbuf, gbuf, w, sbuf, abuf, bbuf, cbuf, esend, erecv, s_in,
                   r_scr, u_scr, c_scr, kf, vf, a0, a1, a2, a3, a4, a5, a6,
                   lsem, xs, xp, xr, wsem, ss, ar, br, cr, es, er, ins, fsem, fss, fzr, fys, fyr):
    k, t, g = lax.axis_index("kv"), lax.axis_index("tp"), lax.axis_index("grp")
    depth, width = w.shape[1], w.shape[2]
    features = gain_ref.shape[0] * depth
    rows = x_ref.shape[0]
    blocks = state.shape[0] // SB
    heads = state.shape[1]

    def remote(src, dst, send, recv, kv, tp, grp=g):
        return pltpu.make_async_remote_copy(
            src, dst, send, recv, device_id={"grp": grp, "kv": kv, "tp": tp}, device_id_type=pl.DeviceIdType.MESH
        )

    here = pl.ds(k * depth, depth)
    locals_ = [
        pltpu.make_async_copy(src, dst, lsem.at[n])
        for n, (src, dst) in enumerate(
            (
                (x_hbm, x_ref), (gain_hbm, gain_ref), (keys_hbm, keys), (values_hbm, values), (fade_hbm, fade),
                (pull_hbm, pull), (count_hbm, counts), (extra_hbm, extra), (rate_hbm, rates), (offset_hbm, offset), (outer_hbm, outer),
                (wf.at[:, here], fs.at[0]), (ws.at[:, here], fs.at[1]),
            )
        )
    ]
    for load in locals_:
        load.start()
    f_load = pltpu.make_async_copy(wo, fbuf.at[k], fsem)
    f_load.start()
    loads = [
        pltpu.make_async_copy(
            src.at[:, pl.ds(h * DK, DK)], w.at[h, :, pl.ds(n * DK, DK)], wsem.at[h * 4 + n]
        )
        for h in range(heads)
        for n, src in enumerate((wq, wk, wv, wz))
    ]
    for load in loads:
        load.start()

    def fetch(i):
        return pltpu.make_async_copy(state.at[pl.ds(i * SB, SB)], s_in.at[i % 2], ins.at[i % 2])

    fetch(0).start()

    beside = t + 1 - 2 * (t % 2)
    across = (t + 2) % 4
    corner = t % 2
    landing = 2 * (t // 2) + k % 2
    home = corner == k % 2
    top_kind = t // 2 == k // 2
    source = jnp.where(top_kind, k, (k + 2) % 4)
    near_src = jnp.where(k <= 1, corner, corner + 2)
    far_src = jnp.where(k <= 1, corner + 2, corner)
    barrier = pltpu.get_barrier_semaphore()

    def greet(kv, tp, grp=g):
        pl.semaphore_signal(
            barrier, inc=1, device_id={"grp": grp, "kv": kv, "tp": tp}, device_id_type=pl.DeviceIdType.MESH
        )

    greet(k, beside)
    greet(k, across)
    greet(k, t, 1 - g)
    for step in range(1, 4):
        greet((k + step) % 4, t)

    @pl.when(t != k)
    def _():
        greet(t, landing)

    @pl.when(across != k)
    def _():
        greet(across, landing)

    @pl.when(near_src != k)
    def _():
        greet(near_src, source)

    @pl.when(far_src != k)
    def _():
        greet(far_src, source)

    @pl.when(home)
    def _():
        pl.semaphore_wait(barrier, 8)

    @pl.when(jnp.logical_not(home))
    def _():
        pl.semaphore_wait(barrier, 10)

    quarter = rows // 4
    locals_[0].wait()

    def part(q):
        return pl.ds(q * quarter, quarter)

    def forward(q):
        return remote(xpre.at[q], xbuf.at[k, part(2 + q)], xs.at[4 + q], xr.at[k, 2 + q], across, landing)

    def outward(q):
        return remote(x_ref.at[part(q)], xbuf.at[k, part(q)], xs.at[2 + q], xr.at[k, q], t, landing)

    def settled_copy(q):
        return pltpu.make_async_copy(x_ref.at[part(q)], xbuf.at[k, part(q)], xr.at[k, q])

    def sideways(q):
        return remote(x_ref.at[part(2 + q)], xpre.at[q], xs.at[q], xp.at[q], k, across)

    @pl.when(t == k)
    def _():
        for q in range(2):
            remote(x_ref.at[part(2 + q)], xbuf.at[k, part(2 + q)], xs.at[q], xr.at[k, 2 + q], k, across).start()
        for q in range(2):
            settled_copy(q).start()

    @pl.when(t != k)
    def _():
        for q in range(2):
            sideways(q).start()
        for q in range(2):
            outward(q).start()

    @pl.when(across != k)
    def _():
        for q in range(2):
            sideways(q).wait_recv()
            forward(q).start()

    end = jnp.where(k <= 1, 0, 3)
    near = jnp.where(k <= 1, 1, 2)
    is_end = k == end
    inside = jnp.logical_not(is_end)
    kind = jnp.where(top_kind, 0, 1)

    def piece(r, q, send, tp):
        at = pl.ds(q * quarter, quarter)
        return remote(xbuf.at[r, at], xbuf.at[r, at], xs.at[send], xr.at[r, q], k, tp)

    def spread(r, n, q):
        settled = jnp.logical_and(t == k, r == k)

        @pl.when(settled)
        def _():
            settled_copy(q).wait()

        @pl.when(jnp.logical_not(settled))
        def _():
            piece(r, 2 * kind + q, 6, across).wait_recv()

        piece(r, 2 * kind + q, 6 + n, across).start()
        piece(r, 2 * kind + q, 10 + n, beside).start()

    half_rows = fbuf.shape[1] // 2
    half = pl.ds(g * half_rows, half_rows)

    def f_pass(c, to, sem):
        return remote(fbuf.at[c, half], fbuf.at[c, half], fss.at[sem], fzr.at[c], to, t)

    def f_swap(c):
        return remote(fbuf.at[c, half], fbuf.at[c, half], fys.at[c], fyr.at[c], k, t, 1 - g)

    def f_begin():
        f_load.wait()

        @pl.when(k < 3)
        def _():
            f_pass(k, k + 1, 4).start()

        @pl.when(k > 0)
        def _():
            f_pass(k, k - 1, 5).start()

    pl.when(is_end)(f_begin)
    for q in range(2):
        spread(far_src, 2 * q + 1, q)
        spread(near_src, 2 * q, q)
    pl.when(inside)(f_begin)
    def cross_in(n, r):
        for q in range(2):
            piece(r, 2 - 2 * kind + q, 6, across).wait_recv()
            piece(r, 2 - 2 * kind + q, 14 + 2 * q + n, beside).start()

    def beside_in(r):
        for q in range(4):
            piece(r, q, 6, beside).wait_recv()

    near_mate = jnp.where(k <= 1, 1 - corner, 3 - corner)
    far_mate = jnp.where(k <= 1, 3 - corner, 1 - corner)
    lazy = jnp.logical_and(is_end, far_mate == 3 - end)
    for load in locals_[1:]:
        load.wait()
    thin[...] = rows_to_columns(
        jnp.concatenate([fade[...], pull[...], jnp.broadcast_to(counts[...].astype(f32), (8, counts.shape[1]))], axis=0)
    )
    for load in loads:
        load.wait()

    @pl.when(jnp.logical_not(lazy))
    def _():
        cross_in(1, far_src)


    def f_forwards(c):
        return jnp.logical_or(jnp.logical_and(c < k, k < 3), jnp.logical_and(c > k, k > 0))

    def f_take(c):
        to = jnp.where(c < k, k + 1, k - 1)
        f_pass(c, k, c).wait_recv()

        @pl.when(f_forwards(c))
        def _():
            f_pass(c, to, c).start()

        f_swap(c).start()

    f_order = (jnp.where(is_end, near, end), 3 - near, 3 - end)

    @pl.when(jnp.logical_or(inside, far_mate == 3 - end))
    def _():
        beside_in(far_mate)

    @pl.when(inside)
    def _():
        cross_in(0, near_src)
        beside_in(near_mate)

    nt = (((1,), (1,)), ((), ()))

    def prepare(r):
        floated = xbuf[r].astype(f32)
        gained = (floated * gain_ref[k]).astype(bf16)
        gbuf[r] = gained
        squares = floated * floated
        high = squares.astype(bf16)
        rest = (squares - high.astype(f32)).astype(bf16)
        ones = jnp.ones((8, depth), bf16)
        for n in range(2):
            every = lax.dot_general(fs[n], gained, nt, preferred_element_type=f32)
            esend[r, n * heads : (n + 1) * heads, :] = pick(t, [every[m * heads : (m + 1) * heads] for m in range(4)])
        esend[r, 2 * heads :, :] = lax.dot_general(ones, high, nt, preferred_element_type=f32) + lax.dot_general(
            ones, rest, nt, preferred_element_type=f32
        )

        @pl.when(r != k)
        def _():
            remote(esend.at[r], erecv.at[k], es.at[r], er.at[k], r, t).start()

    def product(r, c):
        return jnp.dot(gbuf[r], w[c], preferred_element_type=f32)

    def from_end(i):
        remote(abuf.at[i], abuf.at[i], ss.at[i], ar.at[i], k, beside).wait_recv()
        return abuf[i].astype(f32)

    def from_inner(i):
        remote(bbuf.at[i], bbuf.at[i], ss.at[i], br.at[i], k, beside).wait_recv()
        return bbuf[i].astype(f32)

    def accept(i):
        @pl.when(i + 1 < blocks)
        def _():
            fetch(i + 1).start()

        fetch(i).wait()

        few_rows = pl.ds(i * SB, SB)
        accepted_kernel(
            heads, s_in.at[i % 2], keys.at[few_rows], values.at[few_rows], thin.at[few_rows], taken.at[few_rows],
            r_scr, u_scr, c_scr, kf, vf,
        )

    def accept_some(low, high):
        def one(i, carry):
            accept(i)
            return carry

        lax.fori_loop(low, high, one, 0)

    chunk_head, chunk_stage = (0, 1, 0, 0, 2, 1, 1, 3, 2, 3, 2, 3), (0, 0, 1, 2, 0, 1, 2, 0, 1, 1, 2, 2)
    prepared = (3 - end, end, 3 - near, near)
    late = (3 - end, end, 3 - near, near, end)

    def settle_small():
        few_ref[...] = esend[k]
        for src in range(4):

            @pl.when(k != src)
            def _():
                remote(esend.at[src], erecv.at[src], es.at[src], er.at[src], k, beside).wait()
                few_ref[...] += erecv[src]

        small_terms(heads, features, few_ref[...], extra[...], rates[...], offset[...], small)

    def attention(h):
        attend_head(
            h, heads, blocks, (a0, a1, a2, a3, a4, a5, a6),
            lambda at, n: acc[h, at, n * DK : (n + 1) * DK], small, taken, outer[...], flat,
        )

    @pl.when(inside)
    def _():
        def one(i, carry):
            prepare(pick(i, prepared))
            return carry

        lax.fori_loop(0, 4, one, 0)
        f_take(f_order[0])
        accept_some(0, blocks // 2)
        f_take(f_order[1])

    def step(i, carry):
        h, stage = pick(i, chunk_head), pick(i, chunk_stage)
        r = pick(stage, (3 - end, 3 - near, near))

        @pl.when(jnp.logical_and(is_end, i == 2))
        def _():
            pl.when(lazy)(lambda: cross_in(1, far_src))
            cross_in(0, near_src)

            @pl.when(far_mate != 3 - end)
            def _():
                beside_in(far_mate)

            beside_in(near_mate)

        @pl.when(jnp.logical_and(is_end, jnp.logical_and(i < 5, i != 1)))
        def _():
            prepare(pick(i, late))

        @pl.when(is_end)
        def _():
            sbuf[i] = product(r, h).astype(bf16)
            remote(sbuf.at[i], abuf.at[i], ss.at[i], ar.at[i], near, t).start()

        @pl.when(jnp.logical_and(inside, stage < 2))
        def _():
            part = product(r, h)
            sbuf[i] = (part + from_end(i)).astype(bf16)
            remote(sbuf.at[i], bbuf.at[i], ss.at[i], br.at[i], 3 - near, t).start()

        @pl.when(jnp.logical_and(inside, i == 0))
        def _():
            accept_some(blocks // 2, blocks * 2 // 3)

        @pl.when(jnp.logical_and(inside, i == 1))
        def _():
            accept_some(blocks * 2 // 3, blocks)

        @pl.when(jnp.logical_and(inside, i == 3))
        def _():
            f_take(f_order[2])

        back = jnp.logical_or(jnp.logical_or(i == 3, i == 4), jnp.logical_or(i == 6, i == 9))

        @pl.when(jnp.logical_and(inside, back))
        def _():
            m = jnp.where(i <= 4, i - 3, i // 3)
            part = product(end, m)
            sbuf[12 + m] = (part + from_inner(pick(m, (0, 1, 4, 7)))).astype(bf16)
            remote(sbuf.at[12 + m], cbuf.at[m], ss.at[12 + m], cr.at[m], end, t).start()

        @pl.when(jnp.logical_and(inside, i == 5))
        def _():
            settle_small()

        ready = jnp.logical_or(jnp.logical_or(i == 5, i == 8), i == 10)

        @pl.when(jnp.logical_and(inside, ready))
        def _():
            m = i // 3 - 1
            acc[m] = product(near, m) + from_inner(pick(m, (2, 5, 8))) + from_end(pick(m, (3, 6, 10)))

        for m in range(3):

            @pl.when(jnp.logical_and(inside, i == (5, 8, 10)[m]))
            def _():
                attention(m)

        @pl.when(jnp.logical_and(inside, i == 11))
        def _():
            last[...] = product(near, 3) + from_inner(9) + from_end(11)

        return carry

    lax.fori_loop(0, 12, step, 0)

    @pl.when(is_end)
    def _():
        f_take(f_order[0])
        accept_some(0, blocks)
        settle_small()
        f_take(f_order[1])

        def returned(m):
            part = product(end, m)
            remote(cbuf.at[m], cbuf.at[m], ss.at[m], cr.at[m], k, beside).wait_recv()
            return part + cbuf[m].astype(f32)

        for m in range(3):
            acc[m] = returned(m)
            attention(m)
            if m == 0:
                f_take(f_order[2])
        last[...] = returned(3)

    for src in range(4):

        @pl.when(k != src)
        def _():
            remote(fbuf.at[src, half], fbuf.at[src, half], fys.at[src], fyr.at[src], k, beside).wait()

    for q in range(2):
        sideways(q).wait_send()

    @pl.when(t != k)
    def _():
        for q in range(2):
            outward(q).wait_send()

    @pl.when(across != k)
    def _():
        for q in range(2):
            forward(q).wait_send()

    for n in range(12):
        piece(k, 0, 6 + n, beside).wait_send()

    @pl.when(k < 3)
    def _():
        f_pass(k, k, 4).wait_send()

    @pl.when(k > 0)
    def _():
        f_pass(k, k, 5).wait_send()

    for src in range(4):

        @pl.when(jnp.logical_and(k != src, f_forwards(src)))
        def _():
            f_pass(src, k, src).wait_send()

    for i in range(12):

        @pl.when(is_end if chunk_stage[i] == 2 else k >= 0)
        def _():
            remote(sbuf.at[i], abuf.at[i], ss.at[i], ar.at[i], k, beside).wait_send()

    for m in range(4):

        @pl.when(inside)
        def _():
            remote(sbuf.at[12 + m], cbuf.at[m], ss.at[12 + m], cr.at[m], end, t).wait_send()


def project(x, gain, weights, forgetting, strength, final, state, keys, values, fade, pull, counts, extra, rates, offset, outer):
    rows, depth = x.shape
    width = weights[0].shape[1]
    seqs, heads = state.shape[:2]
    few_rows = 2 * heads + 8
    vmem, hbm = pl.BlockSpec(memory_space=pltpu.VMEM), pl.BlockSpec(memory_space=pl.ANY)
    dma = pltpu.SemaphoreType.DMA
    gain = gain.reshape(-1, 1, depth)
    rates, offset, outer = rates.reshape(1, heads), offset.reshape(1, heads), outer.reshape(1, DK)
    forgetting, strength = forgetting.T, strength.T

    def chunks(n):
        return pltpu.VMEM((n, rows, width), bf16)

    def like(a):
        return pltpu.VMEM(a.shape, a.dtype)

    return pl.pallas_call(
        project_kernel,
        in_specs=[hbm] * 19,
        out_specs=[vmem] * 5,
        out_shape=[
            pltpu.VMEM((rows, width), f32),
            pltpu.VMEM((rows, few_rows), f32),
            pltpu.VMEM(state.shape, f32),
            pltpu.VMEM((4,) + final.shape, bf16),
            pltpu.VMEM((rows, width), bf16),
        ],
        scratch_shapes=[
            like(x), like(gain), like(keys), like(values), like(fade), like(pull), like(counts),
            like(extra), like(rates), like(offset), like(outer),
            pltpu.VMEM((2, forgetting.shape[0], depth), bf16),
            pltpu.VMEM((seqs, 2 * P_SIZE * heads + 8), f32),
            pltpu.VMEM((few_rows, rows), f32),
            pltpu.VMEM((3, rows, width), f32),
            pltpu.VMEM((2, rows // 4, depth), bf16),
            pltpu.VMEM((4, rows, depth), bf16),
            pltpu.VMEM((4, rows, depth), bf16),
            pltpu.VMEM((4, depth, width), bf16),
            chunks(16), chunks(12), chunks(12), chunks(4),
            pltpu.VMEM((4, few_rows, rows), f32),
            pltpu.VMEM((4, few_rows, rows), f32),
            pltpu.VMEM((2, SB) + state.shape[1:], f32),
            *[pltpu.VMEM((heads * n, DK), f32) for n in (TALL, TALL, SB, TALL, TALL)],
            *[pltpu.VMEM((GROUP * TALL, DK), f32)] * 7,
            dma((13,)), dma((18,)), dma((2,)), dma((4, 4)), dma((16,)), dma((16,)), dma((12,)), dma((12,)), dma((4,)), dma((4,)),
            dma((4,)), dma((2,)), dma, dma((6,)), dma((4,)), dma((4,)), dma((4,)),
        ],
        compiler_params=pltpu.CompilerParams(has_side_effects=True, collective_id=0, vmem_limit_bytes=LIMIT),
        name="project",
    )(x, gain, keys, values, fade, pull, counts, extra, rates, offset, outer, forgetting, strength, *weights, final, state)


PIECES = 3


def mix_kernel(part, o_ref, mate, sent, cross, ms, mr, xs, xr):
    k, t, g = lax.axis_index("kv"), lax.axis_index("tp"), lax.axis_index("grp")
    rows = part.shape[1]
    piece = rows // PIECES
    beside = t + 1 - 2 * (t % 2)
    across = (t + 2) % 4
    order = ((beside + 2) % 4, beside)

    def remote(src, dst, send, recv, tp):
        return pltpu.make_async_remote_copy(
            src, dst, send, recv, device_id={"grp": g, "kv": k, "tp": tp}, device_id_type=pl.DeviceIdType.MESH
        )

    barrier = pltpu.get_barrier_semaphore()
    for peer in (beside, across):
        pl.semaphore_signal(
            barrier, inc=1, device_id={"grp": g, "kv": k, "tp": peer}, device_id_type=pl.DeviceIdType.MESH
        )
    pl.semaphore_wait(barrier, 2)

    def to_mate(n, s):
        at = pl.ds(s * piece, piece)
        return remote(part.at[order[n], at], mate.at[n, at], ms.at[n, s], mr.at[n, s], beside)

    def to_cross(s):
        at = pl.ds(s * piece, piece)
        return remote(sent.at[at], cross.at[at], xs.at[s], xr.at[s], across)

    for n in range(2):
        for s in range(PIECES):
            to_mate(n, s).start()
    for s in range(PIECES):
        at = slice(s * piece, (s + 1) * piece)
        to_mate(0, s).wait_recv()
        sent[at, :] = (part[across, at, :].astype(f32) + mate[0, at, :].astype(f32)).astype(bf16)
        to_cross(s).start()
    for s in range(PIECES):
        at = slice(s * piece, (s + 1) * piece)
        to_mate(1, s).wait_recv()
        to_cross(s).wait_recv()
        o_ref[at, :] = (
            part[t, at, :].astype(f32) + mate[1, at, :].astype(f32) + cross[at, :].astype(f32)
        ).astype(bf16)
    for s in range(PIECES):
        to_mate(0, s).wait_send()
        to_mate(1, s).wait_send()
        to_cross(s).wait_send()


def mix(part):
    rows, cols = part.shape[1:]
    vmem = pl.BlockSpec(memory_space=pltpu.VMEM)
    dma = pltpu.SemaphoreType.DMA
    return pl.pallas_call(
        mix_kernel,
        in_specs=[vmem],
        out_specs=vmem,
        out_shape=jax.ShapeDtypeStruct((rows, cols), bf16),
        scratch_shapes=[
            pltpu.VMEM((2, rows, cols), bf16),
            pltpu.VMEM((rows, cols), bf16),
            pltpu.VMEM((rows, cols), bf16),
            dma((2, PIECES)), dma((2, PIECES)), dma((PIECES,)), dma((PIECES,)),
        ],
        compiler_params=pltpu.CompilerParams(has_side_effects=True, collective_id=1, vmem_limit_bytes=LIMIT),
        name="mix",
    )(local(part))


def on_device(
    n_kv,
    n_tp,
    candidate_embeddings,
    incoming_rms_scaling,
    probe_projector,
    address_projector,
    content_projector,
    sigmoid_mask_matrix,
    forgetting_projector,
    strength_projector_matrix,
    channel_forgetting_rates,
    forgetting_offset,
    extra_forgetting,
    outgoing_rms_scaling,
    final_projector,
    memory_matrix,
    earlier_addresses,
    earlier_contents,
    earlier_strengths,
    earlier_forgetting,
    admitted_counts,
):
    rows, local_cols = candidate_embeddings.shape
    features = incoming_rms_scaling.shape[0]
    depth, width = probe_projector.shape
    heads = width // DK
    seqs = rows // P_SIZE
    k_index, t_index = lax.axis_index("kv"), lax.axis_index("tp")

    def thin(values):
        return values.transpose(1, 2, 0).reshape(P_SIZE * heads, seqs)

    weights = (probe_projector, address_projector, content_projector, sigmoid_mask_matrix)
    fade, pull, extra = thin(earlier_forgetting), thin(earlier_strengths), thin(extra_forgetting)
    if n_kv == 4 and n_tp == 4:
        last, small, taken, columns, flat = project(
            candidate_embeddings, incoming_rms_scaling, weights, forgetting_projector, strength_projector_matrix,
            final_projector, memory_matrix, earlier_addresses, earlier_contents, fade, pull, admitted_counts.reshape(1, seqs), extra,
            channel_forgetting_rates, forgetting_offset, outgoing_rms_scaling,
        )
        part, taken = last_head(small, outgoing_rms_scaling, last, taken, flat, columns)
        mixed = mix(part)
    else:
        every = lax.all_gather(candidate_embeddings, "tp", axis=1, tiled=True)
        every = lax.all_to_all(every, "kv", split_axis=1, concat_axis=0, tiled=True)
        gain_part = lax.dynamic_slice_in_dim(incoming_rms_scaling, k_index * depth, depth)
        floated = every.astype(f32)
        gained = (floated * gain_part).astype(bf16)
        decay_cols = lax.dynamic_slice(forgetting_projector, (k_index * depth, t_index * heads), (depth, heads))
        beta_cols = lax.dynamic_slice(strength_projector_matrix, (k_index * depth, t_index * heads), (depth, heads))
        few = jnp.concatenate(
            [
                jnp.dot(gained, jnp.concatenate([decay_cols, beta_cols], axis=1), preferred_element_type=f32),
                jnp.sum(floated * floated, axis=1, keepdims=True),
            ],
            axis=1,
        )
        few = lax.psum_scatter(few, "kv", scatter_dimension=0, tiled=True)
        few = jnp.pad(few, ((0, 0), (0, 7))).T
        partial = jnp.stack([jnp.dot(gained, w, preferred_element_type=f32).astype(bf16) for w in weights])
        summed = lax.psum_scatter(partial, "kv", scatter_dimension=1, tiled=True).astype(f32)
        counts = admitted_counts.astype(f32).reshape(seqs, 1)
        keys, values = earlier_addresses.reshape(rows, width), earlier_contents.reshape(rows, width)
        taken = accepted(memory_matrix, keys, values, jnp.concatenate([fade.T, pull.T, counts], axis=1))
        flat, taken = attend(
            features, taken, summed, few, extra, channel_forgetting_rates, forgetting_offset, outgoing_rms_scaling
        )
        gathered = lax.all_gather(flat, "kv", axis=0, tiled=True)
        terms = jnp.dot(gathered, final_projector, preferred_element_type=f32).astype(bf16)
        terms = lax.all_to_all(terms, "kv", split_axis=0, concat_axis=1, tiled=True)
        mixed = lax.psum_scatter(terms, "tp", scatter_dimension=1, tiled=True)
    return (mixed, taken)


def solution(mesh):
    row, per_head = P(("grp", "kv"), "tp"), P(("grp", "kv"), None, "tp")
    four = P(("grp", "kv"), None, "tp", None)
    weight = P("kv", "tp")
    state = P(("grp", "kv"), "tp", None, None)
    in_specs = (
        row, P(), weight, weight, weight, weight, P(), P(), P("tp"), P("tp"), per_head, P(),
        P("tp", "kv"), state, four, four, per_head, per_head, P(("grp", "kv")),
    )
    body = functools.partial(on_device, mesh.shape["kv"], mesh.shape["tp"])
    return jax.shard_map(body, mesh=mesh, in_specs=in_specs, out_specs=(row, state), check_vma=False)
```

```python
import functools

import jax
import jax.numpy as jnp
from jax import lax
from jax.experimental import pallas as pl
from jax.experimental.pallas import tpu as pltpu
from jax.sharding import PartitionSpec as P

DK = 128
P_SIZE = 4
SB = 8
TALL = SB * P_SIZE
epsilon = 1e-06
LIMIT = 42 * 2**20
f32 = jnp.float32
bf16 = jnp.bfloat16


def lane_dot(a, b):
    return jnp.sum(a * b, axis=-1, keepdims=True)


def first_half():
    return lax.broadcasted_iota(jnp.int32, (8, DK), 0) < P_SIZE


def load_heads(heads, src, dst, factor=None):
    if len(src.shape) == 4:
        block = src[...].astype(f32)
        for h in range(heads):
            dst[pl.ds(h * TALL, TALL), :] = block[:, :, h, :].reshape(TALL, DK)
        return
    for h in range(heads):
        part = src[:, h * DK : (h + 1) * DK].astype(f32)
        dst[pl.ds(h * TALL, TALL), :] = part if factor is None else (part * factor).astype(bf16).astype(f32)


def tile(h, pair):
    return pl.ds(h * TALL + pair * 8, 8)


def proposal(h, p):
    return pl.ds(h * TALL + p, SB, stride=P_SIZE)


def rows_to_columns(wide):
    count = wide.shape[1]
    same = lax.broadcasted_iota(jnp.int32, (count, count), 0) == lax.broadcasted_iota(jnp.int32, (count, count), 1)
    return lax.dot_general(
        same.astype(f32), wide, (((1,), (1,)), ((), ())),
        precision=lax.Precision.HIGHEST, preferred_element_type=f32,
    )


def accepted_kernel(heads, s_ref, k_ref, v_ref, n_ref, o_ref, r_scr, u_scr, c_scr, kf, vf):
    load_heads(heads, k_ref, kf)
    load_heads(heads, v_ref, vf)
    low = first_half()
    for pair in range(SB // 2):
        for h in range(heads):
            at = tile(h, pair)
            lhs = kf[at, :].astype(bf16)
            r0 = jnp.dot(lhs, s_ref[2 * pair, h].astype(bf16), preferred_element_type=f32)
            r1 = jnp.dot(lhs, s_ref[2 * pair + 1, h].astype(bf16), preferred_element_type=f32)
            r_scr[at, :] = jnp.where(low, r0, r1)
    few = n_ref[...]
    span = P_SIZE * heads
    count = few[:, 2 * span : 2 * span + 1]
    for h in range(heads):
        scale = jnp.ones((SB, 1), f32)
        ks, us, norms = [], [], []
        for p in range(P_SIZE):
            at = proposal(h, p)
            col = slice(p * heads + h, p * heads + h + 1)
            key = kf[at, :]
            norm = lax.rsqrt(lane_dot(key, key) + epsilon)
            live = count > float(p)
            g = jnp.where(live, jnp.exp(few[:, p * heads + h : p * heads + h + 1]), 1.0)
            b = jnp.where(live, few[:, span + p * heads + h : span + p * heads + h + 1], 0.0)
            rec = (scale * norm) * r_scr[at, :]
            for ki, ui, ni in zip(ks, us, norms):
                rec = rec + (lane_dot(ki, key) * (ni * norm)) * ui
            us = [ui * g for ui in us]
            scale = scale * g
            us.append(b * (vf[at, :] - g * rec))
            ks.append(key)
            norms.append(norm)
        for p in range(P_SIZE):
            u_scr[proposal(h, p), :] = us[p] * norms[p]
        c_scr[pl.ds(h * SB, SB), :] = jnp.broadcast_to(scale, (SB, DK))
    for pair in range(SB // 2):
        for h in range(heads):
            at = tile(h, pair)
            key = kf[at, :]
            lhs = jnp.concatenate([key, key], axis=0).astype(bf16)
            u = u_scr[at, :]
            hi = u.astype(bf16).astype(f32)
            lo = u - hi
            for half in range(2):
                keep = low if half == 0 else jnp.logical_not(low)
                rhs = jnp.concatenate([jnp.where(keep, hi, 0.0), jnp.where(keep, lo, 0.0)], axis=0).astype(bf16)
                seq = 2 * pair + half
                add = lax.dot_general(lhs, rhs, (((0,), (0,)), ((), ())), preferred_element_type=f32)
                o_ref[seq, h] = c_scr[pl.ds(h * SB + seq, 1), :] * s_ref[seq, h] + add


def attend_items(items, scratch, load, factor, state_at, scalars, gain, emit):
    rk, rq, qf, kf, vf, zf, of = scratch
    low = first_half()
    for j, item in enumerate(items):
        for n, dst in enumerate((qf, kf, vf, zf)):
            dst[pl.ds(j * TALL, TALL), :] = (load(item, n) * factor(item)).astype(bf16).astype(f32)
    for pair in range(SB // 2):
        for j, item in enumerate(items):
            at = tile(j, pair)
            lhs = jnp.concatenate([kf[at, :], qf[at, :]], axis=0).astype(bf16)
            r0 = jnp.dot(lhs, state_at(item, 2 * pair).astype(bf16), preferred_element_type=f32)
            r1 = jnp.dot(lhs, state_at(item, 2 * pair + 1).astype(bf16), preferred_element_type=f32)
            rk[at, :] = jnp.where(low, r0[:8], r1[:8])
            rq[at, :] = jnp.where(low, r0[8:], r1[8:])
    for j, item in enumerate(items):
        scale = jnp.ones((SB, 1), f32)
        ks, us, norms = [], [], []
        for p in range(P_SIZE):
            at = proposal(j, p)
            g, strength = scalars(item, p)
            key = kf[at, :]
            query = qf[at, :]
            norm = lax.rsqrt(lane_dot(key, key) + epsilon)
            qnorm = lax.rsqrt(lane_dot(query, query) + epsilon) * DK ** (-0.5)
            rec = (scale * norm) * rk[at, :]
            for ki, ui, ni in zip(ks, us, norms):
                rec = rec + (lane_dot(ki, key) * (ni * norm)) * ui
            us = [ui * g for ui in us]
            scale = scale * g
            us.append(strength * (vf[at, :] - g * rec))
            ks.append(key)
            norms.append(norm)
            att = (scale * qnorm) * rq[at, :]
            for ki, ui, ni in zip(ks, us, norms):
                att = att + (lane_dot(ki, query) * (ni * qnorm)) * ui
            gate = zf[at, :]
            mean = jnp.sum(att * att, axis=-1, keepdims=True) / DK
            of[at, :] = att * lax.rsqrt(mean + epsilon) * gain * (gate * jax.nn.sigmoid(gate))
    for j, item in enumerate(items):
        emit(item, of[pl.ds(j * TALL, TALL), :].astype(bf16))


def small_terms(heads, features, few_wide, extra, rates, offset, thin):
    rows = few_wide.shape[1]
    few = rows_to_columns(few_wide)
    factor = lax.rsqrt(few[:, 2 * heads : 2 * heads + 1] / features + epsilon)
    seqs = extra.shape[1]
    row = lax.broadcasted_iota(jnp.int32, (rows, seqs), 0)
    owner = jnp.right_shift(row, 2) == lax.broadcasted_iota(jnp.int32, (rows, seqs), 1)
    spread = lax.dot_general(
        owner.astype(f32), extra, (((1,), (1,)), ((), ())),
        precision=lax.Precision.HIGHEST, preferred_element_type=f32,
    )
    turn = jnp.bitwise_and(lax.broadcasted_iota(jnp.int32, (rows, heads), 0), 3)
    struck = pick(turn, [spread[:, p * heads : (p + 1) * heads] for p in range(P_SIZE)])
    raised = few[:, :heads] * factor + offset
    soft = jnp.maximum(raised, 0.0) + jnp.log1p(jnp.exp(-jnp.abs(raised)))
    thin[:, :heads] = jnp.exp(struck - jnp.exp(rates) * soft)
    thin[:, heads : 2 * heads] = jax.nn.sigmoid(few[:, heads : 2 * heads] * factor)
    thin[:, 2 * heads : 2 * heads + 1] = factor


def attend_kernel(heads, features, few_ref, extra_ref, rate_ref, offset_ref, w_ref, parts, state, o_ref, kept, thin, *rest):
    scratch, done = rest[:-1], rest[-1]
    keep = pltpu.make_async_copy(state, kept, done)
    keep.start()
    small_terms(heads, features, few_ref[...], extra_ref[...], rate_ref[...], offset_ref[...], thin)

    def block(i, carry):
        base = i * TALL
        tall = pl.ds(base, TALL)

        def scalars(h, p):
            both = thin[pl.ds(base + p, SB, stride=P_SIZE), :]
            return both[:, h : h + 1], both[:, heads + h : heads + h + 1]

        def emit(h, value):
            o_ref[tall, h * DK : (h + 1) * DK] = value

        attend_items(
            range(heads), scratch,
            lambda h, n: parts[n, tall, h * DK : (h + 1) * DK],
            lambda h: thin[tall, 2 * heads : 2 * heads + 1],
            lambda h, seq: state[i * SB + seq, h],
            scalars, w_ref[...], emit,
        )
        return carry

    lax.fori_loop(0, state.shape[0] // SB, block, 0)
    keep.wait()


GROUP = 3
COPIES = 8


def attend_head(h, heads, blocks, scratch, parts_at, thin, state, gain, flat):
    def group(it, carry):
        def tall(j):
            return pl.ds((it * GROUP + j) * TALL, TALL)

        def scalars(j, p):
            both = thin[pl.ds((it * GROUP + j) * TALL + p, SB, stride=P_SIZE), :]
            return both[:, h : h + 1], both[:, heads + h : heads + h + 1]

        def emit(j, value):
            flat[tall(j), h * DK : (h + 1) * DK] = value

        attend_items(
            range(GROUP), scratch,
            lambda j, n: parts_at(tall(j), n),
            lambda j: thin[tall(j), 2 * heads : 2 * heads + 1],
            lambda j, seq: state[(it * GROUP + j) * SB + seq, h],
            scalars, gain, emit,
        )
        return carry

    lax.fori_loop(0, blocks // GROUP, group, 0)


def last_kernel(heads, thin, w_ref, parts, state, some, columns, o_ref, kept, flat, *rest):
    scratch, done = rest[:-1], rest[-1]
    span = state.shape[0] // COPIES
    keeps = [
        pltpu.make_async_copy(state.at[pl.ds(n * span, span)], kept.at[pl.ds(n * span, span)], done.at[n])
        for n in range(COPIES)
    ]
    for keep in keeps:
        keep.start()
    flat[...] = some[...]
    blocks = state.shape[0] // SB
    attend_head(
        heads - 1, heads, blocks, scratch, lambda at, n: parts[at, n * DK : (n + 1) * DK], thin, state, w_ref[...], flat
    )
    for c in range(columns.shape[0]):
        o_ref[c] = jnp.dot(flat[...], columns[c], preferred_element_type=f32).astype(bf16)
    for keep in keeps:
        keep.wait()


def accepted(state, keys, values, few):
    seqs, heads = state.shape[:2]
    width = heads * DK
    rows = TALL
    tall = pl.BlockSpec((rows, width), lambda i: (i, 0))
    thin = pl.BlockSpec((SB, few.shape[1]), lambda i: (i, 0))
    block = pl.BlockSpec((SB, heads, DK, DK), lambda i: (i, 0, 0, 0))
    return pl.pallas_call(
        functools.partial(accepted_kernel, heads),
        grid=(seqs // SB,),
        in_specs=[block, tall, tall, thin],
        out_specs=block,
        out_shape=jax.ShapeDtypeStruct(state.shape, f32),
        scratch_shapes=[pltpu.VMEM((heads * n, DK), f32) for n in (TALL, TALL, SB, TALL, TALL)],
        cost_estimate=pl.CostEstimate(flops=10_000_000_000, bytes_accessed=2 * state.size * 4, transcendentals=0),
        name="accepted",
    )(state, keys, values, few)


def local(array):
    return pltpu.with_memory_space_constraint(array, pltpu.VMEM)


def attend(features, state, parts, few, extra, rates, offset, gain):
    seqs, heads = state.shape[:2]
    rows, width = parts.shape[1:]
    vmem = pl.BlockSpec(memory_space=pltpu.VMEM)
    return pl.pallas_call(
        functools.partial(attend_kernel, heads, features),
        in_specs=[vmem] * 7,
        out_specs=[vmem, pl.BlockSpec(memory_space=pl.ANY)],
        out_shape=[pltpu.VMEM((rows, width), bf16), jax.ShapeDtypeStruct(state.shape, f32)],
        scratch_shapes=[
            pltpu.VMEM((rows, 2 * heads + 8), f32),
            *[pltpu.VMEM((heads * TALL, DK), f32)] * 7,
            pltpu.SemaphoreType.DMA,
        ],
        compiler_params=pltpu.CompilerParams(vmem_limit_bytes=LIMIT),
        cost_estimate=pl.CostEstimate(flops=5_000_000_000, bytes_accessed=state.size * 4, transcendentals=0),
        name="attend",
    )(
        local(few), extra, rates.reshape(1, heads), offset.reshape(1, heads), gain.reshape(1, DK),
        local(parts), local(state),
    )


def pick(index, values):
    chosen = values[-1]
    for at, value in enumerate(values[:-1]):
        chosen = jnp.where(index == at, value, chosen)
    return chosen


def last_head(thin, gain, parts, state, some, columns):
    seqs, heads = state.shape[:2]
    rows, width = some.shape
    vmem = pl.BlockSpec(memory_space=pltpu.VMEM)
    return pl.pallas_call(
        functools.partial(last_kernel, heads),
        in_specs=[vmem] * 6,
        out_specs=[vmem, pl.BlockSpec(memory_space=pl.ANY)],
        out_shape=[
            pltpu.VMEM((columns.shape[0], rows, columns.shape[2]), bf16),
            jax.ShapeDtypeStruct(state.shape, f32),
        ],
        scratch_shapes=[
            pltpu.VMEM((rows, width), bf16),
            *[pltpu.VMEM((GROUP * TALL, DK), f32)] * 7,
            pltpu.SemaphoreType.DMA((COPIES,)),
        ],
        compiler_params=pltpu.CompilerParams(vmem_limit_bytes=LIMIT),
        cost_estimate=pl.CostEstimate(flops=5_000_000_000, bytes_accessed=state.size * 4, transcendentals=0),
        name="last_head",
    )(local(thin), gain.reshape(1, DK), local(parts), local(state), local(some), local(columns))


def turned_slot(t):
    return pick(t, (0, 2, 1, 3))


def project_kernel(x_hbm, gain_hbm, keys_hbm, values_hbm, fade_hbm, pull_hbm, count_hbm, extra_hbm, rate_hbm, offset_hbm,
                   outer_hbm, wf, ws, wq, wk, wv, wz, wo, state, last, small, taken, fbuf, flat,
                   x_ref, gain_ref, keys, values, fade, pull, counts, extra, rates, offset, outer, fs, thin, few_ref, acc,
                   xpre, xbuf, gbuf, w, sbuf, abuf, bbuf, cbuf, esend, erecv, s_in,
                   r_scr, u_scr, c_scr, kf, vf, a0, a1, a2, a3, a4, a5, a6,
                   lsem, xs, xp, xr, wsem, ss, ar, br, cr, es, er, ins, fsem, fss, fzr, fys, fyr):
    k, t, g = lax.axis_index("kv"), lax.axis_index("tp"), lax.axis_index("grp")
    depth, width = w.shape[1], w.shape[2]
    features = gain_ref.shape[0] * depth
    rows = x_ref.shape[0]
    blocks = state.shape[0] // SB
    heads = state.shape[1]

    def remote(src, dst, send, recv, kv, tp, grp=g):
        return pltpu.make_async_remote_copy(
            src, dst, send, recv, device_id={"grp": grp, "kv": kv, "tp": tp}, device_id_type=pl.DeviceIdType.MESH
        )

    here = pl.ds(k * depth, depth)
    locals_ = [
        pltpu.make_async_copy(src, dst, lsem.at[n])
        for n, (src, dst) in enumerate(
            (
                (x_hbm, x_ref), (gain_hbm, gain_ref), (keys_hbm, keys), (values_hbm, values), (fade_hbm, fade),
                (pull_hbm, pull), (count_hbm, counts), (extra_hbm, extra), (rate_hbm, rates), (offset_hbm, offset), (outer_hbm, outer),
                (wf.at[:, here], fs.at[0]), (ws.at[:, here], fs.at[1]),
            )
        )
    ]
    for load in locals_:
        load.start()
    f_load = pltpu.make_async_copy(wo, fbuf.at[k], fsem)
    f_load.start()
    loads = [
        pltpu.make_async_copy(
            src.at[:, pl.ds(h * DK, DK)], w.at[h, :, pl.ds(n * DK, DK)], wsem.at[h * 4 + n]
        )
        for h in range(heads)
        for n, src in enumerate((wq, wk, wv, wz))
    ]
    for load in loads:
        load.start()

    def fetch(i):
        return pltpu.make_async_copy(state.at[pl.ds(i * SB, SB)], s_in.at[i % 2], ins.at[i % 2])

    fetch(0).start()

    beside = t + 1 - 2 * (t % 2)
    across = (t + 2) % 4
    corner = t % 2
    landing = 2 * (t // 2) + k % 2
    home = corner == k % 2
    top_kind = t // 2 == k // 2
    source = jnp.where(top_kind, k, (k + 2) % 4)
    near_src = jnp.where(k <= 1, corner, corner + 2)
    far_src = jnp.where(k <= 1, corner + 2, corner)
    barrier = pltpu.get_barrier_semaphore()

    def greet(kv, tp, grp=g):
        pl.semaphore_signal(
            barrier, inc=1, device_id={"grp": grp, "kv": kv, "tp": tp}, device_id_type=pl.DeviceIdType.MESH
        )

    greet(k, beside)
    greet(k, across)
    greet(k, t, 1 - g)
    for step in range(1, 4):
        greet((k + step) % 4, t)

    @pl.when(t != k)
    def _():
        greet(t, landing)

    @pl.when(across != k)
    def _():
        greet(across, landing)

    @pl.when(near_src != k)
    def _():
        greet(near_src, source)

    @pl.when(far_src != k)
    def _():
        greet(far_src, source)

    @pl.when(home)
    def _():
        pl.semaphore_wait(barrier, 8)

    @pl.when(jnp.logical_not(home))
    def _():
        pl.semaphore_wait(barrier, 10)

    quarter = rows // 4
    locals_[0].wait()

    def part(q):
        return pl.ds(q * quarter, quarter)

    def forward(q):
        return remote(xpre.at[q], xbuf.at[k, part(2 + q)], xs.at[4 + q], xr.at[k, 2 + q], across, landing)

    def outward(q):
        return remote(x_ref.at[part(q)], xbuf.at[k, part(q)], xs.at[2 + q], xr.at[k, q], t, landing)

    def settled_copy(q):
        return pltpu.make_async_copy(x_ref.at[part(q)], xbuf.at[k, part(q)], xr.at[k, q])

    def sideways(q):
        return remote(x_ref.at[part(2 + q)], xpre.at[q], xs.at[q], xp.at[q], k, across)

    @pl.when(t == k)
    def _():
        for q in range(2):
            remote(x_ref.at[part(2 + q)], xbuf.at[k, part(2 + q)], xs.at[q], xr.at[k, 2 + q], k, across).start()
        for q in range(2):
            settled_copy(q).start()

    @pl.when(t != k)
    def _():
        for q in range(2):
            sideways(q).start()
        for q in range(2):
            outward(q).start()

    @pl.when(across != k)
    def _():
        for q in range(2):
            sideways(q).wait_recv()
            forward(q).start()

    end = jnp.where(k <= 1, 0, 3)
    near = jnp.where(k <= 1, 1, 2)
    is_end = k == end
    inside = jnp.logical_not(is_end)
    kind = jnp.where(top_kind, 0, 1)

    def piece(r, q, send, tp):
        at = pl.ds(q * quarter, quarter)
        return remote(xbuf.at[r, at], xbuf.at[r, at], xs.at[send], xr.at[r, q], k, tp)

    def spread(r, n, q):
        settled = jnp.logical_and(t == k, r == k)

        @pl.when(settled)
        def _():
            settled_copy(q).wait()

        @pl.when(jnp.logical_not(settled))
        def _():
            piece(r, 2 * kind + q, 6, across).wait_recv()

        piece(r, 2 * kind + q, 6 + n, across).start()
        piece(r, 2 * kind + q, 10 + n, beside).start()

    half_rows = fbuf.shape[1] // 2
    half = pl.ds(g * half_rows, half_rows)

    def f_pass(c, to, sem):
        return remote(fbuf.at[c, half], fbuf.at[c, half], fss.at[sem], fzr.at[c], to, t)

    def f_swap(c):
        return remote(fbuf.at[c, half], fbuf.at[c, half], fys.at[c], fyr.at[c], k, t, 1 - g)

    def f_begin():
        f_load.wait()

        @pl.when(k < 3)
        def _():
            f_pass(k, k + 1, 4).start()

        @pl.when(k > 0)
        def _():
            f_pass(k, k - 1, 5).start()

    pl.when(is_end)(f_begin)
    for q in range(2):
        spread(far_src, 2 * q + 1, q)
        spread(near_src, 2 * q, q)
    pl.when(inside)(f_begin)
    def cross_in(n, r):
        for q in range(2):
            piece(r, 2 - 2 * kind + q, 6, across).wait_recv()
            piece(r, 2 - 2 * kind + q, 14 + 2 * q + n, beside).start()

    def beside_in(r):
        for q in range(4):
            piece(r, q, 6, beside).wait_recv()

    near_mate = jnp.where(k <= 1, 1 - corner, 3 - corner)
    far_mate = jnp.where(k <= 1, 3 - corner, 1 - corner)
    lazy = jnp.logical_and(is_end, far_mate == 3 - end)
    for load in locals_[1:]:
        load.wait()
    thin[...] = rows_to_columns(
        jnp.concatenate([fade[...], pull[...], jnp.broadcast_to(counts[...].astype(f32), (8, counts.shape[1]))], axis=0)
    )
    for load in loads:
        load.wait()

    @pl.when(jnp.logical_not(lazy))
    def _():
        cross_in(1, far_src)


    def f_forwards(c):
        return jnp.logical_or(jnp.logical_and(c < k, k < 3), jnp.logical_and(c > k, k > 0))

    def f_take(c):
        to = jnp.where(c < k, k + 1, k - 1)
        f_pass(c, k, c).wait_recv()

        @pl.when(f_forwards(c))
        def _():
            f_pass(c, to, c).start()

        f_swap(c).start()

    f_order = (jnp.where(is_end, near, end), 3 - near, 3 - end)

    @pl.when(jnp.logical_or(inside, far_mate == 3 - end))
    def _():
        beside_in(far_mate)

    @pl.when(inside)
    def _():
        cross_in(0, near_src)
        beside_in(near_mate)

    nt = (((1,), (1,)), ((), ()))

    def prepare(r):
        floated = xbuf[r].astype(f32)
        gained = (floated * gain_ref[k]).astype(bf16)
        gbuf[r] = gained
        squares = floated * floated
        high = squares.astype(bf16)
        rest = (squares - high.astype(f32)).astype(bf16)
        ones = jnp.ones((8, depth), bf16)
        for n in range(2):
            every = lax.dot_general(fs[n], gained, nt, preferred_element_type=f32)
            esend[r, n * heads : (n + 1) * heads, :] = pick(t, [every[m * heads : (m + 1) * heads] for m in range(4)])
        esend[r, 2 * heads :, :] = lax.dot_general(ones, high, nt, preferred_element_type=f32) + lax.dot_general(
            ones, rest, nt, preferred_element_type=f32
        )

        @pl.when(r != k)
        def _():
            remote(esend.at[r], erecv.at[k], es.at[r], er.at[k], r, t).start()

    def product(r, c):
        return jnp.dot(gbuf[r], w[c], preferred_element_type=f32)

    def from_end(i):
        remote(abuf.at[i], abuf.at[i], ss.at[i], ar.at[i], k, beside).wait_recv()
        return abuf[i].astype(f32)

    def from_inner(i):
        remote(bbuf.at[i], bbuf.at[i], ss.at[i], br.at[i], k, beside).wait_recv()
        return bbuf[i].astype(f32)

    def accept(i):
        @pl.when(i + 1 < blocks)
        def _():
            fetch(i + 1).start()

        fetch(i).wait()

        few_rows = pl.ds(i * SB, SB)
        accepted_kernel(
            heads, s_in.at[i % 2], keys.at[few_rows], values.at[few_rows], thin.at[few_rows], taken.at[few_rows],
            r_scr, u_scr, c_scr, kf, vf,
        )

    def accept_some(low, high):
        def one(i, carry):
            accept(i)
            return carry

        lax.fori_loop(low, high, one, 0)

    chunk_head, chunk_stage = (0, 1, 0, 0, 2, 1, 1, 3, 2, 3, 2, 3), (0, 0, 1, 2, 0, 1, 2, 0, 1, 1, 2, 2)
    prepared = (3 - end, end, 3 - near, near)
    late = (3 - end, end, 3 - near, near, end)

    def settle_small():
        few_ref[...] = esend[k]
        for src in range(4):

            @pl.when(k != src)
            def _():
                remote(esend.at[src], erecv.at[src], es.at[src], er.at[src], k, beside).wait()
                few_ref[...] += erecv[src]

        small_terms(heads, features, few_ref[...], extra[...], rates[...], offset[...], small)

    def attention(h):
        attend_head(
            h, heads, blocks, (a0, a1, a2, a3, a4, a5, a6),
            lambda at, n: acc[h, at, n * DK : (n + 1) * DK], small, taken, outer[...], flat,
        )

    @pl.when(inside)
    def _():
        def one(i, carry):
            prepare(pick(i, prepared))
            return carry

        lax.fori_loop(0, 4, one, 0)
        f_take(f_order[0])
        accept_some(0, blocks // 2)
        f_take(f_order[1])

    def step(i, carry):
        h, stage = pick(i, chunk_head), pick(i, chunk_stage)
        r = pick(stage, (3 - end, 3 - near, near))

        @pl.when(jnp.logical_and(is_end, i == 2))
        def _():
            pl.when(lazy)(lambda: cross_in(1, far_src))
            cross_in(0, near_src)

            @pl.when(far_mate != 3 - end)
            def _():
                beside_in(far_mate)

            beside_in(near_mate)

        @pl.when(jnp.logical_and(is_end, jnp.logical_and(i < 5, i != 1)))
        def _():
            prepare(pick(i, late))

        @pl.when(is_end)
        def _():
            sbuf[i] = product(r, h).astype(bf16)
            remote(sbuf.at[i], abuf.at[i], ss.at[i], ar.at[i], near, t).start()

        @pl.when(jnp.logical_and(inside, stage < 2))
        def _():
            part = product(r, h)
            sbuf[i] = (part + from_end(i)).astype(bf16)
            remote(sbuf.at[i], bbuf.at[i], ss.at[i], br.at[i], 3 - near, t).start()

        @pl.when(jnp.logical_and(inside, i == 0))
        def _():
            accept_some(blocks // 2, blocks * 2 // 3)

        @pl.when(jnp.logical_and(inside, i == 1))
        def _():
            accept_some(blocks * 2 // 3, blocks)

        @pl.when(jnp.logical_and(inside, i == 3))
        def _():
            f_take(f_order[2])

        back = jnp.logical_or(jnp.logical_or(i == 4, i == 5), jnp.logical_or(i == 7, i == 9))

        @pl.when(jnp.logical_and(inside, back))
        def _():
            m = jnp.where(i <= 5, i - 4, jnp.where(i == 7, 2, 3))
            part = product(end, m)
            sbuf[12 + m] = (part + from_inner(pick(m, (0, 1, 4, 7)))).astype(bf16)
            remote(sbuf.at[12 + m], cbuf.at[m], ss.at[12 + m], cr.at[m], end, t).start()

        @pl.when(jnp.logical_and(inside, i == 5))
        def _():
            settle_small()

        ready = jnp.logical_or(jnp.logical_or(i == 5, i == 8), i == 10)

        @pl.when(jnp.logical_and(inside, ready))
        def _():
            m = i // 3 - 1
            acc[m] = product(near, m) + from_inner(pick(m, (2, 5, 8))) + from_end(pick(m, (3, 6, 10)))

        for m in range(3):

            @pl.when(jnp.logical_and(inside, i == (5, 8, 10)[m]))
            def _():
                attention(m)

        @pl.when(jnp.logical_and(inside, i == 11))
        def _():
            last[...] = product(near, 3) + from_inner(9) + from_end(11)

        return carry

    lax.fori_loop(0, 12, step, 0)

    @pl.when(is_end)
    def _():
        f_take(f_order[0])
        accept_some(0, blocks)
        settle_small()
        f_take(f_order[1])

        def returned(m):
            part = product(end, m)
            remote(cbuf.at[m], cbuf.at[m], ss.at[m], cr.at[m], k, beside).wait_recv()
            return part + cbuf[m].astype(f32)

        for m in range(3):
            acc[m] = returned(m)
            attention(m)
            if m == 0:
                f_take(f_order[2])
        last[...] = returned(3)

    for src in range(4):

        @pl.when(k != src)
        def _():
            remote(fbuf.at[src, half], fbuf.at[src, half], fys.at[src], fyr.at[src], k, beside).wait()

    for q in range(2):
        sideways(q).wait_send()

    @pl.when(t != k)
    def _():
        for q in range(2):
            outward(q).wait_send()

    @pl.when(across != k)
    def _():
        for q in range(2):
            forward(q).wait_send()

    for n in range(12):
        piece(k, 0, 6 + n, beside).wait_send()

    @pl.when(k < 3)
    def _():
        f_pass(k, k, 4).wait_send()

    @pl.when(k > 0)
    def _():
        f_pass(k, k, 5).wait_send()

    for src in range(4):

        @pl.when(jnp.logical_and(k != src, f_forwards(src)))
        def _():
            f_pass(src, k, src).wait_send()

    for i in range(12):

        @pl.when(is_end if chunk_stage[i] == 2 else k >= 0)
        def _():
            remote(sbuf.at[i], abuf.at[i], ss.at[i], ar.at[i], k, beside).wait_send()

    for m in range(4):

        @pl.when(inside)
        def _():
            remote(sbuf.at[12 + m], cbuf.at[m], ss.at[12 + m], cr.at[m], end, t).wait_send()


def project(x, gain, weights, forgetting, strength, final, state, keys, values, fade, pull, counts, extra, rates, offset, outer):
    rows, depth = x.shape
    width = weights[0].shape[1]
    seqs, heads = state.shape[:2]
    few_rows = 2 * heads + 8
    vmem, hbm = pl.BlockSpec(memory_space=pltpu.VMEM), pl.BlockSpec(memory_space=pl.ANY)
    dma = pltpu.SemaphoreType.DMA
    gain = gain.reshape(-1, 1, depth)
    rates, offset, outer = rates.reshape(1, heads), offset.reshape(1, heads), outer.reshape(1, DK)
    forgetting, strength = forgetting.T, strength.T

    def chunks(n):
        return pltpu.VMEM((n, rows, width), bf16)

    def like(a):
        return pltpu.VMEM(a.shape, a.dtype)

    return pl.pallas_call(
        project_kernel,
        in_specs=[hbm] * 19,
        out_specs=[vmem] * 5,
        out_shape=[
            pltpu.VMEM((rows, width), f32),
            pltpu.VMEM((rows, few_rows), f32),
            pltpu.VMEM(state.shape, f32),
            pltpu.VMEM((4,) + final.shape, bf16),
            pltpu.VMEM((rows, width), bf16),
        ],
        scratch_shapes=[
            like(x), like(gain), like(keys), like(values), like(fade), like(pull), like(counts),
            like(extra), like(rates), like(offset), like(outer),
            pltpu.VMEM((2, forgetting.shape[0], depth), bf16),
            pltpu.VMEM((seqs, 2 * P_SIZE * heads + 8), f32),
            pltpu.VMEM((few_rows, rows), f32),
            pltpu.VMEM((3, rows, width), f32),
            pltpu.VMEM((2, rows // 4, depth), bf16),
            pltpu.VMEM((4, rows, depth), bf16),
            pltpu.VMEM((4, rows, depth), bf16),
            pltpu.VMEM((4, depth, width), bf16),
            chunks(16), chunks(12), chunks(12), chunks(4),
            pltpu.VMEM((4, few_rows, rows), f32),
            pltpu.VMEM((4, few_rows, rows), f32),
            pltpu.VMEM((2, SB) + state.shape[1:], f32),
            *[pltpu.VMEM((heads * n, DK), f32) for n in (TALL, TALL, SB, TALL, TALL)],
            *[pltpu.VMEM((GROUP * TALL, DK), f32)] * 7,
            dma((13,)), dma((18,)), dma((2,)), dma((4, 4)), dma((16,)), dma((16,)), dma((12,)), dma((12,)), dma((4,)), dma((4,)),
            dma((4,)), dma((2,)), dma, dma((6,)), dma((4,)), dma((4,)), dma((4,)),
        ],
        compiler_params=pltpu.CompilerParams(has_side_effects=True, collective_id=0, vmem_limit_bytes=LIMIT),
        name="project",
    )(x, gain, keys, values, fade, pull, counts, extra, rates, offset, outer, forgetting, strength, *weights, final, state)


PIECES = 3


def mix_kernel(part, o_ref, mate, sent, cross, ms, mr, xs, xr):
    k, t, g = lax.axis_index("kv"), lax.axis_index("tp"), lax.axis_index("grp")
    rows = part.shape[1]
    piece = rows // PIECES
    beside = t + 1 - 2 * (t % 2)
    across = (t + 2) % 4
    order = ((beside + 2) % 4, beside)

    def remote(src, dst, send, recv, tp):
        return pltpu.make_async_remote_copy(
            src, dst, send, recv, device_id={"grp": g, "kv": k, "tp": tp}, device_id_type=pl.DeviceIdType.MESH
        )

    barrier = pltpu.get_barrier_semaphore()
    for peer in (beside, across):
        pl.semaphore_signal(
            barrier, inc=1, device_id={"grp": g, "kv": k, "tp": peer}, device_id_type=pl.DeviceIdType.MESH
        )
    pl.semaphore_wait(barrier, 2)

    def to_mate(n, s):
        at = pl.ds(s * piece, piece)
        return remote(part.at[order[n], at], mate.at[n, at], ms.at[n, s], mr.at[n, s], beside)

    def to_cross(s):
        at = pl.ds(s * piece, piece)
        return remote(sent.at[at], cross.at[at], xs.at[s], xr.at[s], across)

    for n in range(2):
        for s in range(PIECES):
            to_mate(n, s).start()
    for s in range(PIECES):
        at = slice(s * piece, (s + 1) * piece)
        to_mate(0, s).wait_recv()
        sent[at, :] = (part[across, at, :].astype(f32) + mate[0, at, :].astype(f32)).astype(bf16)
        to_cross(s).start()
    for s in range(PIECES):
        at = slice(s * piece, (s + 1) * piece)
        to_mate(1, s).wait_recv()
        to_cross(s).wait_recv()
        o_ref[at, :] = (
            part[t, at, :].astype(f32) + mate[1, at, :].astype(f32) + cross[at, :].astype(f32)
        ).astype(bf16)
    for s in range(PIECES):
        to_mate(0, s).wait_send()
        to_mate(1, s).wait_send()
        to_cross(s).wait_send()


def mix(part):
    rows, cols = part.shape[1:]
    vmem = pl.BlockSpec(memory_space=pltpu.VMEM)
    dma = pltpu.SemaphoreType.DMA
    return pl.pallas_call(
        mix_kernel,
        in_specs=[vmem],
        out_specs=vmem,
        out_shape=jax.ShapeDtypeStruct((rows, cols), bf16),
        scratch_shapes=[
            pltpu.VMEM((2, rows, cols), bf16),
            pltpu.VMEM((rows, cols), bf16),
            pltpu.VMEM((rows, cols), bf16),
            dma((2, PIECES)), dma((2, PIECES)), dma((PIECES,)), dma((PIECES,)),
        ],
        compiler_params=pltpu.CompilerParams(has_side_effects=True, collective_id=1, vmem_limit_bytes=LIMIT),
        name="mix",
    )(local(part))


def on_device(
    n_kv,
    n_tp,
    candidate_embeddings,
    incoming_rms_scaling,
    probe_projector,
    address_projector,
    content_projector,
    sigmoid_mask_matrix,
    forgetting_projector,
    strength_projector_matrix,
    channel_forgetting_rates,
    forgetting_offset,
    extra_forgetting,
    outgoing_rms_scaling,
    final_projector,
    memory_matrix,
    earlier_addresses,
    earlier_contents,
    earlier_strengths,
    earlier_forgetting,
    admitted_counts,
):
    rows, local_cols = candidate_embeddings.shape
    features = incoming_rms_scaling.shape[0]
    depth, width = probe_projector.shape
    heads = width // DK
    seqs = rows // P_SIZE
    k_index, t_index = lax.axis_index("kv"), lax.axis_index("tp")

    def thin(values):
        return values.transpose(1, 2, 0).reshape(P_SIZE * heads, seqs)

    weights = (probe_projector, address_projector, content_projector, sigmoid_mask_matrix)
    fade, pull, extra = thin(earlier_forgetting), thin(earlier_strengths), thin(extra_forgetting)
    if n_kv == 4 and n_tp == 4:
        last, small, taken, columns, flat = project(
            candidate_embeddings, incoming_rms_scaling, weights, forgetting_projector, strength_projector_matrix,
            final_projector, memory_matrix, earlier_addresses, earlier_contents, fade, pull, admitted_counts.reshape(1, seqs), extra,
            channel_forgetting_rates, forgetting_offset, outgoing_rms_scaling,
        )
        part, taken = last_head(small, outgoing_rms_scaling, last, taken, flat, columns)
        mixed = mix(part)
    else:
        every = lax.all_gather(candidate_embeddings, "tp", axis=1, tiled=True)
        every = lax.all_to_all(every, "kv", split_axis=1, concat_axis=0, tiled=True)
        gain_part = lax.dynamic_slice_in_dim(incoming_rms_scaling, k_index * depth, depth)
        floated = every.astype(f32)
        gained = (floated * gain_part).astype(bf16)
        decay_cols = lax.dynamic_slice(forgetting_projector, (k_index * depth, t_index * heads), (depth, heads))
        beta_cols = lax.dynamic_slice(strength_projector_matrix, (k_index * depth, t_index * heads), (depth, heads))
        few = jnp.concatenate(
            [
                jnp.dot(gained, jnp.concatenate([decay_cols, beta_cols], axis=1), preferred_element_type=f32),
                jnp.sum(floated * floated, axis=1, keepdims=True),
            ],
            axis=1,
        )
        few = lax.psum_scatter(few, "kv", scatter_dimension=0, tiled=True)
        few = jnp.pad(few, ((0, 0), (0, 7))).T
        partial = jnp.stack([jnp.dot(gained, w, preferred_element_type=f32).astype(bf16) for w in weights])
        summed = lax.psum_scatter(partial, "kv", scatter_dimension=1, tiled=True).astype(f32)
        counts = admitted_counts.astype(f32).reshape(seqs, 1)
        keys, values = earlier_addresses.reshape(rows, width), earlier_contents.reshape(rows, width)
        taken = accepted(memory_matrix, keys, values, jnp.concatenate([fade.T, pull.T, counts], axis=1))
        flat, taken = attend(
            features, taken, summed, few, extra, channel_forgetting_rates, forgetting_offset, outgoing_rms_scaling
        )
        gathered = lax.all_gather(flat, "kv", axis=0, tiled=True)
        terms = jnp.dot(gathered, final_projector, preferred_element_type=f32).astype(bf16)
        terms = lax.all_to_all(terms, "kv", split_axis=0, concat_axis=1, tiled=True)
        mixed = lax.psum_scatter(terms, "tp", scatter_dimension=1, tiled=True)
    return (mixed, taken)


def solution(mesh):
    row, per_head = P(("grp", "kv"), "tp"), P(("grp", "kv"), None, "tp")
    four = P(("grp", "kv"), None, "tp", None)
    weight = P("kv", "tp")
    state = P(("grp", "kv"), "tp", None, None)
    in_specs = (
        row, P(), weight, weight, weight, weight, P(), P(), P("tp"), P("tp"), per_head, P(),
        P("tp", "kv"), state, four, four, per_head, per_head, P(("grp", "kv")),
    )
    body = functools.partial(on_device, mesh.shape["kv"], mesh.shape["tp"])
    return jax.shard_map(body, mesh=mesh, in_specs=in_specs, out_specs=(row, state), check_vma=False)
```
